32 devices in a mesh: ep: 8 (over z, x), tp: 4 (over y, core).
Axes of the slice: x: 2, y: 2, z: 4, core: 2. Of those that a mesh axis runs over, the one named last changes fastest.
Arguments:
- queries: bfloat16 [1024, 1024], P('ep', 'tp'), may hold values from -6 to 6
- key_states: bfloat16 [1024, 256], P('ep'), may hold values from -192 to 192
- value_states: bfloat16 [1024, 256], P('ep'), may hold values from -12 to 12
- sink_logit: float32 [16], P('tp'), may hold values from 3 to 7
- out_weight: bfloat16 [1024, 2048], P('tp'), may hold values from -0.1875 to 0.1875
- expert_input: bfloat16 [1024, 2048], P('ep'), may hold values from -6 to 6
- norm_gain: float32 [2048], replicated, may hold values from 0.1 to 1.9
- routes: int32 [1024, 2], P('ep'), may hold values from 0 to 7, all different within a row; in each aligned block of 128 rows (0 to 127, 128 to 255, ...) at most 40 rows name the same one
- route_weight: float32 [1024, 2], P('ep'), may hold values from 0.1 to 1
- gate_weight: bfloat16 [8, 2048, 4096], P('ep', None, 'tp'), may hold values from -0.125 to 0.125
- up_weight: bfloat16 [8, 2048, 4096], P('ep', None, 'tp'), may hold values from -0.125 to 0.125
- down_weight: bfloat16 [8, 4096, 2048], P('ep', 'tp'), may hold values from -0.125 to 0.125
Outputs:
- mixer_out: bfloat16 [1024, 2048], P(('ep', 'tp'))
- expert_out: bfloat16 [1024, 2048], P('ep', 'tp')
The draws below stay inside these ranges and needn't reach their ends.
Inputs may be any that keep to these rules, and one draw needn't show every extreme that they name: `routes`: each row names 2 different experts. Within the rows of one index of ep (aligned blocks of 128 rows) no expert is named more than 40 times, a bound that some blocks reach.
All inputs are finite; a program needn't handle non-finite values.
Results may differ from the reference program's by a relative error of at most 0.025.
Values may be sent and summed in bfloat16 or wider, within the bound.
A program may use at most 64 MiB of HBM per device.

```python
import math
import jax
import jax.numpy as jnp
import numpy as np
from jax import lax

D = 2048
HEADS = 16
KV_HEADS = 4
HEAD_DIM = 64
FF = 4096
WINDOW = 128
TOP = 2
TOK_DEV = 128
TOKENS = 1024
EXPERTS = 8
CAP = 40
HEADS_DEV = 4
FF_DEV = 1024
N_EP = 8
N_TP = 4


def draw_key_states(key, part):
    normal_draw = jax.random.truncated_normal(key, -4.0, 4.0, (TOKENS, KV_HEADS * HEAD_DIM), jnp.float32)
    return normal_draw.astype(jnp.bfloat16)


def spiked(array, own_key, source, target, blocks, factor):
    def block_of(position):
        return (jnp.arange(array.shape[position]) // (array.shape[position] // blocks)).reshape((-1,) + (1,) * (array.ndim - 1 - position))

    first = jax.random.permutation(own_key, blocks)[block_of(target)]
    other_side = (block_of(target) + blocks // 2) % blocks
    return jnp.where((block_of(source) == first) | (block_of(source) == other_side), factor * array, array)


def level_of(key, extent, split, least, top_value):
    level = 1.0
    for position, parts in split:
        steps = jax.random.uniform(jax.random.fold_in(jax.random.fold_in(key, 6), position), (parts,), jnp.float32, least / len(split), top_value / len(split))
        level = level * jnp.repeat(jnp.exp(steps), extent[position] // parts).reshape((-1,) + (1,) * (len(extent) - 1 - position))
    return level


def deal_out(rng, own, number, rows, amount, top, limit, skew):
    sequence = jax.random.permutation(rng, amount)
    crowded, common = shares(amount, rows * top, limit, skew, True), shares(amount, rows * top, limit, skew, False)
    places = jnp.arange(amount)

    def named(lengths, rotation):
        used = int((lengths > 0).sum())
        fixed = max(1, used // 4)
        shifted = fixed + (places - fixed + rotation * (used - fixed)) % max(1, amount - fixed)
        return jnp.zeros((amount,), jnp.int32).at[sequence[jnp.where(places < fixed, places, shifted)]].set(jnp.asarray(lengths, jnp.int32))

    lengths = jnp.where(number % 4 == 0, named(crowded, number // 4), named(common, number - number // 4 - 1))
    mixed = jax.random.permutation(jax.random.fold_in(own, 3), amount)
    source_of, receiver = mixed[0:amount // 2 * 2:2], mixed[1:amount // 2 * 2:2]
    slack = jnp.minimum(lengths[source_of] - 1, limit - lengths[receiver]) // 2
    slack = jnp.where((source_of == sequence[0]) | (receiver == sequence[0]) | (lengths[receiver] == 0), 0, jnp.maximum(slack, 0))
    shifted = jax.random.randint(jax.random.fold_in(own, 4), (amount // 2,), 0, 1 << 20) % (slack + 1)
    lengths = lengths.at[source_of].add(-shifted).at[receiver].add(shifted)
    labels = jnp.searchsorted(jnp.cumsum(lengths), jnp.arange(rows * top), side="right").astype(jnp.int32)
    grid = labels.reshape(top, rows).T
    grid = grid[jax.random.permutation(jax.random.fold_in(own, 1), rows)]
    rotation = jax.random.randint(jax.random.fold_in(own, 2), (rows, 1), 0, top)
    return jnp.take_along_axis(grid, (jnp.arange(top)[None, :] + rotation) % top, axis=1)


def shares(amount, total, reach, slope, full):
    weights = [(1 << 20) // math.isqrt(grade ** slope) + 1 for grade in range(1, amount + 1)]
    largest = reach if full else min(reach, max(-(-total // amount), total * weights[0] // sum(weights)))
    least = 1 if total - largest >= amount - 1 else 0
    counts, rest = [largest] + [least] * (amount - 1), total - largest - least * (amount - 1)
    while rest > 0:
        free = [i for i in range(1, amount) if counts[i] < largest] or [i for i in range(1, amount) if counts[i] < reach]
        pool, remaining = sum([weights[i] for i in free]), rest
        for i in free:
            more = min(reach - counts[i], max(1, remaining * weights[i] // pool), rest)
            counts[i] = counts[i] + more
            rest = rest - more
    return np.array(counts)


def normal_values(stream_key, dims, scale, limit, shards=(), held_as=jnp.bfloat16):
    factor_of = level_of(stream_key, dims, shards, -0.22, 0.18) if shards else 1.0
    array = jax.random.normal(stream_key, dims, jnp.float32) * scale * factor_of
    return jnp.minimum(jnp.maximum(array, -limit), limit).astype(held_as)


def noise_with(own_key, extent, scale, limit, shards, heavy, held_as=jnp.bfloat16):
    entries = scale * jax.random.normal(own_key, extent, jnp.float32)
    if shards:
        entries = entries * level_of(own_key, extent, shards, -0.22, 0.18)
    return jnp.clip(spiked(entries, jax.random.fold_in(own_key, 3), *heavy), -limit, limit).astype(held_as)


def setup_inputs(seed: int = 0) -> dict:
    keys = jax.random.split(jax.random.key(seed), 13)
    queries = normal_values(keys[0], (TOKENS, HEADS * HEAD_DIM), 1.0, 6.0, ((0, 8), (1, 4)))
    key_states = draw_key_states(jax.random.fold_in(keys[12], 71), 0)
    value_states = normal_values(keys[2], (TOKENS, KV_HEADS * HEAD_DIM), 2.0, 12.0, ((0, 8),))
    sink_logit = jnp.clip(3.0 + 4.0 * jax.random.uniform(keys[3], (HEADS,), jnp.float32) ** level_of(keys[3], (HEADS,), ((0, 4),), -0.2, 0.2), 3.0, 7.0)
    out_weight = normal_values(keys[4], (HEADS * HEAD_DIM, D), (HEADS * HEAD_DIM) ** -0.5, 0.1875, ((0, 4),))
    expert_input = normal_values(keys[5], (TOKENS, D), 1.0, 6.0, ((0, 8),))
    norm_gain = jnp.clip(1.0 + 0.18 * jax.random.normal(keys[6], (D,), jnp.float32), 0.1, 1.9)
    routes_keys = jax.random.split(jax.random.fold_in(keys[7], 1), TOKENS // TOK_DEV)
    routes_turns = jax.random.permutation(jax.random.fold_in(keys[7], 3), TOKENS // TOK_DEV)
    routes = jax.vmap(lambda own, number: deal_out(jax.random.fold_in(keys[7], 2), own, number, TOK_DEV, EXPERTS, TOP, CAP, 1))(routes_keys, routes_turns).reshape((TOKENS, TOP))
    route_weight = jnp.clip(0.1 + 0.9 * jax.random.uniform(keys[8], (TOKENS, TOP), jnp.float32) ** level_of(keys[8], (TOKENS, TOP), ((0, 8),), -0.2, 0.2), 0.1, 1.0)
    gate_weight = normal_values(keys[9], (EXPERTS, D, FF), D ** -0.5, 0.125, ((0, 8), (2, 4)))
    up_weight = normal_values(keys[10], (EXPERTS, D, FF), D ** -0.5, 0.125, ((0, 8), (2, 4)))
    down_weight = noise_with(keys[11], (EXPERTS, FF, D), FF ** -0.5, 0.125, ((0, 8), (1, 4)), (1, 2, 4, 2.0))
    return dict(queries=queries, key_states=key_states, value_states=value_states, sink_logit=sink_logit, out_weight=out_weight, expert_input=expert_input, norm_gain=norm_gain, routes=routes, route_weight=route_weight, gate_weight=gate_weight, up_weight=up_weight, down_weight=down_weight)


NORM_EPSILON = 1e-05
ROTARY_BASE = 500000.0
MASK_VALUE = -1e+30

def layer_norm(activations, norm_gain):
    values = activations.astype(jnp.float32)
    average = lax.optimization_barrier(jnp.mean(values, axis=-1, keepdims=True))
    centred = values - average
    variance = lax.optimization_barrier(jnp.mean(centred * centred, axis=-1, keepdims=True))
    return (centred * lax.rsqrt(variance + NORM_EPSILON) * norm_gain).astype(jnp.bfloat16)

def rotate(head_rows, positions):
    half_dim = head_rows.shape[-1] // 2
    exponent = jnp.arange(half_dim, dtype=jnp.float32) * (2.0 / head_rows.shape[-1])
    frequency = jnp.power(jnp.float32(ROTARY_BASE), -exponent)
    angles = positions.astype(jnp.float32)[:, None] * frequency[None, :]
    cosine = jnp.cos(angles)[:, None, :]
    sine_part = jnp.sin(angles)[:, None, :]
    first_half = head_rows[..., :half_dim].astype(jnp.float32)
    second_half = head_rows[..., half_dim:].astype(jnp.float32)
    turned = jnp.concatenate([first_half * cosine - second_half * sine_part, second_half * cosine + first_half * sine_part], axis=-1)
    return turned.astype(jnp.bfloat16)

def attention(queries, key_states, value_states, sink_logit):
    token_count = queries.shape[0]
    group_size = HEADS // KV_HEADS
    positions = jnp.arange(token_count, dtype=jnp.int32)
    turned_query = rotate(queries.reshape(token_count, HEADS, HEAD_DIM), positions)
    turned_key = rotate(key_states.reshape(token_count, KV_HEADS, HEAD_DIM), positions)
    padding = jnp.zeros((WINDOW, KV_HEADS, HEAD_DIM), jnp.bfloat16)
    padded_key = jnp.concatenate([padding, turned_key, padding], axis=0)
    padded_value = jnp.concatenate([padding, value_states.reshape(token_count, KV_HEADS, HEAD_DIM), padding], axis=0)
    span_length = TOK_DEV + 2 * WINDOW
    sinks = sink_logit.astype(jnp.float32).reshape(KV_HEADS, group_size)[:, :, None, None]

    def attend(block_index):
        offset = block_index * TOK_DEV
        block_query = lax.dynamic_slice_in_dim(turned_query, offset, TOK_DEV, 0)
        block_query = block_query.reshape(TOK_DEV, KV_HEADS, group_size, HEAD_DIM).astype(jnp.float32)
        block_key = lax.dynamic_slice_in_dim(padded_key, offset, span_length, 0).astype(jnp.float32)
        block_value = lax.dynamic_slice_in_dim(padded_value, offset, span_length, 0).astype(jnp.float32)
        scores = jnp.einsum('qkgd,skd->kgqs', block_query, block_key) * HEAD_DIM ** (-0.5)
        query_pos = offset + jnp.arange(TOK_DEV, dtype=jnp.int32)[:, None]
        key_pos = offset - WINDOW + jnp.arange(span_length, dtype=jnp.int32)[None, :]
        allowed = (jnp.abs(query_pos - key_pos) <= WINDOW) & (key_pos >= 0) & (key_pos < token_count)
        scores = jnp.where(allowed, scores, MASK_VALUE)
        largest = jnp.maximum(lax.optimization_barrier(jnp.max(scores, axis=-1, keepdims=True)), sinks)
        weights = jnp.exp(scores - largest)
        denominator = lax.optimization_barrier(jnp.sum(weights, axis=-1, keepdims=True)) + jnp.exp(sinks - largest)
        probability = lax.optimization_barrier((weights / denominator).astype(jnp.bfloat16))
        attended = jnp.einsum('kgqs,skd->qkgd', probability.astype(jnp.float32), block_value)
        return attended.astype(jnp.bfloat16).reshape(TOK_DEV, HEADS * HEAD_DIM)
    blocks = lax.map(attend, jnp.arange(token_count // TOK_DEV, dtype=jnp.int32))
    return blocks.reshape(token_count, HEADS * HEAD_DIM)

def reference(queries, key_states, value_states, sink_logit, out_weight, expert_input, norm_gain, routes, route_weight, gate_weight, up_weight, down_weight):
    attended = attention(queries, key_states, value_states, sink_logit)
    column_count = HEADS_DEV * HEAD_DIM

    def add_group(running, group_index):
        part_rows = lax.dynamic_slice_in_dim(attended, group_index * column_count, column_count, 1)
        part_weight = lax.dynamic_slice_in_dim(out_weight, group_index * column_count, column_count, 0)
        partial_value = jnp.dot(part_rows, part_weight, preferred_element_type=jnp.float32).astype(jnp.bfloat16)
        partial_value = lax.optimization_barrier(partial_value)
        return (running + partial_value.astype(jnp.float32), None)
    mixer_total, _ = lax.scan(add_group, jnp.zeros((TOKENS, D), jnp.float32), jnp.arange(N_TP, dtype=jnp.int32))
    mixer_out = mixer_total.astype(jnp.bfloat16)
    normed = layer_norm(expert_input, norm_gain)
    assign_count = TOK_DEV * TOP
    expert_ids = routes.reshape(N_EP, assign_count)
    matches = (expert_ids[:, :, None] == jnp.arange(EXPERTS, dtype=jnp.int32)[None, None, :]).astype(jnp.int32)
    slot_rank = lax.optimization_barrier(jnp.sum((jnp.cumsum(matches, axis=1) - matches) * matches, axis=2))
    slot_index = jnp.arange(N_EP, dtype=jnp.int32)[:, None] * CAP + slot_rank
    token_ids = jnp.arange(N_EP, dtype=jnp.int32)[:, None] * TOK_DEV + jnp.arange(assign_count, dtype=jnp.int32)[None, :] // TOP
    slot_rows = N_EP * CAP
    flat_place = (expert_ids * slot_rows + slot_index).reshape(-1)
    slot_token = jnp.zeros((EXPERTS * slot_rows,), jnp.int32).at[flat_place].set(token_ids.reshape(-1))
    slot_token = slot_token.reshape(EXPERTS, slot_rows)

    def run_expert(expert_id):
        gathered = jnp.take(normed, slot_token[expert_id], axis=0)
        gate_act = jnp.dot(gathered, gate_weight[expert_id], preferred_element_type=jnp.float32)
        up_act = jnp.dot(gathered, up_weight[expert_id], preferred_element_type=jnp.float32)
        hidden = (jax.nn.silu(gate_act) * up_act).astype(jnp.bfloat16)
        hidden_parts = hidden.reshape(slot_rows, N_TP, FF_DEV).astype(jnp.float32)
        down_parts = down_weight[expert_id].reshape(N_TP, FF_DEV, D).astype(jnp.float32)
        partial_value = jnp.einsum('rjf,jfd->jrd', hidden_parts, down_parts).astype(jnp.bfloat16)
        partial_value = lax.optimization_barrier(partial_value)
        return lax.optimization_barrier(jnp.sum(partial_value.astype(jnp.float32), axis=0)).astype(jnp.bfloat16)
    results = lax.map(run_expert, jnp.arange(EXPERTS, dtype=jnp.int32))
    picked = results[expert_ids, slot_index].reshape(TOKENS, TOP, D).astype(jnp.float32)
    rounded_weight = lax.optimization_barrier(route_weight.astype(jnp.bfloat16)).astype(jnp.float32)
    expert_out = lax.optimization_barrier(jnp.sum(rounded_weight[:, :, None] * picked, axis=1)).astype(jnp.bfloat16)
    return (mixer_out, expert_out)
```

```python
import functools

import jax
import jax.numpy as jnp
import numpy as np
from jax import lax
from jax.experimental import pallas as pl
from jax.experimental.pallas import tpu as pltpu
from jax.sharding import PartitionSpec as P

HEADS = 16
KV_HEADS = 4
HEAD_DIM = 64
WINDOW = 128
TOP = 2
LANES = 128


NORM_EPSILON = 1e-05
ROTARY_BASE = 500000.0
MASK_VALUE = -1e30


def layer_norm(activations, norm_gain):
    values = activations.astype(jnp.float32)
    average = jnp.mean(values, axis=-1, keepdims=True)
    centred = values - average
    variance = jnp.mean(centred * centred, axis=-1, keepdims=True)
    return (centred * lax.rsqrt(variance + NORM_EPSILON) * norm_gain).astype(jnp.bfloat16)


def angle_table(row_count, blocks):
    lane = np.arange(LANES) % HEAD_DIM
    half_dim = HEAD_DIM // 2
    frequency = ROTARY_BASE ** (-2.0 * (lane % half_dim) / HEAD_DIM)
    sign = np.where(lane < half_dim, -1.0, 1.0)
    rows = np.arange(row_count)[:, None] * frequency[None, :]
    bases = np.arange(blocks)[:, None] * row_count * frequency[None, :]
    return np.concatenate(
        [np.cos(rows), sign * np.sin(rows), np.cos(bases), sign * np.sin(bases)]
    ).astype(np.float32)


def partner(index, mask):
    flipped, bit = index, 1
    while bit <= mask:
        if mask & bit:
            flipped = flipped + bit * (1 - 2 * lax.rem(index // bit, 2))
        bit *= 2
    return flipped


def fused_kernel(
    sizes,
    query_hbm,
    key_hbm,
    value_hbm,
    table_hbm,
    sink_hbm,
    input_hbm,
    gain_hbm,
    routes_hbm,
    route_weight_hbm,
    out_hbm,
    gate_hbm,
    up_hbm,
    down_hbm,
    mixer_ref,
    expert_ref,
    query_v,
    key_v,
    value_v,
    table_v,
    sink_v,
    input_v,
    gain_v,
    routes_v,
    route_weight_v,
    out_w,
    gate_w,
    up_w,
    down_w,
    normed_v,
    own_kv,
    halo_send,
    low_kv,
    high_kv,
    packed,
    rows_in,
    gathered,
    hidden,
    mix_send,
    mix_sib,
    mix_cross,
    mix_recv,
    sib_send,
    sib_recv,
    own_acc,
    cross_send,
    cross_recv,
    final_send,
    returned,
    combine_left,
    combine_right,
    load_sem,
    halo_send_sem,
    halo_recv_sem,
    send_sem,
    net_recv_sem,
    far_recv_sem,
    near_recv_sem,
    mix_sib_recv_sem,
    mix_recv_sem,
    sib_recv_sem,
    cross_recv_sem,
    final_recv_sem,
):
    n_ep, n_tp, main, tail = sizes
    cap = main + tail
    halves = 2 if tail else 1
    f32, bf16 = jnp.float32, jnp.bfloat16
    me, my_tp = lax.axis_index("ep"), lax.axis_index("tp")
    core = lax.rem(my_tp, 2)
    pair = my_tp // 2
    n_pair = n_tp // 2
    sibling = my_tp + 1 - 2 * core
    row_count, width = input_v.shape
    slice_width = width // n_tp
    piece = slice_width // halves
    head_dim = HEAD_DIM
    local_heads = sink_v.shape[1]
    half_count = n_ep // 2
    near = list(range(half_count))
    groups = [
        list(range(3 * n_ep // 4, n_ep)),
        list(range(half_count, 3 * n_ep // 4)),
        near,
    ]
    experts_of = [partner(me, k) for k in range(n_ep)]
    pair_up = [lax.rem(pair + p, n_pair) for p in range(n_pair)]
    pair_down = [lax.rem(pair + n_pair - p, n_pair) for p in range(n_pair)]

    names = [
        (routes_hbm, routes_v),
        (route_weight_hbm, route_weight_v),
        (gain_hbm, gain_v),
        (input_hbm, input_v),
        (table_hbm, table_v),
        (key_hbm, key_v),
        (value_hbm, value_v),
        (query_hbm, query_v),
        (out_hbm, out_w),
        (gate_hbm.at[0], gate_w),
        (up_hbm.at[0], up_w),
        (down_hbm.at[0], down_w),
        (sink_hbm, sink_v),
    ]
    shared = my_tp * local_heads // (HEADS // KV_HEADS)
    shared_sib = sibling * local_heads // (HEADS // KV_HEADS)
    block = pl.ds(pl.multiple_of(shared // 2 * LANES, LANES), LANES)
    names[5] = (key_hbm.at[:, block], key_v)
    names[6] = (value_hbm.at[:, block], value_v)
    loads = [
        pltpu.make_async_copy(source, target, load_sem.at[number])
        for number, (source, target) in enumerate(names)
    ]

    def remote(source, target, send_sem, recv_sem, ep, tp):
        return pltpu.make_async_remote_copy(
            src_ref=source,
            dst_ref=target,
            send_sem=send_sem,
            recv_sem=recv_sem,
            device_id=(ep, tp),
            device_id_type=pl.DeviceIdType.MESH,
        )

    barrier = pltpu.get_barrier_semaphore()
    for k in range(n_ep - 1, 0, -1):
        pl.semaphore_signal(
            barrier, inc=1, device_id=(experts_of[k], sibling),
            device_id_type=pl.DeviceIdType.MESH,
        )
    for step in range(1, n_tp):
        pl.semaphore_signal(
            barrier, inc=1, device_id=(me, lax.rem(my_tp + step, n_tp)),
            device_id_type=pl.DeviceIdType.MESH,
        )
    for load in loads:
        load.start()

    def start(copy):
        copy.start()

    def arrived(target, sem):
        pltpu.make_async_copy(target, target, sem).wait()

    loads[0].wait()
    routes = [routes_v[k : k + 1, :] for k in range(TOP)]
    expert_iota = lax.broadcasted_iota(jnp.int32, (n_ep, row_count), 0)
    named = [(routes[k] == expert_iota).astype(f32) for k in range(TOP)]
    earlier = (
        lax.broadcasted_iota(jnp.int32, (row_count, row_count), 0)
        < lax.broadcasted_iota(jnp.int32, (row_count, row_count), 1)
    )
    ahead = jnp.dot(
        functools.reduce(jnp.add, named).astype(bf16),
        earlier.astype(f32).astype(bf16),
        preferred_element_type=f32,
    )
    rank = [
        jnp.sum(ahead * named[k], axis=0, keepdims=True).astype(jnp.int32) for k in range(TOP)
    ]

    def slot_onehot(k):
        slot = lax.broadcasted_iota(jnp.int32, (cap, row_count), 0)
        chosen = [(jnp.where(routes[j] == experts_of[k], rank[j], -1) == slot) for j in range(TOP)]
        return functools.reduce(jnp.logical_or, chosen).astype(f32)

    def pack(values):
        if not tail:
            return values
        parts = [values[:main, :piece], values[:main, piece:], values[main:, :piece], values[main:, piece:]]
        return jnp.concatenate(parts, axis=0)

    order = [k for group in groups for k in group]
    far = [k for k in order if k >= half_count]
    close = [k for k in order if k < half_count]
    for number in range(4, 7):
        loads[number].wait()
    lane = lax.broadcasted_iota(jnp.int32, (row_count, LANES), 1)
    low_lane = lane < head_dim
    first_half = lax.rem(lane, head_dim) < head_dim // 2
    row_cos, row_sin = table_v[:row_count], table_v[row_count : 2 * row_count]
    base_cos = table_v[pl.ds(2 * row_count + me, 1), :]
    base_sin = table_v[pl.ds(2 * row_count + n_ep + me, 1), :]
    cosine = base_cos * row_cos - base_sin * row_sin
    sine = base_sin * row_cos + base_cos * row_sin

    def turn(values):
        values = values.astype(f32)
        other = jnp.where(
            first_half,
            pltpu.roll(values, LANES - head_dim // 2, 1),
            pltpu.roll(values, head_dim // 2, 1),
        )
        return values * cosine + other * sine

    turned = turn(key_v[...])
    value = value_v[...].astype(f32)
    turned_roll, value_roll = pltpu.roll(turned, head_dim, 1), pltpu.roll(value, head_dim, 1)

    def key_value(head):
        upper = lax.rem(head, 2) == 1
        return jnp.where(
            low_lane,
            jnp.where(upper, turned_roll, turned),
            jnp.where(upper, value, value_roll),
        ).astype(bf16)

    own_kv[...] = key_value(shared)
    halo_send[...] = key_value(shared_sib)
    to_right = remote(halo_send.at[pl.ds(row_count - WINDOW, WINDOW)], low_kv,
                      halo_send_sem.at[0], halo_recv_sem.at[0], lax.rem(me + 1, n_ep), sibling)
    to_left = remote(halo_send.at[pl.ds(0, WINDOW)], high_kv,
                     halo_send_sem.at[1], halo_recv_sem.at[1], lax.rem(me + n_ep - 1, n_ep), sibling)

    far_onehot = jnp.concatenate([slot_onehot(k) for k in far], axis=0).astype(bf16)
    close_onehot = jnp.concatenate([slot_onehot(k) for k in close], axis=0).astype(bf16)

    loads[2].wait()
    loads[3].wait()
    normed_v[...] = layer_norm(input_v[...], gain_v[...])

    def columns_of(owner, size):
        return pl.ds(pl.multiple_of(owner * size, size), size)

    own_slice = normed_v[:, columns_of(my_tp, slice_width)]
    slots = jnp.dot(far_onehot, own_slice, preferred_element_type=f32)
    for place, k in enumerate(far):
        packed[0, k] = pack(slots[place * cap : (place + 1) * cap]).astype(bf16)

    pl.semaphore_wait(barrier, n_ep + n_tp - 2)

    def net(k, q):
        owner = 2 * pair_up[q] + core
        return remote(packed.at[q, k], rows_in.at[owner, k],
                      send_sem.at[0 if k >= half_count else 1], net_recv_sem.at[k], experts_of[k], sibling)

    @pl.when(me < n_ep - 1)
    def _():
        to_right.start()

    @pl.when(me > 0)
    def _():
        to_left.start()

    @pl.when(me == 0)
    def _():
        low_kv[...] = jnp.zeros_like(low_kv)

    @pl.when(me == n_ep - 1)
    def _():
        high_kv[...] = jnp.zeros_like(high_kv)

    for k in far:
        start(net(k, 0))

    for q in range(n_pair):
        for side in range(2):
            owner = 2 * pair_up[q] + (core if side == 0 else 1 - core)
            rows = close_onehot if side == 0 else close_onehot[:cap]
            slots = jnp.dot(rows, normed_v[:, columns_of(owner, slice_width)], preferred_element_type=f32)
            rows_in[owner, 0] = pack(slots[:cap]).astype(bf16)
            if side == 0:
                for place, k in enumerate(close[1:]):
                    place = (place + 1) * cap
                    packed[q, k] = pack(slots[place : place + cap]).astype(bf16)
        for k in close[1:]:
            start(net(k, q))

    loads[12].wait()
    loads[7].wait()
    query = [
        turn(query_v[:, pl.ds(column, LANES)]) for column in range(0, query_v.shape[1], LANES)
    ]
    span = row_count + 2 * WINDOW
    local = lax.broadcasted_iota(jnp.int32, (row_count, span), 0)
    other = lax.broadcasted_iota(jnp.int32, (row_count, span), 1) - WINDOW
    position = me * row_count + other
    allowed = (
        (jnp.abs(local - other) <= WINDOW) & (position >= 0) & (position < row_count * n_ep)
    )

    @pl.when(me > 0)
    def _():
        to_right.wait_recv()

    @pl.when(me < n_ep - 1)
    def _():
        to_left.wait_recv()

    both = jnp.concatenate([low_kv[...], own_kv[...], high_kv[...]], axis=0).astype(f32)
    both_roll = pltpu.roll(both, head_dim, 1)
    low_span = lax.broadcasted_iota(jnp.int32, (span, LANES), 1) < head_dim
    keys = jnp.where(low_span, both, both_roll).astype(bf16)
    values = jnp.where(low_span, both_roll, both).astype(bf16)
    blocks = []
    for head in range(local_heads):
        mine = low_lane if head % 2 == 0 else jnp.logical_not(low_lane)
        head_query = jnp.where(mine, query[head // 2], 0.0).astype(bf16)
        scores = lax.dot_general(
            head_query, keys, (((1,), (1,)), ((), ())), preferred_element_type=f32
        ) * head_dim ** (-0.5)
        scores = jnp.where(allowed, scores, MASK_VALUE)
        sink = sink_v[:, head : head + 1]
        largest = jnp.maximum(jnp.max(scores, axis=-1, keepdims=True), sink)
        weights = jnp.exp(scores - largest)
        denominator = jnp.sum(weights, axis=-1, keepdims=True) + jnp.exp(sink - largest)
        probability = (weights * (1.0 / denominator)).astype(bf16)
        result = jnp.dot(probability, values, preferred_element_type=f32)
        if head % 2 == 0:
            blocks.append(result)
        else:
            blocks[-1] = jnp.where(low_lane, blocks[-1], result)
    attended = jnp.concatenate(blocks, axis=1).astype(bf16)[:, : local_heads * head_dim]
    loads[8].wait()
    partial_sum = jnp.dot(attended, out_w[...], preferred_element_type=f32)
    mix_send[...] = partial_sum.reshape(mix_send.shape).astype(bf16)

    def mix_own(p):
        return 2 * pair_up[p] + (core if p == 0 else 1 - core)

    def mix_other(p):
        return 2 * pair_up[p] + (1 - core if p == 0 else core)

    mix_pairs = [
        remote(mix_send.at[mix_other(p)], mix_sib.at[p],
               send_sem.at[4], mix_sib_recv_sem.at[p], me, sibling)
        for p in range(n_pair)
    ]
    for p in list(range(1, n_pair)) + [0]:
        start(mix_pairs[p])

    loads[1].wait()
    blocked = halves * cap
    number = lax.broadcasted_iota(jnp.int32, (blocked, row_count), 0)
    slot_of = number
    left = number >= 0
    if tail:
        in_main = number < 2 * main
        slot_of = jnp.where(
            in_main,
            jnp.where(number < main, number, number - main),
            jnp.where(number < 2 * main + tail, number - main, number - main - tail),
        )
        left = (number < main) | (jnp.logical_not(in_main) & (number < 2 * main + tail))
    for k in range(n_ep):
        placed = jnp.zeros((blocked, row_count), f32)
        for j in range(TOP):
            chosen = jnp.where(routes[j] == experts_of[k], rank[j], -1) == slot_of
            placed = jnp.where(chosen, route_weight_v[j : j + 1, :], placed)
        combine_left[pl.ds(k * blocked, blocked)] = jnp.where(left, placed, 0.0).astype(bf16)
        if tail:
            combine_right[pl.ds(k * blocked, blocked)] = jnp.where(left, 0.0, placed).astype(bf16)

    def group_of(k):
        return [number for number, group in enumerate(groups) if k in group][0]

    def near_forward(k, q):
        owner = 2 * pair_up[q] + 1 - core
        return remote(rows_in.at[owner, k], rows_in.at[owner, k],
                      send_sem.at[2], near_recv_sem.at[group_of(k)], me, sibling)

    def far_forward(k, p):
        owner = 2 * pair + 1 - core
        return remote(rows_in.at[owner, k], rows_in.at[owner, k],
                      send_sem.at[3], far_recv_sem.at[p, k - half_count], me, 2 * pair_up[p] + 1 - core)

    def far_relay(k, p):
        owner = 2 * pair_down[p] + core
        return remote(rows_in.at[owner, k], rows_in.at[owner, k],
                      send_sem.at[2], near_recv_sem.at[group_of(k)], me, sibling)

    def forward(group):
        for k in group:
            if k == 0:
                continue
            if k >= half_count:
                net(k, 0).wait_recv()
                for p in range(1, n_pair):
                    start(far_forward(k, p))
                start(near_forward(k, 0))
                continue
            arrived(rows_in.at[pl.ds(0, n_pair), k], net_recv_sem.at[k])
            for q in range(n_pair):
                start(near_forward(k, q))

    def relay(group):
        for k in group:
            if k < half_count:
                continue
            for p in range(1, n_pair):
                far_forward(k, p).wait_recv()
                start(far_relay(k, p))

    def gather(group):
        count = len(group) - (0 in group)
        arrived(rows_in.at[pl.ds(0, n_pair), pl.ds(0, count)], near_recv_sem.at[group_of(group[0])])
        for owner in range(n_tp):
            for half in range(halves):
                columns = pl.ds(owner * slice_width + half * piece, piece)
                for place, k in enumerate(group):
                    gathered[pl.ds(place * main, main), columns] = (
                        rows_in[owner, k, pl.ds(half * main, main), :]
                    )
                if tail:
                    ends = [
                        rows_in[owner, k, pl.ds(2 * main, 2 * tail), :].astype(f32)[
                            half * tail : (half + 1) * tail
                        ]
                        for k in group
                    ]
                    gathered[pl.ds(len(group) * main, len(group) * tail), columns] = (
                        jnp.concatenate(ends, axis=0).astype(bf16)
                    )

    hidden_width = gate_w.shape[1]
    tile = min(hidden_width, 512)

    def expand(group):
        rows = len(group) * cap

        for number in range(hidden_width // tile):
            columns = pl.ds(number * tile, tile)
            gate_act = jnp.dot(gathered[:rows], gate_w[:, columns], preferred_element_type=f32)
            up_act = jnp.dot(gathered[:rows], up_w[:, columns], preferred_element_type=f32)
            hidden[:rows, columns] = (gate_act / (1.0 + jnp.exp(-gate_act)) * up_act).astype(bf16)

    def down_slice(group, owner):
        rows = len(group) * cap
        result = jnp.dot(
            hidden[:rows], down_w[:, columns_of(owner, slice_width)], preferred_element_type=f32
        )
        count = len(group)
        for place, k in enumerate(group):
            values = result[place * main : (place + 1) * main]
            if tail:
                last = count * main + place * tail
                values = jnp.concatenate([values, result[last : last + tail]], axis=0)
            yield k, pack(values)

    def batches(group):
        return [group[0] + start for start in range(0, len(group), 2)]

    def sib_copy(k, p):
        both = pl.ds(k, 2)
        return remote(sib_send.at[p, both], sib_recv.at[p, both],
                      send_sem.at[5], sib_recv_sem.at[p, k // 2], me, sibling)

    def cross_copy(k, p):
        both = pl.ds(k, 2)
        return remote(cross_send.at[p, both], cross_recv.at[p, both],
                      send_sem.at[6], cross_recv_sem.at[p, k // 2], me, 2 * pair_up[p] + 1 - core)

    def return_copy(k):
        return remote(final_send.at[k], returned.at[k],
                      send_sem.at[7], final_recv_sem.at[0], experts_of[k], sibling)

    def contract(group):
        for p in list(range(1, n_pair)) + [0]:
            given = 2 * pair_up[p] + (core if p == 0 else 1 - core)
            kept = 2 * pair_up[p] + (1 - core if p == 0 else core)
            for k, values in down_slice(group, given):
                sib_send[p, k] = values.astype(bf16)
            for k in batches(group):
                start(sib_copy(k, p))
            for k, values in down_slice(group, kept):
                own_acc[p, k] = values

    def cross(group):
        for first in batches(group):
            for p in range(1, n_pair):
                sib_copy(first, p).wait_recv()
                for k in (first, first + 1):
                    cross_send[p, k] = (own_acc[p, k] + sib_recv[p, k].astype(f32)).astype(bf16)
                start(cross_copy(first, p))

    def finish(group):
        for first in batches(group):
            sib_copy(first, 0).wait_recv()
            for p in range(1, n_pair):
                cross_copy(first, p).wait_recv()
            for k in (first, first + 1):
                total = own_acc[0, k] + sib_recv[0, k].astype(f32)
                for p in range(1, n_pair):
                    total += cross_recv[p, k].astype(f32)
                final_send[k] = total.astype(bf16)
                start(return_copy(k))

    def mix_forward():
        for p in range(1, n_pair):
            mix_pairs[p].wait_recv()
            mix_cross[p] = (
                mix_send[mix_own(p)].astype(f32) + mix_sib[p].astype(f32)
            ).astype(bf16)
            start(mix_copy(p))

    def mix_copy(p):
        return remote(mix_cross.at[p], mix_recv.at[p],
                      send_sem.at[8], mix_recv_sem.at[p], me, 2 * pair_up[p] + 1 - core)

    def mix_finish():
        mix_pairs[0].wait_recv()
        mixed = mix_send[mix_own(0)].astype(f32) + mix_sib[0].astype(f32)
        for p in range(1, n_pair):
            mix_copy(p).wait_recv()
            mixed += mix_recv[p].astype(f32)
        mixer_ref[...] = mixed.astype(mixer_ref.dtype)

    first, second, last = groups
    forward(first)
    forward(second)
    mix_forward()
    relay(first)
    forward(last)
    loads[9].wait()
    loads[10].wait()
    gather(first)
    expand(first)
    relay(second)
    loads[11].wait()
    contract(first)
    gather(second)
    cross(first)
    expand(second)
    contract(second)
    gather(last)
    cross(second)
    expand(last)
    finish(first)
    contract(last)
    finish(second)
    cross(last)
    mix_finish()
    finish(last)

    arrived(returned, final_recv_sem.at[0])
    blocks = returned[...].reshape(n_ep * blocked, piece)

    def combined(weights_ref):
        return lax.dot_general(
            weights_ref[...], blocks, (((0,), (0,)), ((), ())), preferred_element_type=f32
        )

    expert_ref[:, :piece] = combined(combine_left).astype(expert_ref.dtype)
    if tail:
        expert_ref[:, piece:] = combined(combine_right).astype(expert_ref.dtype)

    @pl.when(me < n_ep - 1)
    def _():
        to_right.wait_send()

    @pl.when(me > 0)
    def _():
        to_left.wait_send()

    far_count = n_ep - half_count
    arrived(packed.at[0, pl.ds(0, far_count)], send_sem.at[0])
    arrived(packed.at[:, pl.ds(0, half_count - 1)], send_sem.at[1])
    arrived(rows_in.at[pl.ds(0, n_pair), pl.ds(0, n_ep - 1)], send_sem.at[2])
    if n_pair > 1:
        arrived(rows_in.at[pl.ds(0, n_pair - 1), pl.ds(0, far_count)], send_sem.at[3])
    arrived(mix_sib, send_sem.at[4])
    if n_pair > 1:
        arrived(mix_cross.at[pl.ds(0, n_pair - 1)], send_sem.at[8])
    arrived(sib_send, send_sem.at[5])
    if n_pair > 1:
        arrived(cross_send.at[pl.ds(0, n_pair - 1)], send_sem.at[6])
    arrived(final_send, send_sem.at[7])


def on_device(
    queries,
    key_states,
    value_states,
    sink_logit,
    out_weight,
    expert_input,
    norm_gain,
    routes,
    route_weight,
    gate_weight,
    up_weight,
    down_weight,
):
    n_ep = lax.axis_size("ep")
    n_tp = lax.axis_size("tp")
    row_count, width = expert_input.shape
    local_heads = queries.shape[1] // HEAD_DIM
    capacity = row_count * TOP * 5 // (4 * n_ep)
    main, tail = capacity // 16 * 16, 0
    if 0 < capacity - main <= 8 and width // n_tp >= 2 * LANES and main:
        tail = 8
    elif capacity > main:
        main += 16
    halves = 2 if tail else 1
    slice_width = width // n_tp
    piece = slice_width // halves
    blocked = halves * (main + tail)
    hidden_width = gate_weight.shape[2]
    mix_rows = row_count // n_tp
    n_pair = n_tp // 2
    group_rows = n_ep // 2 * (main + tail)
    if queries.shape[1] % LANES:
        queries = jnp.pad(queries, ((0, 0), (0, LANES - queries.shape[1] % LANES)))
    table = jnp.asarray(angle_table(row_count, n_ep))
    vmem = pl.BlockSpec(memory_space=pltpu.VMEM)
    hbm = pl.BlockSpec(memory_space=pltpu.HBM)
    bf16, f32 = jnp.bfloat16, jnp.float32
    dma = pltpu.SemaphoreType.DMA
    traveling = (blocked, piece)
    mixer_out, expert_out = pl.pallas_call(
        functools.partial(fused_kernel, (n_ep, n_tp, main, tail)),
        out_shape=(
            jax.ShapeDtypeStruct((mix_rows, width), bf16),
            jax.ShapeDtypeStruct((row_count, slice_width), bf16),
        ),
        in_specs=[hbm] * 13,
        out_specs=(vmem, vmem),
        scratch_shapes=[
            pltpu.VMEM(queries.shape, bf16),
            pltpu.VMEM((row_count, LANES), bf16),
            pltpu.VMEM((row_count, LANES), bf16),
            pltpu.VMEM(table.shape, f32),
            pltpu.VMEM((1, local_heads), f32),
            pltpu.VMEM(expert_input.shape, bf16),
            pltpu.VMEM((1, width), f32),
            pltpu.VMEM((TOP, row_count), jnp.int32),
            pltpu.VMEM((TOP, row_count), f32),
            pltpu.VMEM(out_weight.shape, bf16),
            pltpu.VMEM(gate_weight.shape[1:], bf16),
            pltpu.VMEM(up_weight.shape[1:], bf16),
            pltpu.VMEM(down_weight.shape[1:], bf16),
            pltpu.VMEM(expert_input.shape, bf16),
            pltpu.VMEM((row_count, LANES), bf16),
            pltpu.VMEM((row_count, LANES), bf16),
            pltpu.VMEM((WINDOW, LANES), bf16),
            pltpu.VMEM((WINDOW, LANES), bf16),
            pltpu.VMEM((n_pair, n_ep) + traveling, bf16),
            pltpu.VMEM((n_tp, n_ep) + traveling, bf16),
            pltpu.VMEM((group_rows, width), bf16),
            pltpu.VMEM((group_rows, hidden_width), bf16),
            pltpu.VMEM((n_tp, mix_rows, width), bf16),
            pltpu.VMEM((n_pair, mix_rows, width), bf16),
            pltpu.VMEM((n_pair, mix_rows, width), bf16),
            pltpu.VMEM((n_pair, mix_rows, width), bf16),
            pltpu.VMEM((n_pair, n_ep) + traveling, bf16),
            pltpu.VMEM((n_pair, n_ep) + traveling, bf16),
            pltpu.VMEM((n_pair, n_ep) + traveling, f32),
            pltpu.VMEM((n_pair, n_ep) + traveling, bf16),
            pltpu.VMEM((n_pair, n_ep) + traveling, bf16),
            pltpu.VMEM((n_ep,) + traveling, bf16),
            pltpu.VMEM((n_ep,) + traveling, bf16),
            pltpu.VMEM((n_ep * blocked, row_count), bf16),
            pltpu.VMEM((n_ep * blocked, row_count), bf16),
            dma((13,)),
            dma((2,)),
            dma((2,)),
            dma((9,)),
            dma((n_ep,)),
            dma((n_pair, n_ep // 2)),
            dma((3,)),
            dma((n_pair,)),
            dma((n_pair,)),
            dma((n_pair, n_ep // 2)),
            dma((n_pair, n_ep // 2)),
            dma((1,)),
        ],
        compiler_params=pltpu.CompilerParams(
            collective_id=0, has_side_effects=True, vmem_limit_bytes=60 * 1024 * 1024
        ),
    )(
        queries,
        key_states,
        value_states,
        table,
        sink_logit[None, :],
        expert_input,
        norm_gain[None, :],
        routes.T,
        route_weight.T,
        out_weight,
        gate_weight,
        up_weight,
        down_weight,
    )
    return mixer_out, expert_out


def solution(mesh):
    in_specs = (
        P("ep", "tp"),
        P("ep", None),
        P("ep", None),
        P("tp"),
        P("tp", None),
        P("ep", None),
        P(),
        P("ep", None),
        P("ep", None),
        P("ep", None, "tp"),
        P("ep", None, "tp"),
        P("ep", "tp", None),
    )
    out_specs = (P(("ep", "tp"), None), P("ep", "tp"))
    return jax.shard_map(
        on_device, mesh=mesh, in_specs=in_specs, out_specs=out_specs, check_vma=False
    )
```

```python
import functools

import jax
import jax.numpy as jnp
import numpy as np
from jax import lax
from jax.experimental import pallas as pl
from jax.experimental.pallas import tpu as pltpu
from jax.sharding import PartitionSpec as P

HEADS = 16
KV_HEADS = 4
HEAD_DIM = 64
WINDOW = 128
TOP = 2
LANES = 128


NORM_EPSILON = 1e-05
ROTARY_BASE = 500000.0
MASK_VALUE = -1e30


def layer_norm(activations, norm_gain):
    values = activations.astype(jnp.float32)
    average = jnp.mean(values, axis=-1, keepdims=True)
    centred = values - average
    variance = jnp.mean(centred * centred, axis=-1, keepdims=True)
    return (centred * lax.rsqrt(variance + NORM_EPSILON) * norm_gain).astype(jnp.bfloat16)


def angle_table(row_count, blocks):
    lane = np.arange(LANES) % HEAD_DIM
    half_dim = HEAD_DIM // 2
    frequency = ROTARY_BASE ** (-2.0 * (lane % half_dim) / HEAD_DIM)
    sign = np.where(lane < half_dim, -1.0, 1.0)
    rows = np.arange(row_count)[:, None] * frequency[None, :]
    bases = np.arange(blocks)[:, None] * row_count * frequency[None, :]
    return np.concatenate(
        [np.cos(rows), sign * np.sin(rows), np.cos(bases), sign * np.sin(bases)]
    ).astype(np.float32)


def partner(index, mask):
    flipped, bit = index, 1
    while bit <= mask:
        if mask & bit:
            flipped = flipped + bit * (1 - 2 * lax.rem(index // bit, 2))
        bit *= 2
    return flipped


def fused_kernel(
    sizes,
    query_hbm,
    key_hbm,
    value_hbm,
    table_hbm,
    sink_hbm,
    input_hbm,
    gain_hbm,
    routes_hbm,
    route_weight_hbm,
    out_hbm,
    gate_hbm,
    up_hbm,
    down_hbm,
    mixer_ref,
    expert_ref,
    query_v,
    key_v,
    value_v,
    table_v,
    sink_v,
    input_v,
    gain_v,
    routes_v,
    route_weight_v,
    out_w,
    gate_w,
    up_w,
    down_w,
    normed_v,
    own_kv,
    halo_send,
    low_kv,
    high_kv,
    packed,
    rows_in,
    gathered,
    hidden,
    mix_send,
    mix_sib,
    mix_cross,
    mix_recv,
    sib_send,
    sib_recv,
    own_acc,
    cross_send,
    cross_recv,
    final_send,
    returned,
    combine_left,
    combine_right,
    load_sem,
    halo_send_sem,
    halo_recv_sem,
    send_sem,
    net_recv_sem,
    far_recv_sem,
    near_recv_sem,
    mix_sib_recv_sem,
    mix_recv_sem,
    sib_recv_sem,
    cross_recv_sem,
    final_recv_sem,
):
    n_ep, n_tp, main, tail = sizes
    cap = main + tail
    halves = 2 if tail else 1
    f32, bf16 = jnp.float32, jnp.bfloat16
    me, my_tp = lax.axis_index("ep"), lax.axis_index("tp")
    core = lax.rem(my_tp, 2)
    pair = my_tp // 2
    n_pair = n_tp // 2
    sibling = my_tp + 1 - 2 * core
    row_count, width = input_v.shape
    slice_width = width // n_tp
    piece = slice_width // halves
    head_dim = HEAD_DIM
    local_heads = sink_v.shape[1]
    half_count = n_ep // 2
    quarter = n_ep // 4
    experts_of = [partner(me, k) for k in range(n_ep)]
    middle = lax.rem(me // half_count + me // quarter, 2)
    bases = [half_count + quarter * (1 - middle), half_count + quarter * middle]
    far_experts = [
        [
            experts_of[half_count + quarter * place + i]
            + middle * (experts_of[half_count + quarter * (1 - place) + i]
                        - experts_of[half_count + quarter * place + i])
            for i in range(quarter)
        ]
        for place in (1, 0)
    ]
    far_batches = [(bases[place], far_experts[place]) for place in range(2)]
    near_batches = [
        (0, experts_of[:quarter]),
        (quarter, experts_of[quarter:half_count]),
    ]
    groups = [(far_batches[place], near_batches[place]) for place in range(2)]
    pair_up = [lax.rem(pair + p, n_pair) for p in range(n_pair)]
    pair_down = [lax.rem(pair + n_pair - p, n_pair) for p in range(n_pair)]

    names = [
        (routes_hbm, routes_v),
        (route_weight_hbm, route_weight_v),
        (gain_hbm, gain_v),
        (input_hbm, input_v),
        (table_hbm, table_v),
        (key_hbm, key_v),
        (value_hbm, value_v),
        (query_hbm, query_v),
        (out_hbm, out_w),
        (gate_hbm.at[0], gate_w),
        (up_hbm.at[0], up_w),
        (down_hbm.at[0], down_w),
        (sink_hbm, sink_v),
    ]
    shared = my_tp * local_heads // (HEADS // KV_HEADS)
    shared_sib = sibling * local_heads // (HEADS // KV_HEADS)
    block = pl.ds(pl.multiple_of(shared // 2 * LANES, LANES), LANES)
    names[5] = (key_hbm.at[:, block], key_v)
    names[6] = (value_hbm.at[:, block], value_v)
    loads = [
        pltpu.make_async_copy(source, target, load_sem.at[number])
        for number, (source, target) in enumerate(names)
    ]

    def remote(source, target, send_sem, recv_sem, ep, tp):
        return pltpu.make_async_remote_copy(
            src_ref=source,
            dst_ref=target,
            send_sem=send_sem,
            recv_sem=recv_sem,
            device_id=(ep, tp),
            device_id_type=pl.DeviceIdType.MESH,
        )

    barrier = pltpu.get_barrier_semaphore()
    for k in range(n_ep - 1, 0, -1):
        pl.semaphore_signal(
            barrier, inc=1, device_id=(experts_of[k], sibling),
            device_id_type=pl.DeviceIdType.MESH,
        )
    for step in range(1, n_tp):
        pl.semaphore_signal(
            barrier, inc=1, device_id=(me, lax.rem(my_tp + step, n_tp)),
            device_id_type=pl.DeviceIdType.MESH,
        )
    for load in loads:
        load.start()

    def start(copy):
        copy.start()

    def arrived(target, sem):
        pltpu.make_async_copy(target, target, sem).wait()

    loads[0].wait()
    routes = [routes_v[k : k + 1, :] for k in range(TOP)]
    expert_iota = lax.broadcasted_iota(jnp.int32, (n_ep, row_count), 0)
    named = [(routes[k] == expert_iota).astype(f32) for k in range(TOP)]
    earlier = (
        lax.broadcasted_iota(jnp.int32, (row_count, row_count), 0)
        < lax.broadcasted_iota(jnp.int32, (row_count, row_count), 1)
    )
    ahead = jnp.dot(
        functools.reduce(jnp.add, named).astype(bf16),
        earlier.astype(f32).astype(bf16),
        preferred_element_type=f32,
    )
    rank = [
        jnp.sum(ahead * named[k], axis=0, keepdims=True).astype(jnp.int32) for k in range(TOP)
    ]

    def slot_onehot(k):
        slot = lax.broadcasted_iota(jnp.int32, (cap, row_count), 0)
        chosen = [(jnp.where(routes[j] == experts_of[k], rank[j], -1) == slot) for j in range(TOP)]
        return functools.reduce(jnp.logical_or, chosen).astype(f32)

    def pack(values):
        if not tail:
            return values
        parts = [values[:main, :piece], values[:main, piece:], values[main:, :piece], values[main:, piece:]]
        return jnp.concatenate(parts, axis=0)

    far = list(range(half_count, n_ep))
    close = list(range(half_count))
    for number in range(4, 7):
        loads[number].wait()
    lane = lax.broadcasted_iota(jnp.int32, (row_count, LANES), 1)
    low_lane = lane < head_dim
    first_half = lax.rem(lane, head_dim) < head_dim // 2
    row_cos, row_sin = table_v[:row_count], table_v[row_count : 2 * row_count]
    base_cos = table_v[pl.ds(2 * row_count + me, 1), :]
    base_sin = table_v[pl.ds(2 * row_count + n_ep + me, 1), :]
    cosine = base_cos * row_cos - base_sin * row_sin
    sine = base_sin * row_cos + base_cos * row_sin

    def turn(values):
        values = values.astype(f32)
        other = jnp.where(
            first_half,
            pltpu.roll(values, LANES - head_dim // 2, 1),
            pltpu.roll(values, head_dim // 2, 1),
        )
        return values * cosine + other * sine

    turned = turn(key_v[...])
    value = value_v[...].astype(f32)
    turned_roll, value_roll = pltpu.roll(turned, head_dim, 1), pltpu.roll(value, head_dim, 1)

    def key_value(head):
        upper = lax.rem(head, 2) == 1
        return jnp.where(
            low_lane,
            jnp.where(upper, turned_roll, turned),
            jnp.where(upper, value, value_roll),
        ).astype(bf16)

    own_kv[...] = key_value(shared)
    halo_send[...] = key_value(shared_sib)
    to_right = remote(halo_send.at[pl.ds(row_count - WINDOW, WINDOW)], low_kv,
                      halo_send_sem.at[0], halo_recv_sem.at[0], lax.rem(me + 1, n_ep), sibling)
    to_left = remote(halo_send.at[pl.ds(0, WINDOW)], high_kv,
                     halo_send_sem.at[1], halo_recv_sem.at[1], lax.rem(me + n_ep - 1, n_ep), sibling)

    far_onehot = jnp.concatenate([slot_onehot(k) for k in far], axis=0).astype(bf16)
    close_onehot = jnp.concatenate([slot_onehot(k) for k in close], axis=0).astype(bf16)

    loads[2].wait()
    loads[3].wait()
    normed_v[...] = layer_norm(input_v[...], gain_v[...])

    def columns_of(owner, size):
        return pl.ds(pl.multiple_of(owner * size, size), size)

    own_slice = normed_v[:, columns_of(my_tp, slice_width)]
    slots = jnp.dot(far_onehot, own_slice, preferred_element_type=f32)
    for place, k in enumerate(far):
        packed[0, k] = pack(slots[place * cap : (place + 1) * cap]).astype(bf16)

    pl.semaphore_wait(barrier, n_ep + n_tp - 2)

    def net(k, expert, q, sem):
        owner = 2 * pair_up[q] + core
        return remote(packed.at[q, k], rows_in.at[owner, k],
                      send_sem.at[sem], net_recv_sem.at[k], expert, sibling)

    @pl.when(me < n_ep - 1)
    def _():
        to_right.start()

    @pl.when(me > 0)
    def _():
        to_left.start()

    @pl.when(me == 0)
    def _():
        low_kv[...] = jnp.zeros_like(low_kv)

    @pl.when(me == n_ep - 1)
    def _():
        high_kv[...] = jnp.zeros_like(high_kv)

    for base, experts in far_batches:
        for i, expert in enumerate(experts):
            start(net(base + i, expert, 0, 0))

    for q in range(n_pair):
        for side in range(2):
            owner = 2 * pair_up[q] + (core if side == 0 else 1 - core)
            rows = close_onehot if side == 0 else close_onehot[:cap]
            slots = jnp.dot(rows, normed_v[:, columns_of(owner, slice_width)], preferred_element_type=f32)
            rows_in[owner, 0] = pack(slots[:cap]).astype(bf16)
            if side == 0:
                for place, k in enumerate(close[1:]):
                    place = (place + 1) * cap
                    packed[q, k] = pack(slots[place : place + cap]).astype(bf16)

    for k in close[1:]:
        for q in range(n_pair):
            start(net(k, experts_of[k], q, 1))

    loads[12].wait()
    loads[7].wait()
    query = [
        turn(query_v[:, pl.ds(column, LANES)]) for column in range(0, query_v.shape[1], LANES)
    ]
    span = row_count + 2 * WINDOW
    local = lax.broadcasted_iota(jnp.int32, (row_count, span), 0)
    other = lax.broadcasted_iota(jnp.int32, (row_count, span), 1) - WINDOW
    position = me * row_count + other
    allowed = (
        (jnp.abs(local - other) <= WINDOW) & (position >= 0) & (position < row_count * n_ep)
    )

    @pl.when(me > 0)
    def _():
        to_right.wait_recv()

    @pl.when(me < n_ep - 1)
    def _():
        to_left.wait_recv()

    both = jnp.concatenate([low_kv[...], own_kv[...], high_kv[...]], axis=0).astype(f32)
    both_roll = pltpu.roll(both, head_dim, 1)
    low_span = lax.broadcasted_iota(jnp.int32, (span, LANES), 1) < head_dim
    keys = jnp.where(low_span, both, both_roll).astype(bf16)
    values = jnp.where(low_span, both_roll, both).astype(bf16)
    blocks = []
    for head in range(local_heads):
        mine = low_lane if head % 2 == 0 else jnp.logical_not(low_lane)
        head_query = jnp.where(mine, query[head // 2], 0.0).astype(bf16)
        scores = lax.dot_general(
            head_query, keys, (((1,), (1,)), ((), ())), preferred_element_type=f32
        ) * head_dim ** (-0.5)
        scores = jnp.where(allowed, scores, MASK_VALUE)
        sink = sink_v[:, head : head + 1]
        largest = jnp.maximum(jnp.max(scores, axis=-1, keepdims=True), sink)
        weights = jnp.exp(scores - largest)
        denominator = jnp.sum(weights, axis=-1, keepdims=True) + jnp.exp(sink - largest)
        probability = (weights * (1.0 / denominator)).astype(bf16)
        result = jnp.dot(probability, values, preferred_element_type=f32)
        if head % 2 == 0:
            blocks.append(result)
        else:
            blocks[-1] = jnp.where(low_lane, blocks[-1], result)
    attended = jnp.concatenate(blocks, axis=1).astype(bf16)[:, : local_heads * head_dim]
    loads[8].wait()
    partial_sum = jnp.dot(attended, out_w[...], preferred_element_type=f32)
    mix_send[...] = partial_sum.reshape(mix_send.shape).astype(bf16)

    def mix_own(p):
        return 2 * pair_up[p] + (core if p == 0 else 1 - core)

    def mix_other(p):
        return 2 * pair_up[p] + (1 - core if p == 0 else core)

    mix_pairs = [
        remote(mix_send.at[mix_other(p)], mix_sib.at[p],
               send_sem.at[4], mix_sib_recv_sem.at[p], me, sibling)
        for p in range(n_pair)
    ]
    for p in list(range(1, n_pair)) + [0]:
        start(mix_pairs[p])

    loads[1].wait()
    blocked = halves * cap
    number = lax.broadcasted_iota(jnp.int32, (blocked, row_count), 0)
    slot_of = number
    left = number >= 0
    if tail:
        in_main = number < 2 * main
        slot_of = jnp.where(
            in_main,
            jnp.where(number < main, number, number - main),
            jnp.where(number < 2 * main + tail, number - main, number - main - tail),
        )
        left = (number < main) | (jnp.logical_not(in_main) & (number < 2 * main + tail))
    for k in range(n_ep):
        placed = jnp.zeros((blocked, row_count), f32)
        for j in range(TOP):
            chosen = jnp.where(routes[j] == experts_of[k], rank[j], -1) == slot_of
            placed = jnp.where(chosen, route_weight_v[j : j + 1, :], placed)
        combine_left[pl.ds(k * blocked, blocked)] = jnp.where(left, placed, 0.0).astype(bf16)
        if tail:
            combine_right[pl.ds(k * blocked, blocked)] = jnp.where(left, 0.0, placed).astype(bf16)

    def near_forward(k, q, sem):
        owner = 2 * pair_up[q] + 1 - core
        return remote(rows_in.at[owner, k], rows_in.at[owner, k],
                      send_sem.at[2], near_recv_sem.at[sem], me, sibling)

    def far_forward(k, p):
        owner = 2 * pair + 1 - core
        return remote(rows_in.at[owner, k], rows_in.at[owner, k],
                      send_sem.at[3], far_recv_sem.at[p, k - half_count], me, 2 * pair_up[p] + 1 - core)

    def far_relay(k, p, sem):
        owner = 2 * pair_down[p] + core
        return remote(rows_in.at[owner, k], rows_in.at[owner, k],
                      send_sem.at[2], near_recv_sem.at[sem], me, sibling)

    def forward_far(number):
        base, experts = far_batches[number]
        for i, expert in enumerate(experts):
            net(base + i, expert, 0, 0).wait_recv()
            for p in range(1, n_pair):
                start(far_forward(base + i, p))
            start(near_forward(base + i, 0, number))

    def relay_far(number):
        base, experts = far_batches[number]
        for i in range(len(experts)):
            for p in range(1, n_pair):
                far_forward(base + i, p).wait_recv()
                start(far_relay(base + i, p, number))

    def forward_near(number):
        base, experts = near_batches[number]
        for k in range(max(base, 1), base + len(experts)):
            arrived(rows_in.at[pl.ds(0, n_pair), k], net_recv_sem.at[k])
            for q in range(n_pair):
                start(near_forward(k, q, 2 + number))

    def gather(number):
        slots = []
        for kind, (base, experts) in enumerate(groups[number]):
            count = len(experts)
            slots += [base + i for i in range(count)]
            if kind == 1 and number == 0:
                count -= 1
            arrived(rows_in.at[pl.ds(0, n_pair), pl.ds(0, count)], near_recv_sem.at[2 * kind + number])
        for owner in range(n_tp):
            for half in range(halves):
                columns = pl.ds(owner * slice_width + half * piece, piece)
                for place, k in enumerate(slots):
                    gathered[pl.ds(place * main, main), columns] = (
                        rows_in[owner, k, pl.ds(half * main, main), :]
                    )
                if tail:
                    ends = [
                        rows_in[owner, k, pl.ds(2 * main, 2 * tail), :].astype(f32)[
                            half * tail : (half + 1) * tail
                        ]
                        for k in slots
                    ]
                    gathered[pl.ds(len(slots) * main, len(slots) * tail), columns] = (
                        jnp.concatenate(ends, axis=0).astype(bf16)
                    )

    hidden_width = gate_w.shape[1]
    tile = min(hidden_width, 512)

    rows = half_count * cap

    def expand():
        for number in range(hidden_width // tile):
            columns = pl.ds(number * tile, tile)
            gate_act = jnp.dot(gathered[...], gate_w[:, columns], preferred_element_type=f32)
            up_act = jnp.dot(gathered[...], up_w[:, columns], preferred_element_type=f32)
            hidden[:, columns] = (gate_act / (1.0 + jnp.exp(-gate_act)) * up_act).astype(bf16)

    def down_slice(number, owner):
        result = jnp.dot(
            hidden[...], down_w[:, columns_of(owner, slice_width)], preferred_element_type=f32
        )
        slots = [base + i for base, experts in groups[number] for i in range(len(experts))]
        for place, k in enumerate(slots):
            values = result[place * main : (place + 1) * main]
            if tail:
                last = half_count * main + place * tail
                values = jnp.concatenate([values, result[last : last + tail]], axis=0)
            yield k, pack(values)

    def sib_copy(base, p):
        batch = pl.ds(base, quarter)
        return remote(sib_send.at[p, batch], sib_recv.at[p, batch],
                      send_sem.at[5], sib_recv_sem.at[p, base // quarter], me, sibling)

    def cross_copy(k, p):
        return remote(cross_send.at[p, k], cross_recv.at[p, k],
                      send_sem.at[6], cross_recv_sem.at[p - 1, k], me, 2 * pair_up[p] + 1 - core)

    def contract(number):
        for p in list(range(1, n_pair)) + [0]:
            given = 2 * pair_up[p] + (core if p == 0 else 1 - core)
            kept = 2 * pair_up[p] + (1 - core if p == 0 else core)
            for k, values in down_slice(number, given):
                sib_send[p, k] = values.astype(bf16)
            for base, _ in groups[number]:
                start(sib_copy(base, p))
            for k, values in down_slice(number, kept):
                own_acc[p, k] = values

    def cross(batch):
        base = batch[0]
        for p in range(1, n_pair):
            sib_copy(base, p).wait_recv()
            for i in range(quarter):
                k = base + i
                cross_send[p, k] = (own_acc[p, k] + sib_recv[p, k].astype(f32)).astype(bf16)
                start(cross_copy(k, p))

    def finish(batch):
        base, experts = batch
        sib_copy(base, 0).wait_recv()
        for i, expert in enumerate(experts):
            k = base + i
            total = own_acc[0, k] + sib_recv[0, k].astype(f32)
            for p in range(1, n_pair):
                cross_copy(k, p).wait_recv()
                total += cross_recv[p, k].astype(f32)
            final_send[k] = total.astype(bf16)
            start(remote(final_send.at[k], returned.at[k],
                         send_sem.at[7], final_recv_sem.at[0], expert, sibling))

    def mix_forward():
        for p in range(1, n_pair):
            mix_pairs[p].wait_recv()
            mix_cross[p] = (
                mix_send[mix_own(p)].astype(f32) + mix_sib[p].astype(f32)
            ).astype(bf16)
            start(mix_copy(p))

    def mix_copy(p):
        return remote(mix_cross.at[p], mix_recv.at[p],
                      send_sem.at[8], mix_recv_sem.at[p], me, 2 * pair_up[p] + 1 - core)

    def mix_finish():
        mix_pairs[0].wait_recv()
        mixed = mix_send[mix_own(0)].astype(f32) + mix_sib[0].astype(f32)
        for p in range(1, n_pair):
            mix_copy(p).wait_recv()
            mixed += mix_recv[p].astype(f32)
        mixer_ref[...] = mixed.astype(mixer_ref.dtype)

    forward_far(0)
    forward_near(0)
    forward_far(1)
    relay_far(0)
    mix_forward()
    loads[9].wait()
    loads[10].wait()
    gather(0)
    expand()
    relay_far(1)
    forward_near(1)
    loads[11].wait()
    contract(0)
    cross(far_batches[0])
    gather(1)
    cross(near_batches[0])
    expand()
    contract(1)
    cross(far_batches[1])
    finish(far_batches[0])
    cross(near_batches[1])
    finish(near_batches[0])
    finish(far_batches[1])
    mix_finish()
    finish(near_batches[1])

    arrived(returned, final_recv_sem.at[0])
    blocks = returned[...].reshape(n_ep * blocked, piece)

    def combined(weights_ref):
        return lax.dot_general(
            weights_ref[...], blocks, (((0,), (0,)), ((), ())), preferred_element_type=f32
        )

    expert_ref[:, :piece] = combined(combine_left).astype(expert_ref.dtype)
    if tail:
        expert_ref[:, piece:] = combined(combine_right).astype(expert_ref.dtype)

    @pl.when(me < n_ep - 1)
    def _():
        to_right.wait_send()

    @pl.when(me > 0)
    def _():
        to_left.wait_send()

    far_count = n_ep - half_count
    arrived(packed.at[0, pl.ds(0, far_count)], send_sem.at[0])
    arrived(packed.at[:, pl.ds(0, half_count - 1)], send_sem.at[1])
    arrived(rows_in.at[pl.ds(0, n_pair), pl.ds(0, n_ep - 1)], send_sem.at[2])
    if n_pair > 1:
        arrived(rows_in.at[pl.ds(0, n_pair - 1), pl.ds(0, far_count)], send_sem.at[3])
    arrived(mix_sib, send_sem.at[4])
    if n_pair > 1:
        arrived(mix_cross.at[pl.ds(0, n_pair - 1)], send_sem.at[8])
    arrived(sib_send, send_sem.at[5])
    if n_pair > 1:
        arrived(cross_send.at[pl.ds(0, n_pair - 1)], send_sem.at[6])
    arrived(final_send, send_sem.at[7])


def on_device(
    queries,
    key_states,
    value_states,
    sink_logit,
    out_weight,
    expert_input,
    norm_gain,
    routes,
    route_weight,
    gate_weight,
    up_weight,
    down_weight,
):
    n_ep = lax.axis_size("ep")
    n_tp = lax.axis_size("tp")
    row_count, width = expert_input.shape
    local_heads = queries.shape[1] // HEAD_DIM
    capacity = row_count * TOP * 5 // (4 * n_ep)
    main, tail = capacity // 16 * 16, 0
    if 0 < capacity - main <= 8 and width // n_tp >= 2 * LANES and main:
        tail = 8
    elif capacity > main:
        main += 16
    halves = 2 if tail else 1
    slice_width = width // n_tp
    piece = slice_width // halves
    blocked = halves * (main + tail)
    hidden_width = gate_weight.shape[2]
    mix_rows = row_count // n_tp
    n_pair = n_tp // 2
    group_rows = n_ep // 2 * (main + tail)
    if queries.shape[1] % LANES:
        queries = jnp.pad(queries, ((0, 0), (0, LANES - queries.shape[1] % LANES)))
    table = jnp.asarray(angle_table(row_count, n_ep))
    vmem = pl.BlockSpec(memory_space=pltpu.VMEM)
    hbm = pl.BlockSpec(memory_space=pltpu.HBM)
    bf16, f32 = jnp.bfloat16, jnp.float32
    dma = pltpu.SemaphoreType.DMA
    traveling = (blocked, piece)
    operands = (
        queries,
        key_states,
        value_states,
        table,
        sink_logit[None, :],
        expert_input,
        norm_gain[None, :],
        routes.T,
        route_weight.T,
        out_weight,
        gate_weight,
        up_weight,
        down_weight,
    )
    mixer_out, expert_out = pl.pallas_call(
        functools.partial(fused_kernel, (n_ep, n_tp, main, tail)),
        out_shape=(
            jax.ShapeDtypeStruct((mix_rows, width), bf16),
            jax.ShapeDtypeStruct((row_count, slice_width), bf16),
        ),
        in_specs=[hbm] * 13,
        out_specs=(vmem, vmem),
        scratch_shapes=[
            pltpu.VMEM(queries.shape, bf16),
            pltpu.VMEM((row_count, LANES), bf16),
            pltpu.VMEM((row_count, LANES), bf16),
            pltpu.VMEM(table.shape, f32),
            pltpu.VMEM((1, local_heads), f32),
            pltpu.VMEM(expert_input.shape, bf16),
            pltpu.VMEM((1, width), f32),
            pltpu.VMEM((TOP, row_count), jnp.int32),
            pltpu.VMEM((TOP, row_count), f32),
            pltpu.VMEM(out_weight.shape, bf16),
            pltpu.VMEM(gate_weight.shape[1:], bf16),
            pltpu.VMEM(up_weight.shape[1:], bf16),
            pltpu.VMEM(down_weight.shape[1:], bf16),
            pltpu.VMEM(expert_input.shape, bf16),
            pltpu.VMEM((row_count, LANES), bf16),
            pltpu.VMEM((row_count, LANES), bf16),
            pltpu.VMEM((WINDOW, LANES), bf16),
            pltpu.VMEM((WINDOW, LANES), bf16),
            pltpu.VMEM((n_pair, n_ep) + traveling, bf16),
            pltpu.VMEM((n_tp, n_ep) + traveling, bf16),
            pltpu.VMEM((group_rows, width), bf16),
            pltpu.VMEM((group_rows, hidden_width), bf16),
            pltpu.VMEM((n_tp, mix_rows, width), bf16),
            pltpu.VMEM((n_pair, mix_rows, width), bf16),
            pltpu.VMEM((n_pair, mix_rows, width), bf16),
            pltpu.VMEM((n_pair, mix_rows, width), bf16),
            pltpu.VMEM((n_pair, n_ep) + traveling, bf16),
            pltpu.VMEM((n_pair, n_ep) + traveling, bf16),
            pltpu.VMEM((n_pair, n_ep) + traveling, f32),
            pltpu.VMEM((n_pair, n_ep) + traveling, bf16),
            pltpu.VMEM((n_pair, n_ep) + traveling, bf16),
            pltpu.VMEM((n_ep,) + traveling, bf16),
            pltpu.VMEM((n_ep,) + traveling, bf16),
            pltpu.VMEM((n_ep * blocked, row_count), bf16),
            pltpu.VMEM((n_ep * blocked, row_count), bf16),
            dma((13,)),
            dma((2,)),
            dma((2,)),
            dma((9,)),
            dma((n_ep,)),
            dma((n_pair, n_ep // 2)),
            dma((4,)),
            dma((n_pair,)),
            dma((n_pair,)),
            dma((n_pair, 4)),
            dma((n_pair - 1, n_ep)),
            dma((1,)),
        ],
        compiler_params=pltpu.CompilerParams(
            collective_id=0, has_side_effects=True, vmem_limit_bytes=50000 * 1024
        ),
    )(*[
        pltpu.with_memory_space_constraint(operand, pltpu.HBM) if operand.size > 1 else operand
        for operand in operands
    ])
    return mixer_out, expert_out


def solution(mesh):
    in_specs = (
        P("ep", "tp"),
        P("ep", None),
        P("ep", None),
        P("tp"),
        P("tp", None),
        P("ep", None),
        P(),
        P("ep", None),
        P("ep", None),
        P("ep", None, "tp"),
        P("ep", None, "tp"),
        P("ep", "tp", None),
    )
    out_specs = (P(("ep", "tp"), None), P("ep", "tp"))
    return jax.shard_map(
        on_device, mesh=mesh, in_specs=in_specs, out_specs=out_specs, check_vma=False
    )
```

```python
import functools

import jax
import jax.numpy as jnp
import numpy as np
from jax import lax
from jax.experimental import pallas as pl
from jax.experimental.pallas import tpu as pltpu
from jax.sharding import PartitionSpec as P

HEADS = 16
KV_HEADS = 4
HEAD_DIM = 64
WINDOW = 128
TOP = 2
LANES = 128


NORM_EPSILON = 1e-05
ROTARY_BASE = 500000.0
MASK_VALUE = -1e30


def layer_norm(activations, norm_gain):
    values = activations.astype(jnp.float32)
    average = jnp.mean(values, axis=-1, keepdims=True)
    centred = values - average
    variance = jnp.mean(centred * centred, axis=-1, keepdims=True)
    return (centred * lax.rsqrt(variance + NORM_EPSILON) * norm_gain).astype(jnp.bfloat16)


def angle_table(row_count, blocks):
    lane = np.arange(LANES) % HEAD_DIM
    half_dim = HEAD_DIM // 2
    frequency = ROTARY_BASE ** (-2.0 * (lane % half_dim) / HEAD_DIM)
    sign = np.where(lane < half_dim, -1.0, 1.0)
    rows = np.arange(row_count)[:, None] * frequency[None, :]
    bases = np.arange(blocks)[:, None] * row_count * frequency[None, :]
    return np.concatenate(
        [np.cos(rows), sign * np.sin(rows), np.cos(bases), sign * np.sin(bases)]
    ).astype(np.float32)


def partner(index, mask):
    flipped, bit = index, 1
    while bit <= mask:
        if mask & bit:
            flipped = flipped + bit * (1 - 2 * lax.rem(index // bit, 2))
        bit *= 2
    return flipped


def fused_kernel(
    sizes,
    query_hbm,
    key_hbm,
    value_hbm,
    table_hbm,
    sink_hbm,
    input_hbm,
    gain_hbm,
    routes_hbm,
    route_weight_hbm,
    out_hbm,
    gate_hbm,
    up_hbm,
    down_hbm,
    mixer_ref,
    expert_ref,
    query_v,
    key_v,
    value_v,
    table_v,
    sink_v,
    input_v,
    gain_v,
    routes_v,
    route_weight_v,
    out_w,
    gate_w,
    up_w,
    down_w,
    normed_v,
    own_kv,
    halo_send,
    low_kv,
    high_kv,
    packed,
    rows_in,
    gathered,
    hidden,
    mix_send,
    mix_sib,
    mix_cross,
    mix_recv,
    sib_send,
    sib_recv,
    own_acc,
    cross_send,
    cross_recv,
    final_send,
    returned,
    combine_left,
    combine_right,
    load_sem,
    halo_send_sem,
    halo_recv_sem,
    send_sem,
    net_recv_sem,
    far_recv_sem,
    near_recv_sem,
    mix_sib_recv_sem,
    mix_recv_sem,
    sib_recv_sem,
    cross_recv_sem,
    final_recv_sem,
):
    n_ep, n_tp, main, tail = sizes
    cap = main + tail
    halves = 2 if tail else 1
    f32, bf16 = jnp.float32, jnp.bfloat16
    me, my_tp = lax.axis_index("ep"), lax.axis_index("tp")
    core = lax.rem(my_tp, 2)
    pair = my_tp // 2
    n_pair = n_tp // 2
    sibling = my_tp + 1 - 2 * core
    row_count, width = input_v.shape
    slice_width = width // n_tp
    piece = slice_width // halves
    head_dim = HEAD_DIM
    local_heads = sink_v.shape[1]
    half_count = n_ep // 2
    quarter = n_ep // 4
    experts_of = [partner(me, k) for k in range(n_ep)]
    middle = lax.rem(me // half_count + me // quarter, 2)
    bases = [half_count + quarter * (1 - middle), half_count + quarter * middle]
    far_experts = [
        [
            experts_of[half_count + quarter * place + i]
            + middle * (experts_of[half_count + quarter * (1 - place) + i]
                        - experts_of[half_count + quarter * place + i])
            for i in range(quarter)
        ]
        for place in (1, 0)
    ]
    far_batches = [(bases[place], far_experts[place]) for place in range(2)]
    near_batches = [
        (0, experts_of[:quarter]),
        (quarter, experts_of[quarter:half_count]),
    ]
    groups = [(far_batches[place], near_batches[place]) for place in range(2)]
    pair_up = [lax.rem(pair + p, n_pair) for p in range(n_pair)]
    pair_down = [lax.rem(pair + n_pair - p, n_pair) for p in range(n_pair)]

    names = [
        (routes_hbm, routes_v),
        (route_weight_hbm, route_weight_v),
        (gain_hbm, gain_v),
        (input_hbm, input_v),
        (table_hbm, table_v),
        (key_hbm, key_v),
        (value_hbm, value_v),
        (query_hbm, query_v),
        (out_hbm, out_w),
        (gate_hbm.at[0], gate_w),
        (up_hbm.at[0], up_w),
        (down_hbm.at[0], down_w),
        (sink_hbm, sink_v),
    ]
    shared = my_tp * local_heads // (HEADS // KV_HEADS)
    shared_sib = sibling * local_heads // (HEADS // KV_HEADS)
    block = pl.ds(pl.multiple_of(shared // 2 * LANES, LANES), LANES)
    names[5] = (key_hbm.at[:, block], key_v)
    names[6] = (value_hbm.at[:, block], value_v)
    loads = [
        pltpu.make_async_copy(source, target, load_sem.at[number])
        for number, (source, target) in enumerate(names)
    ]

    def remote(source, target, send_sem, recv_sem, ep, tp):
        return pltpu.make_async_remote_copy(
            src_ref=source,
            dst_ref=target,
            send_sem=send_sem,
            recv_sem=recv_sem,
            device_id=(ep, tp),
            device_id_type=pl.DeviceIdType.MESH,
        )

    barrier = pltpu.get_barrier_semaphore()
    for k in range(n_ep - 1, 0, -1):
        pl.semaphore_signal(
            barrier, inc=1, device_id=(experts_of[k], sibling),
            device_id_type=pl.DeviceIdType.MESH,
        )
    for step in range(1, n_tp):
        pl.semaphore_signal(
            barrier, inc=1, device_id=(me, lax.rem(my_tp + step, n_tp)),
            device_id_type=pl.DeviceIdType.MESH,
        )
    for number in [0, 2, 3, 4, 5, 6, 7, 12, 1, 8, 9, 10, 11]:
        loads[number].start()

    def start(copy):
        copy.start()

    def arrived(target, sem):
        pltpu.make_async_copy(target, target, sem).wait()

    loads[0].wait()
    routes = [routes_v[k : k + 1, :] for k in range(TOP)]
    expert_iota = lax.broadcasted_iota(jnp.int32, (n_ep, row_count), 0)
    named = [(routes[k] == expert_iota).astype(f32) for k in range(TOP)]
    earlier = (
        lax.broadcasted_iota(jnp.int32, (row_count, row_count), 0)
        < lax.broadcasted_iota(jnp.int32, (row_count, row_count), 1)
    )
    ahead = jnp.dot(
        functools.reduce(jnp.add, named).astype(bf16),
        earlier.astype(f32).astype(bf16),
        preferred_element_type=f32,
    )
    rank = [
        jnp.sum(ahead * named[k], axis=0, keepdims=True).astype(jnp.int32) for k in range(TOP)
    ]

    def slot_onehot(k):
        slot = lax.broadcasted_iota(jnp.int32, (cap, row_count), 0)
        chosen = [(jnp.where(routes[j] == experts_of[k], rank[j], -1) == slot) for j in range(TOP)]
        return functools.reduce(jnp.logical_or, chosen).astype(f32)

    def pack(values):
        if not tail:
            return values
        parts = [values[:main, :piece], values[:main, piece:], values[main:, :piece], values[main:, piece:]]
        return jnp.concatenate(parts, axis=0)

    far = list(range(half_count, n_ep))
    close = list(range(half_count))
    for number in range(4, 7):
        loads[number].wait()
    lane = lax.broadcasted_iota(jnp.int32, (row_count, LANES), 1)
    low_lane = lane < head_dim
    first_half = lax.rem(lane, head_dim) < head_dim // 2
    row_cos, row_sin = table_v[:row_count], table_v[row_count : 2 * row_count]
    base_cos = table_v[pl.ds(2 * row_count + me, 1), :]
    base_sin = table_v[pl.ds(2 * row_count + n_ep + me, 1), :]
    cosine = base_cos * row_cos - base_sin * row_sin
    sine = base_sin * row_cos + base_cos * row_sin

    def turn(values):
        values = values.astype(f32)
        other = jnp.where(
            first_half,
            pltpu.roll(values, LANES - head_dim // 2, 1),
            pltpu.roll(values, head_dim // 2, 1),
        )
        return values * cosine + other * sine

    turned = turn(key_v[...])
    value = value_v[...].astype(f32)
    turned_roll, value_roll = pltpu.roll(turned, head_dim, 1), pltpu.roll(value, head_dim, 1)

    def key_value(head):
        upper = lax.rem(head, 2) == 1
        return jnp.where(
            low_lane,
            jnp.where(upper, turned_roll, turned),
            jnp.where(upper, value, value_roll),
        ).astype(bf16)

    own_kv[...] = key_value(shared)
    halo_send[...] = key_value(shared_sib)
    to_right = remote(halo_send.at[pl.ds(row_count - WINDOW, WINDOW)], low_kv,
                      halo_send_sem.at[0], halo_recv_sem.at[0], lax.rem(me + 1, n_ep), sibling)
    to_left = remote(halo_send.at[pl.ds(0, WINDOW)], high_kv,
                     halo_send_sem.at[1], halo_recv_sem.at[1], lax.rem(me + n_ep - 1, n_ep), sibling)

    far_onehot = jnp.concatenate([slot_onehot(k) for k in far], axis=0).astype(bf16)
    close_onehot = jnp.concatenate([slot_onehot(k) for k in close], axis=0).astype(bf16)

    loads[2].wait()
    loads[3].wait()
    normed_v[...] = layer_norm(input_v[...], gain_v[...])

    def columns_of(owner, size):
        return pl.ds(pl.multiple_of(owner * size, size), size)

    own_slice = normed_v[:, columns_of(my_tp, slice_width)]
    slots = jnp.dot(far_onehot, own_slice, preferred_element_type=f32)
    for place, k in enumerate(far):
        packed[0, k] = pack(slots[place * cap : (place + 1) * cap]).astype(bf16)

    pl.semaphore_wait(barrier, n_ep + n_tp - 2)

    def net(k, expert, q, sem):
        owner = 2 * pair_up[q] + core
        return remote(packed.at[q, k], rows_in.at[owner, k],
                      send_sem.at[sem], net_recv_sem.at[k], expert, sibling)

    @pl.when(me < n_ep - 1)
    def _():
        to_right.start()

    @pl.when(me > 0)
    def _():
        to_left.start()

    @pl.when(me == 0)
    def _():
        low_kv[...] = jnp.zeros_like(low_kv)

    @pl.when(me == n_ep - 1)
    def _():
        high_kv[...] = jnp.zeros_like(high_kv)

    for base, experts in far_batches:
        for i, expert in enumerate(experts):
            start(net(base + i, expert, 0, 0))

    for q in range(n_pair):
        for side in range(2):
            owner = 2 * pair_up[q] + (core if side == 0 else 1 - core)
            rows = close_onehot if side == 0 else close_onehot[:cap]
            slots = jnp.dot(rows, normed_v[:, columns_of(owner, slice_width)], preferred_element_type=f32)
            rows_in[owner, 0] = pack(slots[:cap]).astype(bf16)
            if side == 0:
                for place, k in enumerate(close[1:]):
                    place = (place + 1) * cap
                    packed[q, k] = pack(slots[place : place + cap]).astype(bf16)

    for k in close[1:]:
        for q in range(n_pair):
            start(net(k, experts_of[k], q, 1))

    loads[12].wait()
    loads[7].wait()
    query = [
        turn(query_v[:, pl.ds(column, LANES)]) for column in range(0, query_v.shape[1], LANES)
    ]
    local = lax.broadcasted_iota(jnp.int32, (row_count, WINDOW), 0)
    other = lax.broadcasted_iota(jnp.int32, (row_count, WINDOW), 1)

    def split_heads(packed_rows):
        both = packed_rows.astype(f32)
        swapped = pltpu.roll(both, head_dim, 1)
        low = lax.broadcasted_iota(jnp.int32, both.shape, 1) < head_dim
        return jnp.where(low, both, swapped).astype(bf16), jnp.where(low, swapped, both).astype(bf16)

    own_rows = jnp.abs(
        lax.broadcasted_iota(jnp.int32, (row_count, row_count), 0)
        - lax.broadcasted_iota(jnp.int32, (row_count, row_count), 1)
    ) <= WINDOW
    own_keys, own_values = split_heads(own_kv[...])
    head_queries, own_scores = [], []

    def score(head_query, keys, allowed):
        scores = lax.dot_general(
            head_query, keys, (((1,), (1,)), ((), ())), preferred_element_type=f32
        ) * head_dim ** (-0.5)
        return jnp.where(allowed, scores, MASK_VALUE)

    for head in range(local_heads):
        mine = low_lane if head % 2 == 0 else jnp.logical_not(low_lane)
        head_queries.append(jnp.where(mine, query[head // 2], 0.0).astype(bf16))
        own_scores.append(score(head_queries[head], own_keys, own_rows))

    @pl.when(me > 0)
    def _():
        to_right.wait_recv()

    @pl.when(me < n_ep - 1)
    def _():
        to_left.wait_recv()

    low_allowed = (local - (other - WINDOW) <= WINDOW) & (me > 0)
    high_allowed = (row_count + other - local <= WINDOW) & (me < n_ep - 1)
    low_keys, low_values = split_heads(low_kv[...])
    high_keys, high_values = split_heads(high_kv[...])
    values = jnp.concatenate([low_values, own_values, high_values], axis=0)
    blocks = []
    for head in range(local_heads):
        parts = [
            score(head_queries[head], low_keys, low_allowed),
            own_scores[head],
            score(head_queries[head], high_keys, high_allowed),
        ]
        sink = sink_v[:, head : head + 1]
        highest = [jnp.max(part, axis=-1, keepdims=True) for part in parts]
        if row_count == WINDOW:
            highest = [jnp.max(functools.reduce(jnp.maximum, parts), axis=-1, keepdims=True)]
        largest = functools.reduce(jnp.maximum, highest + [sink])
        weights = [jnp.exp(part - largest) for part in parts]
        totals = [jnp.sum(weight, axis=-1, keepdims=True) for weight in weights]
        if row_count == WINDOW:
            totals = [jnp.sum(functools.reduce(jnp.add, weights), axis=-1, keepdims=True)]
        denominator = functools.reduce(jnp.add, totals) + jnp.exp(sink - largest)
        scale = 1.0 / denominator
        probability = jnp.concatenate([(weight * scale).astype(bf16) for weight in weights], axis=1)
        result = jnp.dot(probability, values, preferred_element_type=f32)
        if head % 2 == 0:
            blocks.append(result)
        else:
            blocks[-1] = jnp.where(low_lane, blocks[-1], result)
    attended = jnp.concatenate(blocks, axis=1).astype(bf16)[:, : local_heads * head_dim]
    loads[8].wait()
    partial_sum = jnp.dot(attended, out_w[...], preferred_element_type=f32)
    mix_send[...] = partial_sum.reshape(mix_send.shape).astype(bf16)

    def mix_own(p):
        return 2 * pair_up[p] + (core if p == 0 else 1 - core)

    def mix_other(p):
        return 2 * pair_up[p] + (1 - core if p == 0 else core)

    mix_pairs = [
        remote(mix_send.at[mix_other(p)], mix_sib.at[p],
               send_sem.at[4], mix_sib_recv_sem.at[p], me, sibling)
        for p in range(n_pair)
    ]
    for p in list(range(1, n_pair)) + [0]:
        start(mix_pairs[p])

    loads[1].wait()
    blocked = halves * cap
    number = lax.broadcasted_iota(jnp.int32, (blocked, row_count), 0)
    slot_of = number
    left = number >= 0
    if tail:
        in_main = number < 2 * main
        slot_of = jnp.where(
            in_main,
            jnp.where(number < main, number, number - main),
            jnp.where(number < 2 * main + tail, number - main, number - main - tail),
        )
        left = (number < main) | (jnp.logical_not(in_main) & (number < 2 * main + tail))
    for k in range(n_ep):
        placed = jnp.zeros((blocked, row_count), f32)
        for j in range(TOP):
            chosen = jnp.where(routes[j] == experts_of[k], rank[j], -1) == slot_of
            placed = jnp.where(chosen, route_weight_v[j : j + 1, :], placed)
        combine_left[pl.ds(k * blocked, blocked)] = jnp.where(left, placed, 0.0).astype(bf16)
        if tail:
            combine_right[pl.ds(k * blocked, blocked)] = jnp.where(left, 0.0, placed).astype(bf16)

    def near_forward(k, q, sem):
        owner = 2 * pair_up[q] + 1 - core
        return remote(rows_in.at[owner, k], rows_in.at[owner, k],
                      send_sem.at[2], near_recv_sem.at[sem], me, sibling)

    def far_forward(k, p):
        owner = 2 * pair + 1 - core
        return remote(rows_in.at[owner, k], rows_in.at[owner, k],
                      send_sem.at[3], far_recv_sem.at[p - 1, k - half_count], me, 2 * pair_up[p] + 1 - core)

    def far_relay(k, p, sem):
        owner = 2 * pair_down[p] + core
        return remote(rows_in.at[owner, k], rows_in.at[owner, k],
                      send_sem.at[2], near_recv_sem.at[sem], me, sibling)

    def forward_far(number):
        base, experts = far_batches[number]
        for i, expert in enumerate(experts):
            net(base + i, expert, 0, 0).wait_recv()
            for p in range(1, n_pair):
                start(far_forward(base + i, p))
            start(near_forward(base + i, 0, number))

    def relay_far(number):
        base, experts = far_batches[number]
        for i in range(len(experts)):
            for p in range(1, n_pair):
                far_forward(base + i, p).wait_recv()
                start(far_relay(base + i, p, number))

    def forward_near(number):
        base, experts = near_batches[number]
        for k in range(max(base, 1), base + len(experts)):
            arrived(rows_in.at[pl.ds(0, n_pair), k], net_recv_sem.at[k])
            for q in range(n_pair):
                start(near_forward(k, q, 2 + number))

    def gather(number):
        slots = []
        for kind, (base, experts) in enumerate(groups[number]):
            count = len(experts)
            slots += [base + i for i in range(count)]
            if kind == 1 and number == 0:
                count -= 1
            arrived(rows_in.at[pl.ds(0, n_pair), pl.ds(0, count)], near_recv_sem.at[2 * kind + number])
        for owner in range(n_tp):
            for half in range(halves):
                columns = pl.ds(owner * slice_width + half * piece, piece)
                for place, k in enumerate(slots):
                    gathered[pl.ds(place * main, main), columns] = (
                        rows_in[owner, k, pl.ds(half * main, main), :]
                    )
                if tail:
                    ends = [
                        rows_in[owner, k, pl.ds(2 * main, 2 * tail), :].astype(f32)[
                            half * tail : (half + 1) * tail
                        ]
                        for k in slots
                    ]
                    gathered[pl.ds(len(slots) * main, len(slots) * tail), columns] = (
                        jnp.concatenate(ends, axis=0).astype(bf16)
                    )

    hidden_width = gate_w.shape[1]
    tile = min(hidden_width, 512)

    rows = half_count * cap

    def expand():
        for number in range(hidden_width // tile):
            columns = pl.ds(number * tile, tile)
            gate_act = jnp.dot(gathered[...], gate_w[:, columns], preferred_element_type=f32)
            up_act = jnp.dot(gathered[...], up_w[:, columns], preferred_element_type=f32)
            hidden[:, columns] = (gate_act / (1.0 + jnp.exp(-gate_act)) * up_act).astype(bf16)

    def down_slice(number, owner):
        result = jnp.dot(
            hidden[...], down_w[:, columns_of(owner, slice_width)], preferred_element_type=f32
        )
        slots = [base + i for base, experts in groups[number] for i in range(len(experts))]
        for place, k in enumerate(slots):
            values = result[place * main : (place + 1) * main]
            if tail:
                last = half_count * main + place * tail
                values = jnp.concatenate([values, result[last : last + tail]], axis=0)
            yield k, pack(values)

    def sib_copy(base, p):
        batch = pl.ds(base, quarter)
        return remote(sib_send.at[p, batch], sib_recv.at[p, batch],
                      send_sem.at[5], sib_recv_sem.at[p, base // quarter], me, sibling)

    def cross_copy(k, p):
        return remote(cross_send.at[p, k], cross_recv.at[p, k],
                      send_sem.at[6], cross_recv_sem.at[p - 1, k], me, 2 * pair_up[p] + 1 - core)

    def give(number, p):
        owner = 2 * pair_up[p] + (core if p == 0 else 1 - core)
        for k, values in down_slice(number, owner):
            sib_send[p, k] = values.astype(bf16)
        for base, _ in groups[number]:
            start(sib_copy(base, p))

    def keep(number, p):
        owner = 2 * pair_up[p] + (1 - core if p == 0 else core)
        for k, values in down_slice(number, owner):
            own_acc[p, k] = values

    def cross(batch, places=range(quarter)):
        base = batch[0]
        for p in range(1, n_pair):
            for i in places:
                k = base + i
                cross_send[p, k] = (own_acc[p, k] + sib_recv[p, k].astype(f32)).astype(bf16)
                start(cross_copy(k, p))

    def met(batch, parts):
        for p in parts:
            sib_copy(batch[0], p).wait_recv()

    def finish(batch, places=range(quarter)):
        base, experts = batch
        for i in places:
            k, expert = base + i, experts[i]
            total = own_acc[0, k] + sib_recv[0, k].astype(f32)
            for p in range(1, n_pair):
                cross_copy(k, p).wait_recv()
                total += cross_recv[p, k].astype(f32)
            final_send[k] = total.astype(bf16)
            start(remote(final_send.at[k], returned.at[k],
                         send_sem.at[7], final_recv_sem.at[0], expert, sibling))

    def mix_forward():
        for p in range(1, n_pair):
            mix_pairs[p].wait_recv()
            mix_cross[p] = (
                mix_send[mix_own(p)].astype(f32) + mix_sib[p].astype(f32)
            ).astype(bf16)
            start(mix_copy(p))

    def mix_copy(p):
        return remote(mix_cross.at[p], mix_recv.at[p],
                      send_sem.at[8], mix_recv_sem.at[p], me, 2 * pair_up[p] + 1 - core)

    def mix_finish():
        mix_pairs[0].wait_recv()
        mixed = mix_send[mix_own(0)].astype(f32) + mix_sib[0].astype(f32)
        for p in range(1, n_pair):
            mix_copy(p).wait_recv()
            mixed += mix_recv[p].astype(f32)
        mixer_ref[...] = mixed.astype(mixer_ref.dtype)

    others, rest = range(1, n_pair), range(1, quarter)
    forward_far(0)
    forward_near(0)
    forward_far(1)
    relay_far(0)
    mix_forward()
    loads[9].wait()
    loads[10].wait()
    gather(0)
    expand()
    loads[11].wait()
    for p in others:
        give(0, p)
    relay_far(1)
    forward_near(1)
    for p in others:
        keep(0, p)
    give(0, 0)
    met(far_batches[0], others)
    cross(far_batches[0])
    keep(0, 0)
    gather(1)
    met(near_batches[0], others)
    cross(near_batches[0], rest)
    expand()
    for p in others:
        give(1, p)
        keep(1, p)
    give(1, 0)
    met(far_batches[1], others)
    cross(far_batches[1])
    met(far_batches[0], [0])
    finish(far_batches[0])
    keep(1, 0)
    met(near_batches[1], others)
    cross(near_batches[1])
    cross(near_batches[0], [0])
    met(near_batches[0], [0])
    finish(near_batches[0], rest)
    met(far_batches[1], [0])
    finish(far_batches[1])
    mix_finish()
    met(near_batches[1], [0])
    finish(near_batches[1])
    finish(near_batches[0], [0])

    arrived(returned, final_recv_sem.at[0])
    blocks = returned[...].reshape(n_ep * blocked, piece)

    def combined(weights_ref):
        return lax.dot_general(
            weights_ref[...], blocks, (((0,), (0,)), ((), ())), preferred_element_type=f32
        )

    expert_ref[:, :piece] = combined(combine_left).astype(expert_ref.dtype)
    if tail:
        expert_ref[:, piece:] = combined(combine_right).astype(expert_ref.dtype)

    @pl.when(me < n_ep - 1)
    def _():
        to_right.wait_send()

    @pl.when(me > 0)
    def _():
        to_left.wait_send()

    far_count = n_ep - half_count
    arrived(packed.at[0, pl.ds(0, far_count)], send_sem.at[0])
    arrived(packed.at[:, pl.ds(0, half_count - 1)], send_sem.at[1])
    arrived(rows_in.at[pl.ds(0, n_pair), pl.ds(0, n_ep - 1)], send_sem.at[2])
    if n_pair > 1:
        arrived(rows_in.at[pl.ds(0, n_pair - 1), pl.ds(0, far_count)], send_sem.at[3])
    arrived(mix_sib, send_sem.at[4])
    if n_pair > 1:
        arrived(mix_cross.at[pl.ds(0, n_pair - 1)], send_sem.at[8])
    arrived(sib_send, send_sem.at[5])
    if n_pair > 1:
        arrived(cross_send.at[pl.ds(0, n_pair - 1)], send_sem.at[6])
    arrived(final_send, send_sem.at[7])


def write_kernel(mixer_in, expert_in, mixer_out, expert_out, sem):
    copies = [
        pltpu.make_async_copy(mixer_in, mixer_out, sem.at[0]),
        pltpu.make_async_copy(expert_in, expert_out, sem.at[1]),
    ]
    for copy in copies:
        copy.start()
    for copy in copies:
        copy.wait()


def on_device(
    queries,
    key_states,
    value_states,
    sink_logit,
    out_weight,
    expert_input,
    norm_gain,
    routes,
    route_weight,
    gate_weight,
    up_weight,
    down_weight,
):
    n_ep = lax.axis_size("ep")
    n_tp = lax.axis_size("tp")
    row_count, width = expert_input.shape
    local_heads = queries.shape[1] // HEAD_DIM
    capacity = row_count * TOP * 5 // (4 * n_ep)
    main, tail = capacity // 16 * 16, 0
    if 0 < capacity - main <= 8 and width // n_tp >= 2 * LANES and main:
        tail = 8
    elif capacity > main:
        main += 16
    halves = 2 if tail else 1
    slice_width = width // n_tp
    piece = slice_width // halves
    blocked = halves * (main + tail)
    hidden_width = gate_weight.shape[2]
    mix_rows = row_count // n_tp
    n_pair = n_tp // 2
    group_rows = n_ep // 2 * (main + tail)
    if queries.shape[1] % LANES:
        queries = jnp.pad(queries, ((0, 0), (0, LANES - queries.shape[1] % LANES)))
    table = jnp.asarray(angle_table(row_count, n_ep))
    vmem = pl.BlockSpec(memory_space=pltpu.VMEM)
    hbm = pl.BlockSpec(memory_space=pltpu.HBM)
    bf16, f32 = jnp.bfloat16, jnp.float32
    dma = pltpu.SemaphoreType.DMA
    traveling = (blocked, piece)
    operands = (
        queries,
        key_states,
        value_states,
        table,
        sink_logit[None, :],
        expert_input,
        norm_gain[None, :],
        routes.T,
        route_weight.T,
        out_weight,
        gate_weight,
        up_weight,
        down_weight,
    )
    mixer_out, expert_out = pl.pallas_call(
        functools.partial(fused_kernel, (n_ep, n_tp, main, tail)),
        out_shape=(
            jax.ShapeDtypeStruct((mix_rows, width), bf16),
            jax.ShapeDtypeStruct((row_count, slice_width), bf16),
        ),
        in_specs=[hbm] * 13,
        out_specs=(vmem, vmem),
        scratch_shapes=[
            pltpu.VMEM(queries.shape, bf16),
            pltpu.VMEM((row_count, LANES), bf16),
            pltpu.VMEM((row_count, LANES), bf16),
            pltpu.VMEM(table.shape, f32),
            pltpu.VMEM((1, local_heads), f32),
            pltpu.VMEM(expert_input.shape, bf16),
            pltpu.VMEM((1, width), f32),
            pltpu.VMEM((TOP, row_count), jnp.int32),
            pltpu.VMEM((TOP, row_count), f32),
            pltpu.VMEM(out_weight.shape, bf16),
            pltpu.VMEM(gate_weight.shape[1:], bf16),
            pltpu.VMEM(up_weight.shape[1:], bf16),
            pltpu.VMEM(down_weight.shape[1:], bf16),
            pltpu.VMEM(expert_input.shape, bf16),
            pltpu.VMEM((row_count, LANES), bf16),
            pltpu.VMEM((row_count, LANES), bf16),
            pltpu.VMEM((WINDOW, LANES), bf16),
            pltpu.VMEM((WINDOW, LANES), bf16),
            pltpu.VMEM((n_pair, n_ep) + traveling, bf16),
            pltpu.VMEM((n_tp, n_ep) + traveling, bf16),
            pltpu.VMEM((group_rows, width), bf16),
            pltpu.VMEM((group_rows, hidden_width), bf16),
            pltpu.VMEM((n_tp, mix_rows, width), bf16),
            pltpu.VMEM((n_pair, mix_rows, width), bf16),
            pltpu.VMEM((n_pair, mix_rows, width), bf16),
            pltpu.VMEM((n_pair, mix_rows, width), bf16),
            pltpu.VMEM((n_pair, n_ep) + traveling, bf16),
            pltpu.VMEM((n_pair, n_ep) + traveling, bf16),
            pltpu.VMEM((n_pair, n_ep) + traveling, f32),
            pltpu.VMEM((n_pair, n_ep) + traveling, bf16),
            pltpu.VMEM((n_pair, n_ep) + traveling, bf16),
            pltpu.VMEM((n_ep,) + traveling, bf16),
            pltpu.VMEM((n_ep,) + traveling, bf16),
            pltpu.VMEM((n_ep * blocked, row_count), bf16),
            pltpu.VMEM((n_ep * blocked, row_count), bf16),
            dma((13,)),
            dma((2,)),
            dma((2,)),
            dma((9,)),
            dma((n_ep,)),
            dma((n_pair - 1, n_ep // 2)),
            dma((4,)),
            dma((n_pair,)),
            dma((n_pair,)),
            dma((n_pair, 4)),
            dma((n_pair - 1, n_ep)),
            dma((1,)),
        ],
        compiler_params=pltpu.CompilerParams(
            collective_id=0, has_side_effects=True, vmem_limit_bytes=50000 * 1024
        ),
    )(*[
        pltpu.with_memory_space_constraint(operand, pltpu.HBM) if operand.size > 1 else operand
        for operand in operands
    ])
    return pl.pallas_call(
        write_kernel,
        out_shape=(
            jax.ShapeDtypeStruct(mixer_out.shape, bf16),
            jax.ShapeDtypeStruct(expert_out.shape, bf16),
        ),
        in_specs=[vmem] * 2,
        out_specs=(hbm, hbm),
        scratch_shapes=[dma((2,))],
        compiler_params=pltpu.CompilerParams(vmem_limit_bytes=1024 * 1024),
    )(*[pltpu.with_memory_space_constraint(x, pltpu.VMEM) for x in (mixer_out, expert_out)])


def solution(mesh):
    in_specs = (
        P("ep", "tp"),
        P("ep", None),
        P("ep", None),
        P("tp"),
        P("tp", None),
        P("ep", None),
        P(),
        P("ep", None),
        P("ep", None),
        P("ep", None, "tp"),
        P("ep", None, "tp"),
        P("ep", "tp", None),
    )
    out_specs = (P(("ep", "tp"), None), P("ep", "tp"))
    return jax.shard_map(
        on_device, mesh=mesh, in_specs=in_specs, out_specs=out_specs, check_vma=False
    )
```

```python
import functools

import jax
import jax.numpy as jnp
import numpy as np
from jax import lax
from jax.experimental import pallas as pl
from jax.experimental.pallas import tpu as pltpu
from jax.sharding import PartitionSpec as P

HEADS = 16
KV_HEADS = 4
HEAD_DIM = 64
WINDOW = 128
TOP = 2
LANES = 128


NORM_EPSILON = 1e-05
ROTARY_BASE = 500000.0
MASK_VALUE = -1e30


def layer_norm(activations, norm_gain):
    values = activations.astype(jnp.float32)
    average = jnp.mean(values, axis=-1, keepdims=True)
    centred = values - average
    variance = jnp.mean(centred * centred, axis=-1, keepdims=True)
    return (centred * lax.rsqrt(variance + NORM_EPSILON) * norm_gain).astype(jnp.bfloat16)


def angle_table(row_count, blocks):
    lane = np.arange(LANES) % HEAD_DIM
    half_dim = HEAD_DIM // 2
    frequency = ROTARY_BASE ** (-2.0 * (lane % half_dim) / HEAD_DIM)
    sign = np.where(lane < half_dim, -1.0, 1.0)
    rows = np.arange(row_count)[:, None] * frequency[None, :]
    bases = np.arange(blocks)[:, None] * row_count * frequency[None, :]
    return np.concatenate(
        [np.cos(rows), sign * np.sin(rows), np.cos(bases), sign * np.sin(bases)]
    ).astype(np.float32)


def partner(index, mask):
    flipped, bit = index, 1
    while bit <= mask:
        if mask & bit:
            flipped = flipped + bit * (1 - 2 * lax.rem(index // bit, 2))
        bit *= 2
    return flipped


def fused_kernel(
    sizes,
    query_hbm,
    key_hbm,
    value_hbm,
    table_hbm,
    sink_hbm,
    input_hbm,
    gain_hbm,
    routes_hbm,
    route_weight_hbm,
    out_hbm,
    gate_hbm,
    up_hbm,
    down_hbm,
    mixer_ref,
    expert_ref,
    query_v,
    key_v,
    value_v,
    table_v,
    sink_v,
    input_v,
    gain_v,
    routes_v,
    route_weight_v,
    out_w,
    gate_w,
    up_w,
    down_w,
    normed_v,
    own_kv,
    halo_send,
    low_kv,
    high_kv,
    packed,
    rows_in,
    gathered,
    hidden,
    mix_send,
    mix_sib,
    mix_cross,
    mix_recv,
    sib_send,
    sib_recv,
    own_acc,
    cross_send,
    cross_recv,
    final_send,
    returned,
    combine_left,
    combine_right,
    load_sem,
    halo_send_sem,
    halo_recv_sem,
    send_sem,
    net_recv_sem,
    far_recv_sem,
    near_recv_sem,
    mix_sib_recv_sem,
    mix_recv_sem,
    sib_recv_sem,
    cross_recv_sem,
    final_recv_sem,
):
    n_ep, n_tp, main, tail = sizes
    cap = main + tail
    halves = 2 if tail else 1
    f32, bf16 = jnp.float32, jnp.bfloat16
    me, my_tp = lax.axis_index("ep"), lax.axis_index("tp")
    core = lax.rem(my_tp, 2)
    pair = my_tp // 2
    n_pair = n_tp // 2
    sibling = my_tp + 1 - 2 * core
    row_count, width = input_v.shape
    slice_width = width // n_tp
    piece = slice_width // halves
    head_dim = HEAD_DIM
    local_heads = sink_v.shape[1]
    half_count = n_ep // 2
    quarter = n_ep // 4
    experts_of = [partner(me, k) for k in range(n_ep)]
    middle = lax.rem(me // half_count + me // quarter, 2)
    bases = [half_count + quarter * (1 - middle), half_count + quarter * middle]
    far_experts = [
        [
            experts_of[half_count + quarter * place + i]
            + middle * (experts_of[half_count + quarter * (1 - place) + i]
                        - experts_of[half_count + quarter * place + i])
            for i in range(quarter)
        ]
        for place in (1, 0)
    ]
    far_batches = [(bases[place], far_experts[place]) for place in range(2)]
    near_batches = [
        (0, experts_of[:quarter]),
        (quarter, experts_of[quarter:half_count]),
    ]
    groups = [(far_batches[place], near_batches[place]) for place in range(2)]
    pair_up = [lax.rem(pair + p, n_pair) for p in range(n_pair)]
    pair_down = [lax.rem(pair + n_pair - p, n_pair) for p in range(n_pair)]

    names = [
        (routes_hbm, routes_v),
        (route_weight_hbm, route_weight_v),
        (gain_hbm, gain_v),
        (input_hbm, input_v),
        (table_hbm, table_v),
        (key_hbm, key_v),
        (value_hbm, value_v),
        (query_hbm, query_v),
        (out_hbm, out_w),
        (gate_hbm.at[0], gate_w),
        (up_hbm.at[0], up_w),
        (down_hbm.at[0], down_w),
        (sink_hbm, sink_v),
    ]
    shared = my_tp * local_heads // (HEADS // KV_HEADS)
    shared_sib = sibling * local_heads // (HEADS // KV_HEADS)
    block = pl.ds(pl.multiple_of(shared // 2 * LANES, LANES), LANES)
    names[5] = (key_hbm.at[:, block], key_v)
    names[6] = (value_hbm.at[:, block], value_v)
    loads = [
        pltpu.make_async_copy(source, target, load_sem.at[number])
        for number, (source, target) in enumerate(names)
    ]

    def remote(source, target, send_sem, recv_sem, ep, tp):
        return pltpu.make_async_remote_copy(
            src_ref=source,
            dst_ref=target,
            send_sem=send_sem,
            recv_sem=recv_sem,
            device_id=(ep, tp),
            device_id_type=pl.DeviceIdType.MESH,
        )

    barrier = pltpu.get_barrier_semaphore()
    for k in range(n_ep - 1, 0, -1):
        pl.semaphore_signal(
            barrier, inc=1, device_id=(experts_of[k], sibling),
            device_id_type=pl.DeviceIdType.MESH,
        )
    for step in range(1, n_tp):
        pl.semaphore_signal(
            barrier, inc=1, device_id=(me, lax.rem(my_tp + step, n_tp)),
            device_id_type=pl.DeviceIdType.MESH,
        )
    for number in [0, 2, 3, 4, 5, 6, 7, 12, 1, 8, 9, 10, 11]:
        loads[number].start()

    def start(copy):
        copy.start()

    def arrived(target, sem):
        pltpu.make_async_copy(target, target, sem).wait()

    loads[0].wait()
    routes = [routes_v[k : k + 1, :] for k in range(TOP)]
    expert_iota = lax.broadcasted_iota(jnp.int32, (n_ep, row_count), 0)
    named = [(routes[k] == expert_iota).astype(f32) for k in range(TOP)]
    earlier = (
        lax.broadcasted_iota(jnp.int32, (row_count, row_count), 0)
        < lax.broadcasted_iota(jnp.int32, (row_count, row_count), 1)
    )
    ahead = jnp.dot(
        functools.reduce(jnp.add, named).astype(bf16),
        earlier.astype(f32).astype(bf16),
        preferred_element_type=f32,
    )
    rank = [
        jnp.sum(ahead * named[k], axis=0, keepdims=True).astype(jnp.int32) for k in range(TOP)
    ]

    def slot_onehot(k):
        slot = lax.broadcasted_iota(jnp.int32, (cap, row_count), 0)
        chosen = [(jnp.where(routes[j] == experts_of[k], rank[j], -1) == slot) for j in range(TOP)]
        return functools.reduce(jnp.logical_or, chosen).astype(f32)

    def pack(values):
        if not tail:
            return values
        parts = [values[:main, :piece], values[:main, piece:], values[main:, :piece], values[main:, piece:]]
        return jnp.concatenate(parts, axis=0)

    far = list(range(half_count, n_ep))
    close = list(range(half_count))
    for number in range(4, 7):
        loads[number].wait()
    lane = lax.broadcasted_iota(jnp.int32, (row_count, LANES), 1)
    low_lane = lane < head_dim
    first_half = lax.rem(lane, head_dim) < head_dim // 2
    row_cos, row_sin = table_v[:row_count], table_v[row_count : 2 * row_count]
    base_cos = table_v[pl.ds(2 * row_count + me, 1), :]
    base_sin = table_v[pl.ds(2 * row_count + n_ep + me, 1), :]
    cosine = base_cos * row_cos - base_sin * row_sin
    sine = base_sin * row_cos + base_cos * row_sin

    def turn(values):
        values = values.astype(f32)
        other = jnp.where(
            first_half,
            pltpu.roll(values, LANES - head_dim // 2, 1),
            pltpu.roll(values, head_dim // 2, 1),
        )
        return values * cosine + other * sine

    turned = turn(key_v[...])
    value = value_v[...].astype(f32)
    turned_roll, value_roll = pltpu.roll(turned, head_dim, 1), pltpu.roll(value, head_dim, 1)

    def key_value(head):
        upper = lax.rem(head, 2) == 1
        return jnp.where(
            low_lane,
            jnp.where(upper, turned_roll, turned),
            jnp.where(upper, value, value_roll),
        ).astype(bf16)

    own_kv[...] = key_value(shared)
    halo_send[...] = key_value(shared_sib)
    to_right = remote(halo_send.at[pl.ds(row_count - WINDOW, WINDOW)], low_kv,
                      halo_send_sem.at[0], halo_recv_sem.at[0], lax.rem(me + 1, n_ep), sibling)
    to_left = remote(halo_send.at[pl.ds(0, WINDOW)], high_kv,
                     halo_send_sem.at[1], halo_recv_sem.at[1], lax.rem(me + n_ep - 1, n_ep), sibling)

    far_onehot = jnp.concatenate([slot_onehot(k) for k in far], axis=0).astype(bf16)
    close_onehot = jnp.concatenate([slot_onehot(k) for k in close], axis=0).astype(bf16)

    loads[2].wait()
    loads[3].wait()
    normed_v[...] = layer_norm(input_v[...], gain_v[...])

    def columns_of(owner, size):
        return pl.ds(pl.multiple_of(owner * size, size), size)

    own_slice = normed_v[:, columns_of(my_tp, slice_width)]
    slots = jnp.dot(far_onehot, own_slice, preferred_element_type=f32)
    for place, k in enumerate(far):
        packed[0, k] = pack(slots[place * cap : (place + 1) * cap]).astype(bf16)

    pl.semaphore_wait(barrier, n_ep + n_tp - 2)

    def net(k, expert, q, sem):
        owner = 2 * pair_up[q] + core
        return remote(packed.at[q, k], rows_in.at[owner, k],
                      send_sem.at[sem], net_recv_sem.at[k], expert, sibling)

    @pl.when(me < n_ep - 1)
    def _():
        to_right.start()

    @pl.when(me > 0)
    def _():
        to_left.start()

    @pl.when(me == 0)
    def _():
        low_kv[...] = jnp.zeros_like(low_kv)

    @pl.when(me == n_ep - 1)
    def _():
        high_kv[...] = jnp.zeros_like(high_kv)

    for base, experts in far_batches:
        for i, expert in enumerate(experts):
            start(net(base + i, expert, 0, 0))

    for q in range(n_pair):
        for side in range(2):
            owner = 2 * pair_up[q] + (core if side == 0 else 1 - core)
            rows = close_onehot if side == 0 else close_onehot[:cap]
            slots = jnp.dot(rows, normed_v[:, columns_of(owner, slice_width)], preferred_element_type=f32)
            rows_in[owner, 0] = pack(slots[:cap]).astype(bf16)
            if side == 0:
                for place, k in enumerate(close[1:]):
                    place = (place + 1) * cap
                    packed[q, k] = pack(slots[place : place + cap]).astype(bf16)

    for k in close[1:]:
        for q in range(n_pair):
            start(net(k, experts_of[k], q, 1))

    loads[12].wait()
    loads[7].wait()
    query = [
        turn(query_v[:, pl.ds(column, LANES)]) for column in range(0, query_v.shape[1], LANES)
    ]
    local = lax.broadcasted_iota(jnp.int32, (row_count, WINDOW), 0)
    other = lax.broadcasted_iota(jnp.int32, (row_count, WINDOW), 1)

    def split_heads(packed_rows):
        both = packed_rows.astype(f32)
        swapped = pltpu.roll(both, head_dim, 1)
        low = lax.broadcasted_iota(jnp.int32, both.shape, 1) < head_dim
        return jnp.where(low, both, swapped).astype(bf16), jnp.where(low, swapped, both).astype(bf16)

    own_rows = jnp.abs(
        lax.broadcasted_iota(jnp.int32, (row_count, row_count), 0)
        - lax.broadcasted_iota(jnp.int32, (row_count, row_count), 1)
    ) <= WINDOW
    own_keys, own_values = split_heads(own_kv[...])
    head_queries, own_scores = [], []

    def score(head_query, keys, allowed):
        scores = lax.dot_general(
            head_query, keys, (((1,), (1,)), ((), ())), preferred_element_type=f32
        ) * head_dim ** (-0.5)
        return jnp.where(allowed, scores, MASK_VALUE)

    for head in range(local_heads):
        mine = low_lane if head % 2 == 0 else jnp.logical_not(low_lane)
        head_queries.append(jnp.where(mine, query[head // 2], 0.0).astype(bf16))
        own_scores.append(score(head_queries[head], own_keys, own_rows))

    @pl.when(me > 0)
    def _():
        to_right.wait_recv()

    @pl.when(me < n_ep - 1)
    def _():
        to_left.wait_recv()

    low_allowed = (local - (other - WINDOW) <= WINDOW) & (me > 0)
    high_allowed = (row_count + other - local <= WINDOW) & (me < n_ep - 1)
    low_keys, low_values = split_heads(low_kv[...])
    high_keys, high_values = split_heads(high_kv[...])
    values = jnp.concatenate([low_values, own_values, high_values], axis=0)
    blocks = []
    for head in range(local_heads):
        parts = [
            score(head_queries[head], low_keys, low_allowed),
            own_scores[head],
            score(head_queries[head], high_keys, high_allowed),
        ]
        sink = sink_v[:, head : head + 1]
        highest = [jnp.max(part, axis=-1, keepdims=True) for part in parts]
        if row_count == WINDOW:
            highest = [jnp.max(functools.reduce(jnp.maximum, parts), axis=-1, keepdims=True)]
        largest = functools.reduce(jnp.maximum, highest + [sink])
        weights = [jnp.exp(part - largest) for part in parts]
        totals = [jnp.sum(weight, axis=-1, keepdims=True) for weight in weights]
        if row_count == WINDOW:
            totals = [jnp.sum(functools.reduce(jnp.add, weights), axis=-1, keepdims=True)]
        denominator = functools.reduce(jnp.add, totals) + jnp.exp(sink - largest)
        scale = 1.0 / denominator
        probability = jnp.concatenate([(weight * scale).astype(bf16) for weight in weights], axis=1)
        result = jnp.dot(probability, values, preferred_element_type=f32)
        if head % 2 == 0:
            blocks.append(result)
        else:
            blocks[-1] = jnp.where(low_lane, blocks[-1], result)
    attended = jnp.concatenate(blocks, axis=1).astype(bf16)[:, : local_heads * head_dim]
    loads[8].wait()
    partial_sum = jnp.dot(attended, out_w[...], preferred_element_type=f32)
    mix_send[...] = partial_sum.reshape(mix_send.shape).astype(bf16)

    def mix_own(p):
        return 2 * pair_up[p] + (core if p == 0 else 1 - core)

    def mix_other(p):
        return 2 * pair_up[p] + (1 - core if p == 0 else core)

    mix_pairs = [
        remote(mix_send.at[mix_other(p)], mix_sib.at[p],
               send_sem.at[4], mix_sib_recv_sem.at[p], me, sibling)
        for p in range(n_pair)
    ]
    for p in list(range(1, n_pair)) + [0]:
        start(mix_pairs[p])

    loads[1].wait()
    blocked = halves * cap
    number = lax.broadcasted_iota(jnp.int32, (blocked, row_count), 0)
    slot_of = number
    left = number >= 0
    if tail:
        in_main = number < 2 * main
        slot_of = jnp.where(
            in_main,
            jnp.where(number < main, number, number - main),
            jnp.where(number < 2 * main + tail, number - main, number - main - tail),
        )
        left = (number < main) | (jnp.logical_not(in_main) & (number < 2 * main + tail))
    for k in range(n_ep):
        placed = jnp.zeros((blocked, row_count), f32)
        for j in range(TOP):
            chosen = jnp.where(routes[j] == experts_of[k], rank[j], -1) == slot_of
            placed = jnp.where(chosen, route_weight_v[j : j + 1, :], placed)
        combine_left[pl.ds(k * blocked, blocked)] = jnp.where(left, placed, 0.0).astype(bf16)
        if tail:
            combine_right[pl.ds(k * blocked, blocked)] = jnp.where(left, 0.0, placed).astype(bf16)

    def near_forward(k, q, sem):
        owner = 2 * pair_up[q] + 1 - core
        return remote(rows_in.at[owner, k], rows_in.at[owner, k],
                      send_sem.at[2], near_recv_sem.at[sem], me, sibling)

    def far_forward(k, p):
        owner = 2 * pair + 1 - core
        return remote(rows_in.at[owner, k], rows_in.at[owner, k],
                      send_sem.at[3], far_recv_sem.at[p - 1, k - half_count], me, 2 * pair_up[p] + 1 - core)

    def far_relay(k, p, sem):
        owner = 2 * pair_down[p] + core
        return remote(rows_in.at[owner, k], rows_in.at[owner, k],
                      send_sem.at[2], near_recv_sem.at[sem], me, sibling)

    def forward_far(number):
        base, experts = far_batches[number]
        for i, expert in enumerate(experts):
            net(base + i, expert, 0, 0).wait_recv()
            for p in range(1, n_pair):
                start(far_forward(base + i, p))
            start(near_forward(base + i, 0, number))

    def relay_far(number):
        base, experts = far_batches[number]
        for i in range(len(experts)):
            for p in range(1, n_pair):
                far_forward(base + i, p).wait_recv()
                start(far_relay(base + i, p, number))

    def forward_near(number):
        base, experts = near_batches[number]
        for k in range(max(base, 1), base + len(experts)):
            arrived(rows_in.at[pl.ds(0, n_pair), k], net_recv_sem.at[k])
            for q in range(n_pair):
                start(near_forward(k, q, 2 + number))

    def gather(number):
        slots = []
        for kind, (base, experts) in enumerate(groups[number]):
            count = len(experts)
            slots += [base + i for i in range(count)]
            if kind == 1 and number == 0:
                count -= 1
            arrived(rows_in.at[pl.ds(0, n_pair), pl.ds(0, count)], near_recv_sem.at[2 * kind + number])
        for owner in range(n_tp):
            for half in range(halves):
                columns = pl.ds(owner * slice_width + half * piece, piece)
                for place, k in enumerate(slots):
                    gathered[pl.ds(place * main, main), columns] = (
                        rows_in[owner, k, pl.ds(half * main, main), :]
                    )
                if tail:
                    ends = [
                        rows_in[owner, k, pl.ds(2 * main, 2 * tail), :].astype(f32)[
                            half * tail : (half + 1) * tail
                        ]
                        for k in slots
                    ]
                    gathered[pl.ds(len(slots) * main, len(slots) * tail), columns] = (
                        jnp.concatenate(ends, axis=0).astype(bf16)
                    )

    hidden_width = gate_w.shape[1]
    tile = min(hidden_width, 512)

    rows = half_count * cap

    def expand():
        for number in range(hidden_width // tile):
            columns = pl.ds(number * tile, tile)
            gate_act = jnp.dot(gathered[...], gate_w[:, columns], preferred_element_type=f32)
            up_act = jnp.dot(gathered[...], up_w[:, columns], preferred_element_type=f32)
            hidden[:, columns] = (gate_act / (1.0 + jnp.exp(-gate_act)) * up_act).astype(bf16)

    def down_slice(number, owner):
        result = jnp.dot(
            hidden[...], down_w[:, columns_of(owner, slice_width)], preferred_element_type=f32
        )
        slots = [base + i for base, experts in groups[number] for i in range(len(experts))]
        for place, k in enumerate(slots):
            values = result[place * main : (place + 1) * main]
            if tail:
                last = half_count * main + place * tail
                values = jnp.concatenate([values, result[last : last + tail]], axis=0)
            yield k, pack(values)

    def sib_copy(base, p):
        batch = pl.ds(base, quarter)
        return remote(sib_send.at[p, batch], sib_recv.at[p, batch],
                      send_sem.at[5], sib_recv_sem.at[p, base // quarter], me, sibling)

    def cross_copy(k, p):
        return remote(cross_send.at[p, k], cross_recv.at[p, k],
                      send_sem.at[6], cross_recv_sem.at[p - 1, k], me, 2 * pair_up[p] + 1 - core)

    def give(number, p):
        owner = 2 * pair_up[p] + (core if p == 0 else 1 - core)
        for k, values in down_slice(number, owner):
            sib_send[p, k] = values.astype(bf16)
        for base, _ in groups[number]:
            start(sib_copy(base, p))

    def keep(number, p):
        owner = 2 * pair_up[p] + (1 - core if p == 0 else core)
        for k, values in down_slice(number, owner):
            own_acc[p, k] = values

    def in_order(batch, places):
        base, experts = batch
        if places is not None or quarter % 2:
            return [(base + i, experts[i]) for i in places or range(quarter)]
        odd = lax.rem(me, 2)
        return [
            (base + i + odd * (j - i), experts[i] + odd * (experts[j] - experts[i]))
            for i, j in [(i, i + 1 - 2 * (i % 2)) for i in range(quarter)]
        ]

    def cross(batch, places=None):
        for p in range(1, n_pair):
            for k, _ in in_order(batch, places):
                cross_send[p, k] = (own_acc[p, k] + sib_recv[p, k].astype(f32)).astype(bf16)
                start(cross_copy(k, p))

    def met(batch, parts):
        for p in parts:
            sib_copy(batch[0], p).wait_recv()

    def finish(batch, places=None):
        for k, expert in in_order(batch, places):
            total = own_acc[0, k] + sib_recv[0, k].astype(f32)
            for p in range(1, n_pair):
                cross_copy(k, p).wait_recv()
                total += cross_recv[p, k].astype(f32)
            final_send[k] = total.astype(bf16)
            start(remote(final_send.at[k], returned.at[k],
                         send_sem.at[7], final_recv_sem.at[0], expert, sibling))

    def mix_forward():
        for p in range(1, n_pair):
            mix_pairs[p].wait_recv()
            mix_cross[p] = (
                mix_send[mix_own(p)].astype(f32) + mix_sib[p].astype(f32)
            ).astype(bf16)
            start(mix_copy(p))

    def mix_copy(p):
        return remote(mix_cross.at[p], mix_recv.at[p],
                      send_sem.at[8], mix_recv_sem.at[p], me, 2 * pair_up[p] + 1 - core)

    def mix_finish():
        mix_pairs[0].wait_recv()
        mixed = mix_send[mix_own(0)].astype(f32) + mix_sib[0].astype(f32)
        for p in range(1, n_pair):
            mix_copy(p).wait_recv()
            mixed += mix_recv[p].astype(f32)
        mixer_ref[...] = mixed.astype(mixer_ref.dtype)

    others, rest = range(1, n_pair), range(1, quarter)
    forward_far(0)
    forward_near(0)
    forward_far(1)
    relay_far(0)
    mix_forward()
    loads[9].wait()
    loads[10].wait()
    gather(0)
    expand()
    loads[11].wait()
    for p in others:
        give(0, p)
    relay_far(1)
    forward_near(1)
    for p in others:
        keep(0, p)
    give(0, 0)
    met(far_batches[0], others)
    cross(far_batches[0])
    keep(0, 0)
    gather(1)
    met(near_batches[0], others)
    cross(near_batches[0], rest)
    expand()
    for p in others:
        give(1, p)
        keep(1, p)
    give(1, 0)
    swap = middle * (1 - me // half_count)

    def mixed(one, two):
        return (
            one[0] + swap * (two[0] - one[0]),
            [first + swap * (second - first) for first, second in zip(one[1], two[1])],
        )

    sooner = mixed(far_batches[1], near_batches[1])
    later = mixed(near_batches[1], far_batches[1])
    met(sooner, others)
    cross(sooner)
    met(far_batches[0], [0])
    finish(far_batches[0])
    met(later, others)
    cross(later)
    keep(1, 0)
    cross(near_batches[0], [0])
    met(near_batches[0], [0])
    finish(near_batches[0], rest)
    met(sooner, [0])
    finish(sooner)
    mix_finish()
    met(later, [0])
    finish(later)
    finish(near_batches[0], [0])

    arrived(returned, final_recv_sem.at[0])
    blocks = returned[...].reshape(n_ep * blocked, piece)

    def combined(weights_ref):
        return lax.dot_general(
            weights_ref[...], blocks, (((0,), (0,)), ((), ())), preferred_element_type=f32
        )

    expert_ref[:, :piece] = combined(combine_left).astype(expert_ref.dtype)
    if tail:
        expert_ref[:, piece:] = combined(combine_right).astype(expert_ref.dtype)

    @pl.when(me < n_ep - 1)
    def _():
        to_right.wait_send()

    @pl.when(me > 0)
    def _():
        to_left.wait_send()

    far_count = n_ep - half_count
    arrived(packed.at[0, pl.ds(0, far_count)], send_sem.at[0])
    arrived(packed.at[:, pl.ds(0, half_count - 1)], send_sem.at[1])
    arrived(rows_in.at[pl.ds(0, n_pair), pl.ds(0, n_ep - 1)], send_sem.at[2])
    if n_pair > 1:
        arrived(rows_in.at[pl.ds(0, n_pair - 1), pl.ds(0, far_count)], send_sem.at[3])
    arrived(mix_sib, send_sem.at[4])
    if n_pair > 1:
        arrived(mix_cross.at[pl.ds(0, n_pair - 1)], send_sem.at[8])
    arrived(sib_send, send_sem.at[5])
    if n_pair > 1:
        arrived(cross_send.at[pl.ds(0, n_pair - 1)], send_sem.at[6])
    arrived(final_send, send_sem.at[7])


def write_kernel(mixer_in, expert_in, mixer_out, expert_out, sem):
    copies = [
        pltpu.make_async_copy(mixer_in, mixer_out, sem.at[0]),
        pltpu.make_async_copy(expert_in, expert_out, sem.at[1]),
    ]
    for copy in copies:
        copy.start()
    for copy in copies:
        copy.wait()


def on_device(
    queries,
    key_states,
    value_states,
    sink_logit,
    out_weight,
    expert_input,
    norm_gain,
    routes,
    route_weight,
    gate_weight,
    up_weight,
    down_weight,
):
    n_ep = lax.axis_size("ep")
    n_tp = lax.axis_size("tp")
    row_count, width = expert_input.shape
    local_heads = queries.shape[1] // HEAD_DIM
    capacity = row_count * TOP * 5 // (4 * n_ep)
    main, tail = capacity // 16 * 16, 0
    if 0 < capacity - main <= 8 and width // n_tp >= 2 * LANES and main:
        tail = 8
    elif capacity > main:
        main += 16
    halves = 2 if tail else 1
    slice_width = width // n_tp
    piece = slice_width // halves
    blocked = halves * (main + tail)
    hidden_width = gate_weight.shape[2]
    mix_rows = row_count // n_tp
    n_pair = n_tp // 2
    group_rows = n_ep // 2 * (main + tail)
    if queries.shape[1] % LANES:
        queries = jnp.pad(queries, ((0, 0), (0, LANES - queries.shape[1] % LANES)))
    table = jnp.asarray(angle_table(row_count, n_ep))
    vmem = pl.BlockSpec(memory_space=pltpu.VMEM)
    hbm = pl.BlockSpec(memory_space=pltpu.HBM)
    bf16, f32 = jnp.bfloat16, jnp.float32
    dma = pltpu.SemaphoreType.DMA
    traveling = (blocked, piece)
    operands = (
        queries,
        key_states,
        value_states,
        table,
        sink_logit[None, :],
        expert_input,
        norm_gain[None, :],
        routes.T,
        route_weight.T,
        out_weight,
        gate_weight,
        up_weight,
        down_weight,
    )
    mixer_out, expert_out = pl.pallas_call(
        functools.partial(fused_kernel, (n_ep, n_tp, main, tail)),
        out_shape=(
            jax.ShapeDtypeStruct((mix_rows, width), bf16),
            jax.ShapeDtypeStruct((row_count, slice_width), bf16),
        ),
        in_specs=[hbm] * 13,
        out_specs=(vmem, vmem),
        scratch_shapes=[
            pltpu.VMEM(queries.shape, bf16),
            pltpu.VMEM((row_count, LANES), bf16),
            pltpu.VMEM((row_count, LANES), bf16),
            pltpu.VMEM(table.shape, f32),
            pltpu.VMEM((1, local_heads), f32),
            pltpu.VMEM(expert_input.shape, bf16),
            pltpu.VMEM((1, width), f32),
            pltpu.VMEM((TOP, row_count), jnp.int32),
            pltpu.VMEM((TOP, row_count), f32),
            pltpu.VMEM(out_weight.shape, bf16),
            pltpu.VMEM(gate_weight.shape[1:], bf16),
            pltpu.VMEM(up_weight.shape[1:], bf16),
            pltpu.VMEM(down_weight.shape[1:], bf16),
            pltpu.VMEM(expert_input.shape, bf16),
            pltpu.VMEM((row_count, LANES), bf16),
            pltpu.VMEM((row_count, LANES), bf16),
            pltpu.VMEM((WINDOW, LANES), bf16),
            pltpu.VMEM((WINDOW, LANES), bf16),
            pltpu.VMEM((n_pair, n_ep) + traveling, bf16),
            pltpu.VMEM((n_tp, n_ep) + traveling, bf16),
            pltpu.VMEM((group_rows, width), bf16),
            pltpu.VMEM((group_rows, hidden_width), bf16),
            pltpu.VMEM((n_tp, mix_rows, width), bf16),
            pltpu.VMEM((n_pair, mix_rows, width), bf16),
            pltpu.VMEM((n_pair, mix_rows, width), bf16),
            pltpu.VMEM((n_pair, mix_rows, width), bf16),
            pltpu.VMEM((n_pair, n_ep) + traveling, bf16),
            pltpu.VMEM((n_pair, n_ep) + traveling, bf16),
            pltpu.VMEM((n_pair, n_ep) + traveling, f32),
            pltpu.VMEM((n_pair, n_ep) + traveling, bf16),
            pltpu.VMEM((n_pair, n_ep) + traveling, bf16),
            pltpu.VMEM((n_ep,) + traveling, bf16),
            pltpu.VMEM((n_ep,) + traveling, bf16),
            pltpu.VMEM((n_ep * blocked, row_count), bf16),
            pltpu.VMEM((n_ep * blocked, row_count), bf16),
            dma((13,)),
            dma((2,)),
            dma((2,)),
            dma((9,)),
            dma((n_ep,)),
            dma((n_pair - 1, n_ep // 2)),
            dma((4,)),
            dma((n_pair,)),
            dma((n_pair,)),
            dma((n_pair, 4)),
            dma((n_pair - 1, n_ep)),
            dma((1,)),
        ],
        compiler_params=pltpu.CompilerParams(
            collective_id=0, has_side_effects=True, vmem_limit_bytes=50000 * 1024
        ),
    )(*[
        pltpu.with_memory_space_constraint(operand, pltpu.HBM) if operand.size > 1 else operand
        for operand in operands
    ])
    return pl.pallas_call(
        write_kernel,
        out_shape=(
            jax.ShapeDtypeStruct(mixer_out.shape, bf16),
            jax.ShapeDtypeStruct(expert_out.shape, bf16),
        ),
        in_specs=[vmem] * 2,
        out_specs=(hbm, hbm),
        scratch_shapes=[dma((2,))],
        compiler_params=pltpu.CompilerParams(vmem_limit_bytes=1024 * 1024),
    )(*[pltpu.with_memory_space_constraint(x, pltpu.VMEM) for x in (mixer_out, expert_out)])


def solution(mesh):
    in_specs = (
        P("ep", "tp"),
        P("ep", None),
        P("ep", None),
        P("tp"),
        P("tp", None),
        P("ep", None),
        P(),
        P("ep", None),
        P("ep", None),
        P("ep", None, "tp"),
        P("ep", None, "tp"),
        P("ep", "tp", None),
    )
    out_specs = (P(("ep", "tp"), None), P("ep", "tp"))
    return jax.shard_map(
        on_device, mesh=mesh, in_specs=in_specs, out_specs=out_specs, check_vma=False
    )
```

```python
import functools

import jax
import jax.numpy as jnp
import numpy as np
from jax import lax
from jax.experimental import pallas as pl
from jax.experimental.pallas import tpu as pltpu
from jax.sharding import PartitionSpec as P

HEADS = 16
KV_HEADS = 4
HEAD_DIM = 64
WINDOW = 128
TOP = 2
LANES = 128


NORM_EPSILON = 1e-05
ROTARY_BASE = 500000.0
MASK_VALUE = -1e30


def layer_norm(activations, norm_gain):
    values = activations.astype(jnp.float32)
    average = jnp.mean(values, axis=-1, keepdims=True)
    centred = values - average
    variance = jnp.mean(centred * centred, axis=-1, keepdims=True)
    return (centred * lax.rsqrt(variance + NORM_EPSILON) * norm_gain).astype(jnp.bfloat16)


def angle_table(row_count, blocks):
    lane = np.arange(LANES) % HEAD_DIM
    half_dim = HEAD_DIM // 2
    frequency = ROTARY_BASE ** (-2.0 * (lane % half_dim) / HEAD_DIM)
    sign = np.where(lane < half_dim, -1.0, 1.0)
    rows = np.arange(row_count)[:, None] * frequency[None, :]
    bases = np.arange(blocks)[:, None] * row_count * frequency[None, :]
    return np.concatenate(
        [np.cos(rows), sign * np.sin(rows), np.cos(bases), sign * np.sin(bases)]
    ).astype(np.float32)


def partner(index, mask):
    flipped, bit = index, 1
    while bit <= mask:
        if mask & bit:
            flipped = flipped + bit * (1 - 2 * lax.rem(index // bit, 2))
        bit *= 2
    return flipped


def fused_kernel(
    sizes,
    query_hbm,
    key_hbm,
    value_hbm,
    table_hbm,
    sink_hbm,
    input_hbm,
    gain_hbm,
    routes_hbm,
    route_weight_hbm,
    out_hbm,
    gate_hbm,
    up_hbm,
    down_hbm,
    mixer_ref,
    expert_ref,
    query_v,
    key_v,
    value_v,
    table_v,
    sink_v,
    input_v,
    gain_v,
    routes_v,
    route_weight_v,
    out_w,
    gate_w,
    up_w,
    down_w,
    normed_v,
    own_kv,
    halo_send,
    low_kv,
    high_kv,
    packed,
    rows_in,
    gathered,
    hidden,
    mix_send,
    mix_sib,
    mix_cross,
    mix_recv,
    sib_send,
    sib_recv,
    own_acc,
    cross_send,
    cross_recv,
    final_send,
    returned,
    combine_left,
    combine_right,
    load_sem,
    halo_send_sem,
    halo_recv_sem,
    send_sem,
    net_recv_sem,
    far_recv_sem,
    near_recv_sem,
    mix_sib_recv_sem,
    mix_recv_sem,
    sib_recv_sem,
    cross_recv_sem,
    final_recv_sem,
):
    n_ep, n_tp, main, tail = sizes
    cap = main + tail
    halves = 2 if tail else 1
    f32, bf16 = jnp.float32, jnp.bfloat16
    me, my_tp = lax.axis_index("ep"), lax.axis_index("tp")
    core = lax.rem(my_tp, 2)
    pair = my_tp // 2
    n_pair = n_tp // 2
    sibling = my_tp + 1 - 2 * core
    row_count, width = input_v.shape
    slice_width = width // n_tp
    piece = slice_width // halves
    head_dim = HEAD_DIM
    local_heads = sink_v.shape[1]
    half_count = n_ep // 2
    quarter = n_ep // 4
    experts_of = [partner(me, k) for k in range(n_ep)]
    middle = lax.rem(me // half_count + me // quarter, 2)
    bases = [half_count + quarter * (1 - middle), half_count + quarter * middle]
    far_experts = [
        [
            experts_of[half_count + quarter * place + i]
            + middle * (experts_of[half_count + quarter * (1 - place) + i]
                        - experts_of[half_count + quarter * place + i])
            for i in range(quarter)
        ]
        for place in (1, 0)
    ]
    far_batches = [(bases[place], far_experts[place]) for place in range(2)]
    swap = middle * (1 - me // half_count)

    def mixed(one, two):
        return (
            one[0] + swap * (two[0] - one[0]),
            [first + swap * (second - first) for first, second in zip(one[1], two[1])],
        )

    near_lists = [list(range(quarter)), list(range(quarter, half_count))]
    near_pair = [(slots[0], [experts_of[k] for k in slots]) for slots in near_lists]
    near_batches = [mixed(near_pair[0], near_pair[1]), mixed(near_pair[1], near_pair[0])]
    groups = [(far_batches[place], near_batches[place]) for place in range(2)]
    pair_up = [lax.rem(pair + p, n_pair) for p in range(n_pair)]
    pair_down = [lax.rem(pair + n_pair - p, n_pair) for p in range(n_pair)]

    names = [
        (routes_hbm, routes_v),
        (route_weight_hbm, route_weight_v),
        (gain_hbm, gain_v),
        (input_hbm, input_v),
        (table_hbm, table_v),
        (key_hbm, key_v),
        (value_hbm, value_v),
        (query_hbm, query_v),
        (out_hbm, out_w),
        (gate_hbm.at[0], gate_w),
        (up_hbm.at[0], up_w),
        (down_hbm.at[0], down_w),
        (sink_hbm, sink_v),
    ]
    shared = my_tp * local_heads // (HEADS // KV_HEADS)
    shared_sib = sibling * local_heads // (HEADS // KV_HEADS)
    block = pl.ds(pl.multiple_of(shared // 2 * LANES, LANES), LANES)
    names[5] = (key_hbm.at[:, block], key_v)
    names[6] = (value_hbm.at[:, block], value_v)
    loads = [
        pltpu.make_async_copy(source, target, load_sem.at[number])
        for number, (source, target) in enumerate(names)
    ]

    def remote(source, target, send_sem, recv_sem, ep, tp):
        return pltpu.make_async_remote_copy(
            src_ref=source,
            dst_ref=target,
            send_sem=send_sem,
            recv_sem=recv_sem,
            device_id=(ep, tp),
            device_id_type=pl.DeviceIdType.MESH,
        )

    barrier = pltpu.get_barrier_semaphore()
    for k in range(n_ep - 1, 0, -1):
        pl.semaphore_signal(
            barrier, inc=1, device_id=(experts_of[k], sibling),
            device_id_type=pl.DeviceIdType.MESH,
        )
    for step in range(1, n_tp):
        pl.semaphore_signal(
            barrier, inc=1, device_id=(me, lax.rem(my_tp + step, n_tp)),
            device_id_type=pl.DeviceIdType.MESH,
        )
    for number in [0, 2, 3, 4, 5, 6, 7, 12, 1, 8, 9, 10, 11]:
        loads[number].start()

    def start(copy):
        copy.start()

    def arrived(target, sem):
        pltpu.make_async_copy(target, target, sem).wait()

    loads[0].wait()
    routes = [routes_v[k : k + 1, :] for k in range(TOP)]
    expert_iota = lax.broadcasted_iota(jnp.int32, (n_ep, row_count), 0)
    named = [(routes[k] == expert_iota).astype(f32) for k in range(TOP)]
    earlier = (
        lax.broadcasted_iota(jnp.int32, (row_count, row_count), 0)
        < lax.broadcasted_iota(jnp.int32, (row_count, row_count), 1)
    )
    ahead = jnp.dot(
        functools.reduce(jnp.add, named).astype(bf16),
        earlier.astype(f32).astype(bf16),
        preferred_element_type=f32,
    )
    rank = [
        jnp.sum(ahead * named[k], axis=0, keepdims=True).astype(jnp.int32) for k in range(TOP)
    ]

    def slot_onehot(k):
        slot = lax.broadcasted_iota(jnp.int32, (cap, row_count), 0)
        chosen = [(jnp.where(routes[j] == experts_of[k], rank[j], -1) == slot) for j in range(TOP)]
        return functools.reduce(jnp.logical_or, chosen).astype(f32)

    def pack(values):
        if not tail:
            return values
        parts = [values[:main, :piece], values[:main, piece:], values[main:, :piece], values[main:, piece:]]
        return jnp.concatenate(parts, axis=0)

    far = list(range(half_count, n_ep))
    close = list(range(half_count))
    for number in range(4, 7):
        loads[number].wait()
    lane = lax.broadcasted_iota(jnp.int32, (row_count, LANES), 1)
    low_lane = lane < head_dim
    first_half = lax.rem(lane, head_dim) < head_dim // 2
    row_cos, row_sin = table_v[:row_count], table_v[row_count : 2 * row_count]
    base_cos = table_v[pl.ds(2 * row_count + me, 1), :]
    base_sin = table_v[pl.ds(2 * row_count + n_ep + me, 1), :]
    cosine = base_cos * row_cos - base_sin * row_sin
    sine = base_sin * row_cos + base_cos * row_sin

    def turn(values):
        values = values.astype(f32)
        other = jnp.where(
            first_half,
            pltpu.roll(values, LANES - head_dim // 2, 1),
            pltpu.roll(values, head_dim // 2, 1),
        )
        return values * cosine + other * sine

    turned = turn(key_v[...])
    value = value_v[...].astype(f32)
    turned_roll, value_roll = pltpu.roll(turned, head_dim, 1), pltpu.roll(value, head_dim, 1)

    def key_value(head):
        upper = lax.rem(head, 2) == 1
        return jnp.where(
            low_lane,
            jnp.where(upper, turned_roll, turned),
            jnp.where(upper, value, value_roll),
        ).astype(bf16)

    own_kv[...] = key_value(shared)
    halo_send[...] = key_value(shared_sib)
    to_right = remote(halo_send.at[pl.ds(row_count - WINDOW, WINDOW)], low_kv,
                      halo_send_sem.at[0], halo_recv_sem.at[0], lax.rem(me + 1, n_ep), sibling)
    to_left = remote(halo_send.at[pl.ds(0, WINDOW)], high_kv,
                     halo_send_sem.at[1], halo_recv_sem.at[1], lax.rem(me + n_ep - 1, n_ep), sibling)

    far_onehot = jnp.concatenate([slot_onehot(k) for k in far], axis=0).astype(bf16)
    close_onehot = jnp.concatenate([slot_onehot(k) for k in close], axis=0).astype(bf16)

    loads[2].wait()
    loads[3].wait()
    normed_v[...] = layer_norm(input_v[...], gain_v[...])

    def columns_of(owner, size):
        return pl.ds(pl.multiple_of(owner * size, size), size)

    own_slice = normed_v[:, columns_of(my_tp, slice_width)]
    slots = jnp.dot(far_onehot, own_slice, preferred_element_type=f32)
    for place, k in enumerate(far):
        packed[0, k] = pack(slots[place * cap : (place + 1) * cap]).astype(bf16)

    pl.semaphore_wait(barrier, n_ep + n_tp - 2)

    def net(k, expert, q, sem):
        owner = 2 * pair_up[q] + core
        return remote(packed.at[q, k], rows_in.at[owner, k],
                      send_sem.at[sem], net_recv_sem.at[k], expert, sibling)

    @pl.when(me < n_ep - 1)
    def _():
        to_right.start()

    @pl.when(me > 0)
    def _():
        to_left.start()

    @pl.when(me == 0)
    def _():
        low_kv[...] = jnp.zeros_like(low_kv)

    @pl.when(me == n_ep - 1)
    def _():
        high_kv[...] = jnp.zeros_like(high_kv)

    for base, experts in far_batches:
        for i, expert in enumerate(experts):
            start(net(base + i, expert, 0, 0))

    for q in range(n_pair):
        for side in range(2):
            owner = 2 * pair_up[q] + (core if side == 0 else 1 - core)
            rows = close_onehot if side == 0 else close_onehot[:cap]
            slots = jnp.dot(rows, normed_v[:, columns_of(owner, slice_width)], preferred_element_type=f32)
            rows_in[owner, 0] = pack(slots[:cap]).astype(bf16)
            if side == 0:
                for place, k in enumerate(close[1:]):
                    place = (place + 1) * cap
                    packed[q, k] = pack(slots[place : place + cap]).astype(bf16)

    for k in close[1:]:
        for q in range(n_pair):
            start(net(k, experts_of[k], q, 1))

    loads[12].wait()
    loads[7].wait()
    query = [
        turn(query_v[:, pl.ds(column, LANES)]) for column in range(0, query_v.shape[1], LANES)
    ]
    local = lax.broadcasted_iota(jnp.int32, (row_count, WINDOW), 0)
    other = lax.broadcasted_iota(jnp.int32, (row_count, WINDOW), 1)

    def split_heads(packed_rows):
        both = packed_rows.astype(f32)
        swapped = pltpu.roll(both, head_dim, 1)
        low = lax.broadcasted_iota(jnp.int32, both.shape, 1) < head_dim
        return jnp.where(low, both, swapped).astype(bf16), jnp.where(low, swapped, both).astype(bf16)

    own_rows = jnp.abs(
        lax.broadcasted_iota(jnp.int32, (row_count, row_count), 0)
        - lax.broadcasted_iota(jnp.int32, (row_count, row_count), 1)
    ) <= WINDOW
    own_keys, own_values = split_heads(own_kv[...])
    head_queries, own_scores = [], []

    def score(head_query, keys, allowed):
        scores = lax.dot_general(
            head_query, keys, (((1,), (1,)), ((), ())), preferred_element_type=f32
        ) * head_dim ** (-0.5)
        return jnp.where(allowed, scores, MASK_VALUE)

    for head in range(local_heads):
        mine = low_lane if head % 2 == 0 else jnp.logical_not(low_lane)
        head_queries.append(jnp.where(mine, query[head // 2], 0.0).astype(bf16))
        own_scores.append(score(head_queries[head], own_keys, own_rows))

    @pl.when(me > 0)
    def _():
        to_right.wait_recv()

    @pl.when(me < n_ep - 1)
    def _():
        to_left.wait_recv()

    low_allowed = (local - (other - WINDOW) <= WINDOW) & (me > 0)
    high_allowed = (row_count + other - local <= WINDOW) & (me < n_ep - 1)
    low_keys, low_values = split_heads(low_kv[...])
    high_keys, high_values = split_heads(high_kv[...])
    values = jnp.concatenate([low_values, own_values, high_values], axis=0)
    blocks = []
    for head in range(local_heads):
        parts = [
            score(head_queries[head], low_keys, low_allowed),
            own_scores[head],
            score(head_queries[head], high_keys, high_allowed),
        ]
        sink = sink_v[:, head : head + 1]
        highest = [jnp.max(part, axis=-1, keepdims=True) for part in parts]
        if row_count == WINDOW:
            highest = [jnp.max(functools.reduce(jnp.maximum, parts), axis=-1, keepdims=True)]
        largest = functools.reduce(jnp.maximum, highest + [sink])
        weights = [jnp.exp(part - largest) for part in parts]
        totals = [jnp.sum(weight, axis=-1, keepdims=True) for weight in weights]
        if row_count == WINDOW:
            totals = [jnp.sum(functools.reduce(jnp.add, weights), axis=-1, keepdims=True)]
        denominator = functools.reduce(jnp.add, totals) + jnp.exp(sink - largest)
        scale = 1.0 / denominator
        probability = jnp.concatenate([(weight * scale).astype(bf16) for weight in weights], axis=1)
        result = jnp.dot(probability, values, preferred_element_type=f32)
        if head % 2 == 0:
            blocks.append(result)
        else:
            blocks[-1] = jnp.where(low_lane, blocks[-1], result)
    attended = jnp.concatenate(blocks, axis=1).astype(bf16)[:, : local_heads * head_dim]
    loads[8].wait()
    partial_sum = jnp.dot(attended, out_w[...], preferred_element_type=f32)
    mix_send[...] = partial_sum.reshape(mix_send.shape).astype(bf16)

    def mix_own(p):
        return 2 * pair_up[p] + (core if p == 0 else 1 - core)

    def mix_other(p):
        return 2 * pair_up[p] + (1 - core if p == 0 else core)

    mix_pairs = [
        remote(mix_send.at[mix_other(p)], mix_sib.at[p],
               send_sem.at[4], mix_sib_recv_sem.at[p], me, sibling)
        for p in range(n_pair)
    ]
    for p in list(range(1, n_pair)) + [0]:
        start(mix_pairs[p])

    loads[1].wait()
    blocked = halves * cap
    number = lax.broadcasted_iota(jnp.int32, (blocked, row_count), 0)
    slot_of = number
    left = number >= 0
    if tail:
        in_main = number < 2 * main
        slot_of = jnp.where(
            in_main,
            jnp.where(number < main, number, number - main),
            jnp.where(number < 2 * main + tail, number - main, number - main - tail),
        )
        left = (number < main) | (jnp.logical_not(in_main) & (number < 2 * main + tail))
    for k in range(n_ep):
        placed = jnp.zeros((blocked, row_count), f32)
        for j in range(TOP):
            chosen = jnp.where(routes[j] == experts_of[k], rank[j], -1) == slot_of
            placed = jnp.where(chosen, route_weight_v[j : j + 1, :], placed)
        combine_left[pl.ds(k * blocked, blocked)] = jnp.where(left, placed, 0.0).astype(bf16)
        if tail:
            combine_right[pl.ds(k * blocked, blocked)] = jnp.where(left, 0.0, placed).astype(bf16)

    def near_forward(k, q, sem):
        owner = 2 * pair_up[q] + 1 - core
        return remote(rows_in.at[owner, k], rows_in.at[owner, k],
                      send_sem.at[2], near_recv_sem.at[sem], me, sibling)

    def far_forward(k, p):
        owner = 2 * pair + 1 - core
        return remote(rows_in.at[owner, k], rows_in.at[owner, k],
                      send_sem.at[3], far_recv_sem.at[p - 1, k - half_count], me, 2 * pair_up[p] + 1 - core)

    def far_relay(k, p, sem):
        owner = 2 * pair_down[p] + core
        return remote(rows_in.at[owner, k], rows_in.at[owner, k],
                      send_sem.at[2], near_recv_sem.at[sem], me, sibling)

    def forward_far(number):
        base, experts = far_batches[number]
        for i, expert in enumerate(experts):
            net(base + i, expert, 0, 0).wait_recv()
            for p in range(1, n_pair):
                start(far_forward(base + i, p))
            start(near_forward(base + i, 0, number))

    def relay_far(number):
        base, experts = far_batches[number]
        for i in range(len(experts)):
            for p in range(1, n_pair):
                far_forward(base + i, p).wait_recv()
                start(far_relay(base + i, p, number))

    def either(number, action):
        for swapped in range(2):
            @pl.when(swap == swapped)
            def _():
                action([k for k in near_lists[(number + swapped) % 2] if k])

    def forward_near(number):
        def action(slots):
            for k in slots:
                arrived(rows_in.at[pl.ds(0, n_pair), k], net_recv_sem.at[k])
                for q in range(n_pair):
                    start(near_forward(k, q, 2 + number))

        either(number, action)

    def gather(number):
        slots = []
        for base, experts in groups[number]:
            slots += [base + i for i in range(len(experts))]
        arrived(rows_in.at[pl.ds(0, n_pair), pl.ds(0, quarter)], near_recv_sem.at[number])
        either(number, lambda near: arrived(
            rows_in.at[pl.ds(0, n_pair), pl.ds(0, len(near))], near_recv_sem.at[2 + number]
        ))
        for owner in range(n_tp):
            for half in range(halves):
                columns = pl.ds(owner * slice_width + half * piece, piece)
                for place, k in enumerate(slots):
                    gathered[pl.ds(place * main, main), columns] = (
                        rows_in[owner, k, pl.ds(half * main, main), :]
                    )
                if tail:
                    ends = [
                        rows_in[owner, k, pl.ds(2 * main, 2 * tail), :].astype(f32)[
                            half * tail : (half + 1) * tail
                        ]
                        for k in slots
                    ]
                    gathered[pl.ds(len(slots) * main, len(slots) * tail), columns] = (
                        jnp.concatenate(ends, axis=0).astype(bf16)
                    )

    hidden_width = gate_w.shape[1]
    tile = min(hidden_width, 512)

    rows = half_count * cap

    def expand():
        for number in range(hidden_width // tile):
            columns = pl.ds(number * tile, tile)
            gate_act = jnp.dot(gathered[...], gate_w[:, columns], preferred_element_type=f32)
            up_act = jnp.dot(gathered[...], up_w[:, columns], preferred_element_type=f32)
            hidden[:, columns] = (gate_act / (1.0 + jnp.exp(-gate_act)) * up_act).astype(bf16)

    def down_slice(number, owner):
        result = jnp.dot(
            hidden[...], down_w[:, columns_of(owner, slice_width)], preferred_element_type=f32
        )
        slots = [base + i for base, experts in groups[number] for i in range(len(experts))]
        for place, k in enumerate(slots):
            values = result[place * main : (place + 1) * main]
            if tail:
                last = half_count * main + place * tail
                values = jnp.concatenate([values, result[last : last + tail]], axis=0)
            yield k, pack(values)

    def sib_copy(base, p):
        batch = pl.ds(base, quarter)
        return remote(sib_send.at[p, batch], sib_recv.at[p, batch],
                      send_sem.at[5], sib_recv_sem.at[p, base // quarter], me, sibling)

    def cross_copy(k, p):
        return remote(cross_send.at[p, k], cross_recv.at[p, k],
                      send_sem.at[6], cross_recv_sem.at[p - 1, k], me, 2 * pair_up[p] + 1 - core)

    def give(number, p):
        owner = 2 * pair_up[p] + (core if p == 0 else 1 - core)
        for k, values in down_slice(number, owner):
            sib_send[p, k] = values.astype(bf16)
        for base, _ in groups[number]:
            start(sib_copy(base, p))

    def keep(number, p):
        owner = 2 * pair_up[p] + (1 - core if p == 0 else core)
        for k, values in down_slice(number, owner):
            own_acc[p, k] = values

    def in_order(batch):
        base, experts = batch
        if quarter % 2:
            return [(base + i, experts[i]) for i in range(quarter)]
        odd = lax.rem(me, 2)
        return [
            (base + i + odd * (j - i), experts[i] + odd * (experts[j] - experts[i]))
            for i, j in [(i, i + 1 - 2 * (i % 2)) for i in range(quarter)]
        ]

    outer = in_order(near_pair[1])
    inner = [(k, experts_of[k]) for k in range(1, quarter)]
    own = [(0, me)]

    def cross(slots):
        for p in range(1, n_pair):
            for k, _ in slots:
                cross_send[p, k] = (own_acc[p, k] + sib_recv[p, k].astype(f32)).astype(bf16)
                start(cross_copy(k, p))

    def met(batch, parts):
        for p in parts:
            sib_copy(batch[0], p).wait_recv()

    def finish(slots):
        for k, expert in slots:
            total = own_acc[0, k] + sib_recv[0, k].astype(f32)
            for p in range(1, n_pair):
                cross_copy(k, p).wait_recv()
                total += cross_recv[p, k].astype(f32)
            final_send[k] = total.astype(bf16)
            start(remote(final_send.at[k], returned.at[k],
                         send_sem.at[7], final_recv_sem.at[0], expert, sibling))

    def mix_forward():
        for p in range(1, n_pair):
            mix_pairs[p].wait_recv()
            mix_cross[p] = (
                mix_send[mix_own(p)].astype(f32) + mix_sib[p].astype(f32)
            ).astype(bf16)
            start(mix_copy(p))

    def mix_copy(p):
        return remote(mix_cross.at[p], mix_recv.at[p],
                      send_sem.at[8], mix_recv_sem.at[p], me, 2 * pair_up[p] + 1 - core)

    def mix_finish():
        mix_pairs[0].wait_recv()
        mixed = mix_send[mix_own(0)].astype(f32) + mix_sib[0].astype(f32)
        for p in range(1, n_pair):
            mix_copy(p).wait_recv()
            mixed += mix_recv[p].astype(f32)
        mixer_ref[...] = mixed.astype(mixer_ref.dtype)

    others = range(1, n_pair)
    forward_far(0)
    forward_far(1)
    relay_far(0)
    mix_forward()
    forward_near(0)
    loads[9].wait()
    loads[10].wait()
    gather(0)
    expand()
    loads[11].wait()
    for p in others:
        give(0, p)
    relay_far(1)
    forward_near(1)
    for p in others:
        keep(0, p)
    give(0, 0)
    def where(swapped, action, slots):
        @pl.when(swap == swapped)
        def _():
            action(slots)

    far_slots = [in_order(batch) for batch in far_batches]
    met(far_batches[0], others)
    cross(far_slots[0])
    keep(0, 0)
    gather(1)
    met(near_batches[0], others)
    where(0, cross, inner)
    where(1, cross, outer)
    expand()
    for p in others:
        give(1, p)
        keep(1, p)
    give(1, 0)
    met(far_batches[1], others)
    met(near_batches[1], others)
    where(1, cross, inner)
    cross(far_slots[1])
    met(far_batches[0], [0])
    finish(far_slots[0])
    where(0, cross, outer)
    cross(own)
    keep(1, 0)
    met(near_batches[0], [0])
    where(0, finish, inner)
    where(1, finish, outer)
    met(far_batches[1], [0])
    met(near_batches[1], [0])
    where(1, finish, inner)
    finish(far_slots[1])
    mix_finish()
    where(0, finish, outer)
    finish(own)

    arrived(returned, final_recv_sem.at[0])
    blocks = returned[...].reshape(n_ep * blocked, piece)

    def combined(weights_ref):
        return lax.dot_general(
            weights_ref[...], blocks, (((0,), (0,)), ((), ())), preferred_element_type=f32
        )

    expert_ref[:, :piece] = combined(combine_left).astype(expert_ref.dtype)
    if tail:
        expert_ref[:, piece:] = combined(combine_right).astype(expert_ref.dtype)

    @pl.when(me < n_ep - 1)
    def _():
        to_right.wait_send()

    @pl.when(me > 0)
    def _():
        to_left.wait_send()

    far_count = n_ep - half_count
    arrived(packed.at[0, pl.ds(0, far_count)], send_sem.at[0])
    arrived(packed.at[:, pl.ds(0, half_count - 1)], send_sem.at[1])
    arrived(rows_in.at[pl.ds(0, n_pair), pl.ds(0, n_ep - 1)], send_sem.at[2])
    if n_pair > 1:
        arrived(rows_in.at[pl.ds(0, n_pair - 1), pl.ds(0, far_count)], send_sem.at[3])
    arrived(mix_sib, send_sem.at[4])
    if n_pair > 1:
        arrived(mix_cross.at[pl.ds(0, n_pair - 1)], send_sem.at[8])
    arrived(sib_send, send_sem.at[5])
    if n_pair > 1:
        arrived(cross_send.at[pl.ds(0, n_pair - 1)], send_sem.at[6])
    arrived(final_send, send_sem.at[7])


def write_kernel(mixer_in, expert_in, mixer_out, expert_out, sem):
    copies = [
        pltpu.make_async_copy(mixer_in, mixer_out, sem.at[0]),
        pltpu.make_async_copy(expert_in, expert_out, sem.at[1]),
    ]
    for copy in copies:
        copy.start()
    for copy in copies:
        copy.wait()


def on_device(
    queries,
    key_states,
    value_states,
    sink_logit,
    out_weight,
    expert_input,
    norm_gain,
    routes,
    route_weight,
    gate_weight,
    up_weight,
    down_weight,
):
    n_ep = lax.axis_size("ep")
    n_tp = lax.axis_size("tp")
    row_count, width = expert_input.shape
    local_heads = queries.shape[1] // HEAD_DIM
    capacity = row_count * TOP * 5 // (4 * n_ep)
    main, tail = capacity // 16 * 16, 0
    if 0 < capacity - main <= 8 and width // n_tp >= 2 * LANES and main:
        tail = 8
    elif capacity > main:
        main += 16
    halves = 2 if tail else 1
    slice_width = width // n_tp
    piece = slice_width // halves
    blocked = halves * (main + tail)
    hidden_width = gate_weight.shape[2]
    mix_rows = row_count // n_tp
    n_pair = n_tp // 2
    group_rows = n_ep // 2 * (main + tail)
    if queries.shape[1] % LANES:
        queries = jnp.pad(queries, ((0, 0), (0, LANES - queries.shape[1] % LANES)))
    table = jnp.asarray(angle_table(row_count, n_ep))
    vmem = pl.BlockSpec(memory_space=pltpu.VMEM)
    hbm = pl.BlockSpec(memory_space=pltpu.HBM)
    bf16, f32 = jnp.bfloat16, jnp.float32
    dma = pltpu.SemaphoreType.DMA
    traveling = (blocked, piece)
    operands = (
        queries,
        key_states,
        value_states,
        table,
        sink_logit[None, :],
        expert_input,
        norm_gain[None, :],
        routes.T,
        route_weight.T,
        out_weight,
        gate_weight,
        up_weight,
        down_weight,
    )
    mixer_out, expert_out = pl.pallas_call(
        functools.partial(fused_kernel, (n_ep, n_tp, main, tail)),
        out_shape=(
            jax.ShapeDtypeStruct((mix_rows, width), bf16),
            jax.ShapeDtypeStruct((row_count, slice_width), bf16),
        ),
        in_specs=[hbm] * 13,
        out_specs=(vmem, vmem),
        scratch_shapes=[
            pltpu.VMEM(queries.shape, bf16),
            pltpu.VMEM((row_count, LANES), bf16),
            pltpu.VMEM((row_count, LANES), bf16),
            pltpu.VMEM(table.shape, f32),
            pltpu.VMEM((1, local_heads), f32),
            pltpu.VMEM(expert_input.shape, bf16),
            pltpu.VMEM((1, width), f32),
            pltpu.VMEM((TOP, row_count), jnp.int32),
            pltpu.VMEM((TOP, row_count), f32),
            pltpu.VMEM(out_weight.shape, bf16),
            pltpu.VMEM(gate_weight.shape[1:], bf16),
            pltpu.VMEM(up_weight.shape[1:], bf16),
            pltpu.VMEM(down_weight.shape[1:], bf16),
            pltpu.VMEM(expert_input.shape, bf16),
            pltpu.VMEM((row_count, LANES), bf16),
            pltpu.VMEM((row_count, LANES), bf16),
            pltpu.VMEM((WINDOW, LANES), bf16),
            pltpu.VMEM((WINDOW, LANES), bf16),
            pltpu.VMEM((n_pair, n_ep) + traveling, bf16),
            pltpu.VMEM((n_tp, n_ep) + traveling, bf16),
            pltpu.VMEM((group_rows, width), bf16),
            pltpu.VMEM((group_rows, hidden_width), bf16),
            pltpu.VMEM((n_tp, mix_rows, width), bf16),
            pltpu.VMEM((n_pair, mix_rows, width), bf16),
            pltpu.VMEM((n_pair, mix_rows, width), bf16),
            pltpu.VMEM((n_pair, mix_rows, width), bf16),
            pltpu.VMEM((n_pair, n_ep) + traveling, bf16),
            pltpu.VMEM((n_pair, n_ep) + traveling, bf16),
            pltpu.VMEM((n_pair, n_ep) + traveling, f32),
            pltpu.VMEM((n_pair, n_ep) + traveling, bf16),
            pltpu.VMEM((n_pair, n_ep) + traveling, bf16),
            pltpu.VMEM((n_ep,) + traveling, bf16),
            pltpu.VMEM((n_ep,) + traveling, bf16),
            pltpu.VMEM((n_ep * blocked, row_count), bf16),
            pltpu.VMEM((n_ep * blocked, row_count), bf16),
            dma((13,)),
            dma((2,)),
            dma((2,)),
            dma((9,)),
            dma((n_ep,)),
            dma((n_pair - 1, n_ep // 2)),
            dma((4,)),
            dma((n_pair,)),
            dma((n_pair,)),
            dma((n_pair, 4)),
            dma((n_pair - 1, n_ep)),
            dma((1,)),
        ],
        compiler_params=pltpu.CompilerParams(
            collective_id=0, has_side_effects=True, vmem_limit_bytes=50000 * 1024
        ),
    )(*[
        pltpu.with_memory_space_constraint(operand, pltpu.HBM) if operand.size > 1 else operand
        for operand in operands
    ])
    return pl.pallas_call(
        write_kernel,
        out_shape=(
            jax.ShapeDtypeStruct(mixer_out.shape, bf16),
            jax.ShapeDtypeStruct(expert_out.shape, bf16),
        ),
        in_specs=[vmem] * 2,
        out_specs=(hbm, hbm),
        scratch_shapes=[dma((2,))],
        compiler_params=pltpu.CompilerParams(vmem_limit_bytes=1024 * 1024),
    )(*[pltpu.with_memory_space_constraint(x, pltpu.VMEM) for x in (mixer_out, expert_out)])


def solution(mesh):
    in_specs = (
        P("ep", "tp"),
        P("ep", None),
        P("ep", None),
        P("tp"),
        P("tp", None),
        P("ep", None),
        P(),
        P("ep", None),
        P("ep", None),
        P("ep", None, "tp"),
        P("ep", None, "tp"),
        P("ep", "tp", None),
    )
    out_specs = (P(("ep", "tp"), None), P("ep", "tp"))
    return jax.shard_map(
        on_device, mesh=mesh, in_specs=in_specs, out_specs=out_specs, check_vma=False
    )
```

```python
import functools

import jax
import jax.numpy as jnp
import numpy as np
from jax import lax
from jax.experimental import pallas as pl
from jax.experimental.pallas import tpu as pltpu
from jax.sharding import PartitionSpec as P

HEADS = 16
KV_HEADS = 4
HEAD_DIM = 64
WINDOW = 128
TOP = 2
LANES = 128


NORM_EPSILON = 1e-05
ROTARY_BASE = 500000.0
MASK_VALUE = -1e30


def layer_norm(activations, norm_gain):
    values = activations.astype(jnp.float32)
    average = jnp.mean(values, axis=-1, keepdims=True)
    centred = values - average
    variance = jnp.mean(centred * centred, axis=-1, keepdims=True)
    return (centred * lax.rsqrt(variance + NORM_EPSILON) * norm_gain).astype(jnp.bfloat16)


def angle_table(row_count, blocks):
    lane = np.arange(LANES) % HEAD_DIM
    half_dim = HEAD_DIM // 2
    frequency = ROTARY_BASE ** (-2.0 * (lane % half_dim) / HEAD_DIM)
    sign = np.where(lane < half_dim, -1.0, 1.0)
    rows = np.arange(row_count)[:, None] * frequency[None, :]
    bases = np.arange(blocks)[:, None] * row_count * frequency[None, :]
    return np.concatenate(
        [np.cos(rows), sign * np.sin(rows), np.cos(bases), sign * np.sin(bases)]
    ).astype(np.float32)


def partner(index, mask):
    flipped, bit = index, 1
    while bit <= mask:
        if mask & bit:
            flipped = flipped + bit * (1 - 2 * lax.rem(index // bit, 2))
        bit *= 2
    return flipped


def fused_kernel(
    sizes,
    query_hbm,
    key_hbm,
    value_hbm,
    table_hbm,
    sink_hbm,
    input_hbm,
    gain_hbm,
    routes_hbm,
    route_weight_hbm,
    out_hbm,
    gate_hbm,
    up_hbm,
    down_hbm,
    mixer_ref,
    expert_ref,
    query_v,
    key_v,
    value_v,
    table_v,
    sink_v,
    input_v,
    gain_v,
    routes_v,
    route_weight_v,
    out_w,
    gate_w,
    up_w,
    down_w,
    normed_v,
    own_kv,
    halo_send,
    low_kv,
    high_kv,
    packed,
    rows_in,
    gathered,
    hidden,
    mix_send,
    mix_sib,
    mix_cross,
    mix_recv,
    sib_send,
    sib_recv,
    own_acc,
    cross_send,
    cross_recv,
    final_send,
    returned,
    combine_left,
    combine_right,
    load_sem,
    halo_send_sem,
    halo_recv_sem,
    send_sem,
    net_recv_sem,
    far_recv_sem,
    near_recv_sem,
    mix_sib_recv_sem,
    mix_recv_sem,
    sib_recv_sem,
    cross_recv_sem,
    final_recv_sem,
):
    n_ep, n_tp, main, tail = sizes
    cap = main + tail
    halves = 2 if tail else 1
    f32, bf16 = jnp.float32, jnp.bfloat16
    me, my_tp = lax.axis_index("ep"), lax.axis_index("tp")
    core = lax.rem(my_tp, 2)
    pair = my_tp // 2
    n_pair = n_tp // 2
    sibling = my_tp + 1 - 2 * core
    row_count, width = input_v.shape
    slice_width = width // n_tp
    piece = slice_width // halves
    head_dim = HEAD_DIM
    local_heads = sink_v.shape[1]
    half_count = n_ep // 2
    quarter = n_ep // 4
    experts_of = [partner(me, k) for k in range(n_ep)]
    middle = lax.rem(me // half_count + me // quarter, 2)
    bases = [half_count + quarter * (1 - middle), half_count + quarter * middle]
    far_experts = [
        [
            experts_of[half_count + quarter * place + i]
            + middle * (experts_of[half_count + quarter * (1 - place) + i]
                        - experts_of[half_count + quarter * place + i])
            for i in range(quarter)
        ]
        for place in (1, 0)
    ]
    far_batches = [(bases[place], far_experts[place]) for place in range(2)]
    swap = middle * (1 - me // half_count)

    def mixed(one, two):
        return (
            one[0] + swap * (two[0] - one[0]),
            [first + swap * (second - first) for first, second in zip(one[1], two[1])],
        )

    near_lists = [list(range(quarter)), list(range(quarter, half_count))]
    near_pair = [(slots[0], [experts_of[k] for k in slots]) for slots in near_lists]
    near_batches = [mixed(near_pair[0], near_pair[1]), mixed(near_pair[1], near_pair[0])]
    groups = [(far_batches[place], near_batches[place]) for place in range(2)]
    pair_up = [lax.rem(pair + p, n_pair) for p in range(n_pair)]
    pair_down = [lax.rem(pair + n_pair - p, n_pair) for p in range(n_pair)]

    names = [
        (routes_hbm, routes_v),
        (route_weight_hbm, route_weight_v),
        (gain_hbm, gain_v),
        (input_hbm, input_v),
        (table_hbm, table_v),
        (key_hbm, key_v),
        (value_hbm, value_v),
        (query_hbm, query_v),
        (out_hbm, out_w),
        (gate_hbm.at[0], gate_w),
        (up_hbm.at[0], up_w),
        (down_hbm.at[0], down_w),
        (sink_hbm, sink_v),
    ]
    shared = my_tp * local_heads // (HEADS // KV_HEADS)
    shared_sib = sibling * local_heads // (HEADS // KV_HEADS)
    block = pl.ds(pl.multiple_of(shared // 2 * LANES, LANES), LANES)
    names[5] = (key_hbm.at[:, block], key_v)
    names[6] = (value_hbm.at[:, block], value_v)
    loads = [
        pltpu.make_async_copy(source, target, load_sem.at[number])
        for number, (source, target) in enumerate(names)
    ]

    def remote(source, target, send_sem, recv_sem, ep, tp):
        return pltpu.make_async_remote_copy(
            src_ref=source,
            dst_ref=target,
            send_sem=send_sem,
            recv_sem=recv_sem,
            device_id=(ep, tp),
            device_id_type=pl.DeviceIdType.MESH,
        )

    barrier = pltpu.get_barrier_semaphore()
    for k in range(n_ep - 1, 0, -1):
        pl.semaphore_signal(
            barrier, inc=1, device_id=(experts_of[k], sibling),
            device_id_type=pl.DeviceIdType.MESH,
        )
    for step in range(1, n_tp):
        pl.semaphore_signal(
            barrier, inc=1, device_id=(me, lax.rem(my_tp + step, n_tp)),
            device_id_type=pl.DeviceIdType.MESH,
        )
    for number in [0, 2, 3, 4, 5, 6, 7, 12, 1, 8, 9, 10, 11]:
        loads[number].start()

    def start(copy):
        copy.start()

    def arrived(target, sem):
        pltpu.make_async_copy(target, target, sem).wait()

    loads[0].wait()
    routes = [routes_v[k : k + 1, :] for k in range(TOP)]
    expert_iota = lax.broadcasted_iota(jnp.int32, (n_ep, row_count), 0)
    named = [(routes[k] == expert_iota).astype(f32) for k in range(TOP)]
    earlier = (
        lax.broadcasted_iota(jnp.int32, (row_count, row_count), 0)
        < lax.broadcasted_iota(jnp.int32, (row_count, row_count), 1)
    )
    ahead = jnp.dot(
        functools.reduce(jnp.add, named).astype(bf16),
        earlier.astype(f32).astype(bf16),
        preferred_element_type=f32,
    )
    rank = [
        jnp.sum(ahead * named[k], axis=0, keepdims=True).astype(jnp.int32) for k in range(TOP)
    ]

    def slot_onehot(k):
        slot = lax.broadcasted_iota(jnp.int32, (cap, row_count), 0)
        chosen = [(jnp.where(routes[j] == experts_of[k], rank[j], -1) == slot) for j in range(TOP)]
        return functools.reduce(jnp.logical_or, chosen).astype(f32)

    def pack(values):
        if not tail:
            return values
        parts = [values[:main, :piece], values[:main, piece:], values[main:, :piece], values[main:, piece:]]
        return jnp.concatenate(parts, axis=0)

    far = list(range(half_count, n_ep))
    close = list(range(half_count))
    for number in range(4, 7):
        loads[number].wait()
    lane = lax.broadcasted_iota(jnp.int32, (row_count, LANES), 1)
    low_lane = lane < head_dim
    first_half = lax.rem(lane, head_dim) < head_dim // 2
    row_cos, row_sin = table_v[:row_count], table_v[row_count : 2 * row_count]
    base_cos = table_v[pl.ds(2 * row_count + me, 1), :]
    base_sin = table_v[pl.ds(2 * row_count + n_ep + me, 1), :]
    cosine = base_cos * row_cos - base_sin * row_sin
    sine = base_sin * row_cos + base_cos * row_sin

    def turn(values):
        values = values.astype(f32)
        other = jnp.where(
            first_half,
            pltpu.roll(values, LANES - head_dim // 2, 1),
            pltpu.roll(values, head_dim // 2, 1),
        )
        return values * cosine + other * sine

    turned = turn(key_v[...])
    value = value_v[...].astype(f32)
    turned_roll, value_roll = pltpu.roll(turned, head_dim, 1), pltpu.roll(value, head_dim, 1)

    def key_value(head):
        upper = lax.rem(head, 2) == 1
        return jnp.where(
            low_lane,
            jnp.where(upper, turned_roll, turned),
            jnp.where(upper, value, value_roll),
        ).astype(bf16)

    own_kv[...] = key_value(shared)
    halo_send[...] = key_value(shared_sib)
    to_right = remote(halo_send.at[pl.ds(row_count - WINDOW, WINDOW)], low_kv,
                      halo_send_sem.at[0], halo_recv_sem.at[0], lax.rem(me + 1, n_ep), sibling)
    to_left = remote(halo_send.at[pl.ds(0, WINDOW)], high_kv,
                     halo_send_sem.at[1], halo_recv_sem.at[1], lax.rem(me + n_ep - 1, n_ep), sibling)

    far_onehot = jnp.concatenate([slot_onehot(k) for k in far], axis=0).astype(bf16)
    close_onehot = jnp.concatenate([slot_onehot(k) for k in close], axis=0).astype(bf16)

    loads[2].wait()
    loads[3].wait()
    normed_v[...] = layer_norm(input_v[...], gain_v[...])

    def columns_of(owner, size):
        return pl.ds(pl.multiple_of(owner * size, size), size)

    own_slice = normed_v[:, columns_of(my_tp, slice_width)]
    slots = jnp.dot(far_onehot, own_slice, preferred_element_type=f32)
    for place, k in enumerate(far):
        packed[0, k] = pack(slots[place * cap : (place + 1) * cap]).astype(bf16)

    pl.semaphore_wait(barrier, n_ep + n_tp - 2)

    def net(k, expert, q, sem):
        owner = 2 * pair_up[q] + core
        return remote(packed.at[q, k], rows_in.at[owner, k],
                      send_sem.at[sem], net_recv_sem.at[k], expert, sibling)

    @pl.when(me < n_ep - 1)
    def _():
        to_right.start()

    @pl.when(me > 0)
    def _():
        to_left.start()

    @pl.when(me == 0)
    def _():
        low_kv[...] = jnp.zeros_like(low_kv)

    @pl.when(me == n_ep - 1)
    def _():
        high_kv[...] = jnp.zeros_like(high_kv)

    for base, experts in far_batches:
        for i, expert in enumerate(experts):
            start(net(base + i, expert, 0, 0))

    for q in range(n_pair):
        for side in range(2):
            owner = 2 * pair_up[q] + (core if side == 0 else 1 - core)
            rows = close_onehot if side == 0 else close_onehot[:cap]
            slots = jnp.dot(rows, normed_v[:, columns_of(owner, slice_width)], preferred_element_type=f32)
            rows_in[owner, 0] = pack(slots[:cap]).astype(bf16)
            if side == 0:
                for place, k in enumerate(close[1:]):
                    place = (place + 1) * cap
                    packed[q, k] = pack(slots[place : place + cap]).astype(bf16)

    for k in close[1:]:
        for q in range(n_pair):
            start(net(k, experts_of[k], q, 1))

    loads[12].wait()
    loads[7].wait()
    query = [
        turn(query_v[:, pl.ds(column, LANES)]) for column in range(0, query_v.shape[1], LANES)
    ]
    local = lax.broadcasted_iota(jnp.int32, (row_count, WINDOW), 0)
    other = lax.broadcasted_iota(jnp.int32, (row_count, WINDOW), 1)

    def split_heads(packed_rows):
        both = packed_rows.astype(f32)
        swapped = pltpu.roll(both, head_dim, 1)
        low = lax.broadcasted_iota(jnp.int32, both.shape, 1) < head_dim
        return jnp.where(low, both, swapped).astype(bf16), jnp.where(low, swapped, both).astype(bf16)

    own_rows = jnp.abs(
        lax.broadcasted_iota(jnp.int32, (row_count, row_count), 0)
        - lax.broadcasted_iota(jnp.int32, (row_count, row_count), 1)
    ) <= WINDOW
    own_keys, own_values = split_heads(own_kv[...])
    head_queries, own_scores = [], []

    def score(head_query, keys, allowed):
        scores = lax.dot_general(
            head_query, keys, (((1,), (1,)), ((), ())), preferred_element_type=f32
        ) * head_dim ** (-0.5)
        return jnp.where(allowed, scores, MASK_VALUE)

    for head in range(local_heads):
        mine = low_lane if head % 2 == 0 else jnp.logical_not(low_lane)
        head_queries.append(jnp.where(mine, query[head // 2], 0.0).astype(bf16))
        own_scores.append(score(head_queries[head], own_keys, own_rows))

    @pl.when(me > 0)
    def _():
        to_right.wait_recv()

    @pl.when(me < n_ep - 1)
    def _():
        to_left.wait_recv()

    low_allowed = (local - (other - WINDOW) <= WINDOW) & (me > 0)
    high_allowed = (row_count + other - local <= WINDOW) & (me < n_ep - 1)
    low_keys, low_values = split_heads(low_kv[...])
    high_keys, high_values = split_heads(high_kv[...])
    values = jnp.concatenate([low_values, own_values, high_values], axis=0)
    blocks = []
    for head in range(local_heads):
        parts = [
            score(head_queries[head], low_keys, low_allowed),
            own_scores[head],
            score(head_queries[head], high_keys, high_allowed),
        ]
        sink = sink_v[:, head : head + 1]
        highest = [jnp.max(part, axis=-1, keepdims=True) for part in parts]
        if row_count == WINDOW:
            highest = [jnp.max(functools.reduce(jnp.maximum, parts), axis=-1, keepdims=True)]
        largest = functools.reduce(jnp.maximum, highest + [sink])
        weights = [jnp.exp(part - largest) for part in parts]
        totals = [jnp.sum(weight, axis=-1, keepdims=True) for weight in weights]
        if row_count == WINDOW:
            totals = [jnp.sum(functools.reduce(jnp.add, weights), axis=-1, keepdims=True)]
        denominator = functools.reduce(jnp.add, totals) + jnp.exp(sink - largest)
        scale = 1.0 / denominator
        probability = jnp.concatenate([(weight * scale).astype(bf16) for weight in weights], axis=1)
        result = jnp.dot(probability, values, preferred_element_type=f32)
        if head % 2 == 0:
            blocks.append(result)
        else:
            blocks[-1] = jnp.where(low_lane, blocks[-1], result)
    attended = jnp.concatenate(blocks, axis=1).astype(bf16)[:, : local_heads * head_dim]
    loads[8].wait()
    partial_sum = jnp.dot(attended, out_w[...], preferred_element_type=f32)
    mix_send[...] = partial_sum.reshape(mix_send.shape).astype(bf16)

    def mix_own(p):
        return 2 * pair_up[p] + (core if p == 0 else 1 - core)

    def mix_other(p):
        return 2 * pair_up[p] + (1 - core if p == 0 else core)

    mix_pairs = [
        remote(mix_send.at[mix_other(p)], mix_sib.at[p],
               send_sem.at[4], mix_sib_recv_sem.at[p], me, sibling)
        for p in range(n_pair)
    ]
    for p in list(range(1, n_pair)) + [0]:
        start(mix_pairs[p])

    loads[1].wait()
    blocked = halves * cap
    number = lax.broadcasted_iota(jnp.int32, (blocked, row_count), 0)
    slot_of = number
    left = number >= 0
    if tail:
        in_main = number < 2 * main
        slot_of = jnp.where(
            in_main,
            jnp.where(number < main, number, number - main),
            jnp.where(number < 2 * main + tail, number - main, number - main - tail),
        )
        left = (number < main) | (jnp.logical_not(in_main) & (number < 2 * main + tail))
    lefts, rights = [], []
    for k in range(n_ep):
        placed = jnp.zeros((blocked, row_count), f32)
        for j in range(TOP):
            chosen = jnp.where(routes[j] == experts_of[k], rank[j], -1) == slot_of
            placed = jnp.where(chosen, route_weight_v[j : j + 1, :], placed)
        lefts.append(jnp.where(left, placed, 0.0))
        rights.append(jnp.where(left, 0.0, placed))
    combine_left[...] = jnp.concatenate(lefts, axis=0).T.astype(bf16)
    if tail:
        combine_right[...] = jnp.concatenate(rights, axis=0).T.astype(bf16)

    def near_forward(k, q, sem):
        owner = 2 * pair_up[q] + 1 - core
        return remote(rows_in.at[owner, k], rows_in.at[owner, k],
                      send_sem.at[2], near_recv_sem.at[sem], me, sibling)

    def far_forward(k, p):
        owner = 2 * pair + 1 - core
        return remote(rows_in.at[owner, k], rows_in.at[owner, k],
                      send_sem.at[3], far_recv_sem.at[p - 1, k - half_count], me, 2 * pair_up[p] + 1 - core)

    def far_relay(k, p, sem):
        owner = 2 * pair_down[p] + core
        return remote(rows_in.at[owner, k], rows_in.at[owner, k],
                      send_sem.at[2], near_recv_sem.at[sem], me, sibling)

    def forward_far(number):
        base, experts = far_batches[number]
        for i, expert in enumerate(experts):
            net(base + i, expert, 0, 0).wait_recv()
            for p in range(1, n_pair):
                start(far_forward(base + i, p))
            start(near_forward(base + i, 0, number))

    def relay_far(number):
        base, experts = far_batches[number]
        for i in range(len(experts)):
            for p in range(1, n_pair):
                far_forward(base + i, p).wait_recv()
                start(far_relay(base + i, p, number))

    def either(number, action):
        for swapped in range(2):
            @pl.when(swap == swapped)
            def _():
                action([k for k in near_lists[(number + swapped) % 2] if k])

    def forward_near(number):
        def action(slots):
            for k in slots:
                arrived(rows_in.at[pl.ds(0, n_pair), k], net_recv_sem.at[k])
                for q in range(n_pair):
                    start(near_forward(k, q, 2 + number))

        either(number, action)

    def gather(number):
        slots = []
        for base, experts in groups[number]:
            slots += [base + i for i in range(len(experts))]
        arrived(rows_in.at[pl.ds(0, n_pair), pl.ds(0, quarter)], near_recv_sem.at[number])
        either(number, lambda near: arrived(
            rows_in.at[pl.ds(0, n_pair), pl.ds(0, len(near))], near_recv_sem.at[2 + number]
        ))
        for owner in range(n_tp):
            for half in range(halves):
                columns = pl.ds(owner * slice_width + half * piece, piece)
                for place, k in enumerate(slots):
                    gathered[pl.ds(place * main, main), columns] = (
                        rows_in[owner, k, pl.ds(half * main, main), :]
                    )
                if tail:
                    ends = [
                        rows_in[owner, k, pl.ds(2 * main, 2 * tail), :].astype(f32)[
                            half * tail : (half + 1) * tail
                        ]
                        for k in slots
                    ]
                    gathered[pl.ds(len(slots) * main, len(slots) * tail), columns] = (
                        jnp.concatenate(ends, axis=0).astype(bf16)
                    )

    hidden_width = gate_w.shape[1]
    tile = min(hidden_width, 512)

    rows = half_count * cap

    def expand():
        for number in range(hidden_width // tile):
            columns = pl.ds(number * tile, tile)
            gate_act = jnp.dot(gathered[...], gate_w[:, columns], preferred_element_type=f32)
            up_act = jnp.dot(gathered[...], up_w[:, columns], preferred_element_type=f32)
            hidden[:, columns] = (gate_act / (1.0 + jnp.exp(-gate_act)) * up_act).astype(bf16)

    def down_slice(number, owner):
        result = jnp.dot(
            hidden[...], down_w[:, columns_of(owner, slice_width)], preferred_element_type=f32
        )
        slots = [base + i for base, experts in groups[number] for i in range(len(experts))]
        for place, k in enumerate(slots):
            values = result[place * main : (place + 1) * main]
            if tail:
                last = half_count * main + place * tail
                values = jnp.concatenate([values, result[last : last + tail]], axis=0)
            yield k, pack(values)

    def sib_copy(base, p):
        batch = pl.ds(base, quarter)
        return remote(sib_send.at[p, batch], sib_recv.at[p, batch],
                      send_sem.at[5], sib_recv_sem.at[p, base // quarter], me, sibling)

    def cross_copy(k, p):
        return remote(cross_send.at[p, k], cross_recv.at[p, k],
                      send_sem.at[6], cross_recv_sem.at[p - 1, k], me, 2 * pair_up[p] + 1 - core)

    def give(number, p):
        owner = 2 * pair_up[p] + (core if p == 0 else 1 - core)
        for k, values in down_slice(number, owner):
            sib_send[p, k] = values.astype(bf16)
        for base, _ in groups[number]:
            start(sib_copy(base, p))

    def keep(number, p):
        owner = 2 * pair_up[p] + (1 - core if p == 0 else core)
        for k, values in down_slice(number, owner):
            own_acc[p, k] = values

    def in_order(batch):
        base, experts = batch
        if quarter % 2:
            return [(base + i, experts[i]) for i in range(quarter)]
        odd = lax.rem(me, 2)
        return [
            (base + i + odd * (j - i), experts[i] + odd * (experts[j] - experts[i]))
            for i, j in [(i, i + 1 - 2 * (i % 2)) for i in range(quarter)]
        ]

    outer = in_order(near_pair[1])
    inner = [(k, experts_of[k]) for k in range(1, quarter)]
    own = [(0, me)]

    def cross(slots):
        for p in range(1, n_pair):
            for k, _ in slots:
                cross_send[p, k] = (own_acc[p, k] + sib_recv[p, k].astype(f32)).astype(bf16)
                start(cross_copy(k, p))

    def met(batch, parts):
        for p in parts:
            sib_copy(batch[0], p).wait_recv()

    def finish(slots):
        for k, expert in slots:
            total = own_acc[0, k] + sib_recv[0, k].astype(f32)
            for p in range(1, n_pair):
                cross_copy(k, p).wait_recv()
                total += cross_recv[p, k].astype(f32)
            final_send[k] = total.astype(bf16)
            start(remote(final_send.at[k], returned.at[k],
                         send_sem.at[7], final_recv_sem.at[0], expert, sibling))

    def mix_forward():
        for p in range(1, n_pair):
            mix_pairs[p].wait_recv()
            mix_cross[p] = (
                mix_send[mix_own(p)].astype(f32) + mix_sib[p].astype(f32)
            ).astype(bf16)
            start(mix_copy(p))

    def mix_copy(p):
        return remote(mix_cross.at[p], mix_recv.at[p],
                      send_sem.at[8], mix_recv_sem.at[p], me, 2 * pair_up[p] + 1 - core)

    def mix_finish():
        mix_pairs[0].wait_recv()
        mixed = mix_send[mix_own(0)].astype(f32) + mix_sib[0].astype(f32)
        for p in range(1, n_pair):
            mix_copy(p).wait_recv()
            mixed += mix_recv[p].astype(f32)
        mixer_ref[...] = mixed.astype(mixer_ref.dtype)

    others = range(1, n_pair)
    forward_far(0)
    forward_far(1)
    relay_far(0)
    mix_forward()
    forward_near(0)
    loads[9].wait()
    loads[10].wait()
    gather(0)
    expand()
    loads[11].wait()
    for p in others:
        give(0, p)
    relay_far(1)
    forward_near(1)
    for p in others:
        keep(0, p)
    give(0, 0)
    def where(swapped, action, slots):
        @pl.when(swap == swapped)
        def _():
            action(slots)

    far_slots = [in_order(batch) for batch in far_batches]
    met(far_batches[0], others)
    cross(far_slots[0])
    keep(0, 0)
    gather(1)
    met(near_batches[0], others)
    where(0, cross, inner)
    where(1, cross, outer)
    expand()
    for p in others:
        give(1, p)
        keep(1, p)
    give(1, 0)
    met(far_batches[1], others)
    met(near_batches[1], others)
    where(1, cross, inner)
    cross(far_slots[1])
    met(far_batches[0], [0])
    finish(far_slots[0])
    where(0, cross, outer)
    cross(own)
    keep(1, 0)
    met(near_batches[0], [0])
    where(0, finish, inner)
    where(1, finish, outer)
    met(far_batches[1], [0])
    met(near_batches[1], [0])
    where(1, finish, inner)
    finish(far_slots[1])
    mix_finish()
    where(0, finish, outer)
    finish(own)

    arrived(returned, final_recv_sem.at[0])
    blocks = returned[...].reshape(n_ep * blocked, piece)

    def combined(weights_ref):
        return lax.dot_general(
            weights_ref[...], blocks, (((1,), (0,)), ((), ())), preferred_element_type=f32
        )

    expert_ref[:, :piece] = combined(combine_left).astype(expert_ref.dtype)
    if tail:
        expert_ref[:, piece:] = combined(combine_right).astype(expert_ref.dtype)

    @pl.when(me < n_ep - 1)
    def _():
        to_right.wait_send()

    @pl.when(me > 0)
    def _():
        to_left.wait_send()

    far_count = n_ep - half_count
    arrived(packed.at[0, pl.ds(0, far_count)], send_sem.at[0])
    arrived(packed.at[:, pl.ds(0, half_count - 1)], send_sem.at[1])
    arrived(rows_in.at[pl.ds(0, n_pair), pl.ds(0, n_ep - 1)], send_sem.at[2])
    if n_pair > 1:
        arrived(rows_in.at[pl.ds(0, n_pair - 1), pl.ds(0, far_count)], send_sem.at[3])
    arrived(mix_sib, send_sem.at[4])
    if n_pair > 1:
        arrived(mix_cross.at[pl.ds(0, n_pair - 1)], send_sem.at[8])
    arrived(sib_send, send_sem.at[5])
    if n_pair > 1:
        arrived(cross_send.at[pl.ds(0, n_pair - 1)], send_sem.at[6])
    arrived(final_send, send_sem.at[7])


def write_kernel(mixer_in, expert_in, mixer_out, expert_out, sem):
    copies = [
        pltpu.make_async_copy(mixer_in, mixer_out, sem.at[0]),
        pltpu.make_async_copy(expert_in, expert_out, sem.at[1]),
    ]
    for copy in copies:
        copy.start()
    for copy in copies:
        copy.wait()


def on_device(
    queries,
    key_states,
    value_states,
    sink_logit,
    out_weight,
    expert_input,
    norm_gain,
    routes,
    route_weight,
    gate_weight,
    up_weight,
    down_weight,
):
    n_ep = lax.axis_size("ep")
    n_tp = lax.axis_size("tp")
    row_count, width = expert_input.shape
    local_heads = queries.shape[1] // HEAD_DIM
    capacity = row_count * TOP * 5 // (4 * n_ep)
    main, tail = capacity // 16 * 16, 0
    if 0 < capacity - main <= 8 and width // n_tp >= 2 * LANES and main:
        tail = 8
    elif capacity > main:
        main += 16
    halves = 2 if tail else 1
    slice_width = width // n_tp
    piece = slice_width // halves
    blocked = halves * (main + tail)
    hidden_width = gate_weight.shape[2]
    mix_rows = row_count // n_tp
    n_pair = n_tp // 2
    group_rows = n_ep // 2 * (main + tail)
    if queries.shape[1] % LANES:
        queries = jnp.pad(queries, ((0, 0), (0, LANES - queries.shape[1] % LANES)))
    table = jnp.asarray(angle_table(row_count, n_ep))
    vmem = pl.BlockSpec(memory_space=pltpu.VMEM)
    hbm = pl.BlockSpec(memory_space=pltpu.HBM)
    bf16, f32 = jnp.bfloat16, jnp.float32
    dma = pltpu.SemaphoreType.DMA
    traveling = (blocked, piece)
    operands = (
        queries,
        key_states,
        value_states,
        table,
        sink_logit[None, :],
        expert_input,
        norm_gain[None, :],
        routes.T,
        route_weight.T,
        out_weight,
        gate_weight,
        up_weight,
        down_weight,
    )
    mixer_out, expert_out = pl.pallas_call(
        functools.partial(fused_kernel, (n_ep, n_tp, main, tail)),
        out_shape=(
            jax.ShapeDtypeStruct((mix_rows, width), bf16),
            jax.ShapeDtypeStruct((row_count, slice_width), bf16),
        ),
        in_specs=[hbm] * 13,
        out_specs=(vmem, vmem),
        scratch_shapes=[
            pltpu.VMEM(queries.shape, bf16),
            pltpu.VMEM((row_count, LANES), bf16),
            pltpu.VMEM((row_count, LANES), bf16),
            pltpu.VMEM(table.shape, f32),
            pltpu.VMEM((1, local_heads), f32),
            pltpu.VMEM(expert_input.shape, bf16),
            pltpu.VMEM((1, width), f32),
            pltpu.VMEM((TOP, row_count), jnp.int32),
            pltpu.VMEM((TOP, row_count), f32),
            pltpu.VMEM(out_weight.shape, bf16),
            pltpu.VMEM(gate_weight.shape[1:], bf16),
            pltpu.VMEM(up_weight.shape[1:], bf16),
            pltpu.VMEM(down_weight.shape[1:], bf16),
            pltpu.VMEM(expert_input.shape, bf16),
            pltpu.VMEM((row_count, LANES), bf16),
            pltpu.VMEM((row_count, LANES), bf16),
            pltpu.VMEM((WINDOW, LANES), bf16),
            pltpu.VMEM((WINDOW, LANES), bf16),
            pltpu.VMEM((n_pair, n_ep) + traveling, bf16),
            pltpu.VMEM((n_tp, n_ep) + traveling, bf16),
            pltpu.VMEM((group_rows, width), bf16),
            pltpu.VMEM((group_rows, hidden_width), bf16),
            pltpu.VMEM((n_tp, mix_rows, width), bf16),
            pltpu.VMEM((n_pair, mix_rows, width), bf16),
            pltpu.VMEM((n_pair, mix_rows, width), bf16),
            pltpu.VMEM((n_pair, mix_rows, width), bf16),
            pltpu.VMEM((n_pair, n_ep) + traveling, bf16),
            pltpu.VMEM((n_pair, n_ep) + traveling, bf16),
            pltpu.VMEM((n_pair, n_ep) + traveling, f32),
            pltpu.VMEM((n_pair, n_ep) + traveling, bf16),
            pltpu.VMEM((n_pair, n_ep) + traveling, bf16),
            pltpu.VMEM((n_ep,) + traveling, bf16),
            pltpu.VMEM((n_ep,) + traveling, bf16),
            pltpu.VMEM((row_count, n_ep * blocked), bf16),
            pltpu.VMEM((row_count, n_ep * blocked), bf16),
            dma((13,)),
            dma((2,)),
            dma((2,)),
            dma((9,)),
            dma((n_ep,)),
            dma((n_pair - 1, n_ep // 2)),
            dma((4,)),
            dma((n_pair,)),
            dma((n_pair,)),
            dma((n_pair, 4)),
            dma((n_pair - 1, n_ep)),
            dma((1,)),
        ],
        compiler_params=pltpu.CompilerParams(
            collective_id=0, has_side_effects=True, vmem_limit_bytes=50000 * 1024
        ),
    )(*[
        pltpu.with_memory_space_constraint(operand, pltpu.HBM) if operand.size > 1 else operand
        for operand in operands
    ])
    return pl.pallas_call(
        write_kernel,
        out_shape=(
            jax.ShapeDtypeStruct(mixer_out.shape, bf16),
            jax.ShapeDtypeStruct(expert_out.shape, bf16),
        ),
        in_specs=[vmem] * 2,
        out_specs=(hbm, hbm),
        scratch_shapes=[dma((2,))],
        compiler_params=pltpu.CompilerParams(vmem_limit_bytes=1024 * 1024),
    )(*[pltpu.with_memory_space_constraint(x, pltpu.VMEM) for x in (mixer_out, expert_out)])


def solution(mesh):
    in_specs = (
        P("ep", "tp"),
        P("ep", None),
        P("ep", None),
        P("tp"),
        P("tp", None),
        P("ep", None),
        P(),
        P("ep", None),
        P("ep", None),
        P("ep", None, "tp"),
        P("ep", None, "tp"),
        P("ep", "tp", None),
    )
    out_specs = (P(("ep", "tp"), None), P("ep", "tp"))
    return jax.shard_map(
        on_device, mesh=mesh, in_specs=in_specs, out_specs=out_specs, check_vma=False
    )
```
